32 devices in a mesh: sp: 4 (over z), fs: 4 (over y, core), tp: 2 (over x).
Axes of the slice: x: 2, y: 2, z: 4, core: 2. Of those that a mesh axis runs over, the one named last changes fastest.
Arguments:
- tokens: bfloat16 [4, 4096, 2048], P('fs', 'sp', 'tp'), may hold values from -8 to 8
- norm_gain: float32 [2048], replicated, may hold values from 0.1 to 1.9
- w_query: bfloat16 [2048, 1024], P(('sp', 'fs'), 'tp'), may hold values from -4 to 4
- w_key: bfloat16 [2048, 512], P(('sp', 'fs'), 'tp'), may hold values from -0.16 to 0.16
- w_value: bfloat16 [2048, 512], P(('sp', 'fs'), 'tp'), may hold values from -0.125 to 0.125
- w_conv_in: bfloat16 [2048, 1024], P(('sp', 'fs'), 'tp'), may hold values from -0.125 to 0.125
- w_conv_b: bfloat16 [2048, 1024], P(('sp', 'fs'), 'tp'), may hold values from -0.125 to 0.125
- w_conv_c: bfloat16 [2048, 1024], P(('sp', 'fs'), 'tp'), may hold values from -0.125 to 0.125
- conv_taps: bfloat16 [3, 1024], P(None, 'tp'), may hold values from -3.5 to 3.5
- sink_logits: float32 [16], P('tp'), may hold values from 1 to 5
- w_attn_out: bfloat16 [1024, 2048], P('tp', ('sp', 'fs')), may hold values from -0.375 to 0.375
- w_conv_out: bfloat16 [1024, 2048], P('tp', ('sp', 'fs')), may hold values from -0.125 to 0.125
Outputs:
- mixed: bfloat16 [4, 4096, 2048], P('fs', ('sp', 'tp'))
The draws below stay inside these ranges and needn't reach their ends.
All inputs are finite; a program needn't handle non-finite values.
Results may differ from the reference program's by a relative error of at most 0.02.
Values may be sent and summed in bfloat16 or wider, within the bound.
A program may use at most 128 MiB of HBM per device.

```python
import jax
import jax.numpy as jnp
from jax import lax

D = 2048
HEADS = 16
KV_HEADS = 8
HEAD = 64
CONV = 1024
WINDOW = 128
SEQS = 4
LENGTH = 4096
N_TP = 2


def query_key_pair(key):
    folded = jax.random.fold_in(key, 11)
    first, second = jax.random.split(folded, 2)
    key_weights = jnp.clip(jax.random.normal(first, (D, KV_HEADS * HEAD), jnp.float32) * D ** (-0.5), -0.15, 0.15)
    query_weights = jax.random.normal(second, (D, HEADS * HEAD), jnp.float32) * D ** (-0.5)
    query_weights = jnp.clip(query_weights, -4.0, 4.0)
    return (query_weights, key_weights)


def draw_w_query(key, part):
    return query_key_pair(key)[0].astype(jnp.bfloat16)


def draw_w_key(key, part):
    return query_key_pair(key)[1].astype(jnp.bfloat16)


def draw_tokens(key, part):
    folded = jax.random.fold_in(key, 23)
    first = jax.random.fold_in(folded, 0)
    values = jax.random.normal(first, (SEQS, LENGTH, D), jnp.float32)
    return jnp.clip(values, -8.0, 8.0).astype(jnp.bfloat16)


def block_levels(own_key, extent, shards, least, top_value):
    def one(axis_at, shards_of):
        heights = jax.random.uniform(jax.random.fold_in(jax.random.fold_in(own_key, 6), axis_at), (shards_of,), jnp.float32, least / len(shards), top_value / len(shards))
        return jnp.repeat(jnp.exp(heights), extent[axis_at] // shards_of).reshape((-1,) + (1,) * (len(extent) - axis_at - 1))

    gain = one(*shards[0])
    for cut in shards[1:]:
        gain = gain * one(*cut)
    return gain


def normal_values(key, dims, deviation, bound, shards=(), kind=jnp.bfloat16):
    entries = jax.random.normal(key, dims, jnp.float32) * deviation
    if len(shards) > 0:
        entries = block_levels(key, dims, shards, -0.22, 0.18) * entries
    return jnp.clip(entries, min=-bound, max=bound).astype(kind)


def setup_inputs(seed: int = 0) -> dict:
    key_list = jax.random.split(jax.random.key(seed), 13)
    return {
        "tokens": draw_tokens(jax.random.fold_in(key_list[12], 71), 0),
        "norm_gain": jnp.clip(1.0 + 0.18 * jax.random.normal(key_list[1], (D,), jnp.float32), 0.1, 1.9),
        "w_query": draw_w_query(jax.random.fold_in(key_list[12], 71), 0),
        "w_key": draw_w_key(jax.random.fold_in(key_list[12], 71), 0),
        "w_value": normal_values(key_list[4], (D, KV_HEADS * HEAD), D ** -0.5, 0.125, ((0, 16), (1, 2))),
        "w_conv_in": normal_values(key_list[5], (D, CONV), D ** -0.5, 0.125, ((0, 16), (1, 2))),
        "w_conv_b": normal_values(key_list[6], (D, CONV), D ** -0.5, 0.125, ((0, 16), (1, 2))),
        "w_conv_c": normal_values(key_list[7], (D, CONV), D ** -0.5, 0.125, ((0, 16), (1, 2))),
        "conv_taps": normal_values(key_list[8], (3, CONV), 3 ** -0.5, 3.5, ((1, 2),)),
        "sink_logits": jnp.clip(1.0 + 4.0 * jax.random.uniform(key_list[9], (HEADS,), jnp.float32) ** block_levels(key_list[9], (HEADS,), ((0, 2),), -0.2, 0.2), 1.0, 5.0),
        "w_attn_out": normal_values(key_list[10], (HEADS * HEAD, D), (D // 8) ** -0.5, 0.375, ((0, 2), (1, 16))),
        "w_conv_out": normal_values(key_list[11], (CONV, D), D ** -0.5, 0.125, ((0, 2), (1, 16))),
    }


def norm_rows(tokens, norm_gain):
    values = tokens.astype(jnp.float32)
    average = lax.optimization_barrier(jnp.mean(values, axis=-1, keepdims=True))
    centred = values - average
    variance = lax.optimization_barrier(jnp.mean(centred * centred, axis=-1, keepdims=True))
    return (centred * lax.rsqrt(variance + 1e-05) * norm_gain.astype(jnp.float32)).astype(jnp.bfloat16)

def project(normed, weight):
    return jnp.dot(normed, weight, preferred_element_type=jnp.float32).astype(jnp.bfloat16)

def window_attention(queries, keys, values, sink_logits):
    length = queries.shape[0]
    blocks = length // WINDOW
    group = HEADS // KV_HEADS
    query_form = queries.astype(jnp.float32).reshape(blocks, WINDOW, KV_HEADS, group, HEAD)
    zero_rows = jnp.zeros((WINDOW, KV_HEADS * HEAD), jnp.bfloat16)
    padded_keys = jnp.concatenate([zero_rows, keys], axis=0).astype(jnp.float32).reshape(blocks + 1, WINDOW, KV_HEADS, HEAD)
    padded_values = jnp.concatenate([zero_rows, values], axis=0).astype(jnp.float32).reshape(blocks + 1, WINDOW, KV_HEADS, HEAD)
    band_keys = jnp.concatenate([padded_keys[:-1], padded_keys[1:]], axis=1)
    band_values = jnp.concatenate([padded_values[:-1], padded_values[1:]], axis=1)
    scores = jnp.einsum('bqkgd,bskd->bkgqs', query_form, band_keys) * HEAD ** (-0.5)
    row_ids = jnp.arange(WINDOW, dtype=jnp.int32)[:, None]
    col_ids = jnp.arange(2 * WINDOW, dtype=jnp.int32)[None, :]
    distance = WINDOW + row_ids - col_ids
    head_ids = jnp.arange(HEADS, dtype=jnp.int32).reshape(KV_HEADS, group)
    slopes = jnp.exp2(-8.0 * (head_ids + 1).astype(jnp.float32) / HEADS)
    scores = scores - slopes[:, :, None, None] * distance.astype(jnp.float32)
    key_place = jnp.arange(blocks, dtype=jnp.int32)[:, None] * WINDOW - WINDOW + jnp.arange(2 * WINDOW, dtype=jnp.int32)[None, :]
    inside = (distance >= 0) & (distance < WINDOW)
    keep = inside[None, None, None, :, :] & (key_place >= 0)[:, None, None, None, :]
    scores = jnp.where(keep, scores, -jnp.inf)
    sinks = sink_logits.astype(jnp.float32).reshape(KV_HEADS, group)[:, :, None, None]
    highest = jnp.maximum(lax.optimization_barrier(jnp.max(scores, axis=-1, keepdims=True)), sinks)
    raised = jnp.exp(scores - highest)
    denominator = lax.optimization_barrier(jnp.sum(raised, axis=-1, keepdims=True)) + jnp.exp(sinks - highest)
    weights = (raised / denominator).astype(jnp.bfloat16)
    mixed = jnp.einsum('bkgqs,bskd->bqkgd', weights.astype(jnp.float32), band_values)
    return mixed.astype(jnp.bfloat16).reshape(length, HEADS * HEAD)

def reference(tokens, norm_gain, w_query, w_key, w_value, w_conv_in, w_conv_b, w_conv_c, conv_taps, sink_logits, w_attn_out, w_conv_out):
    normed_all = norm_rows(tokens, norm_gain)
    head_cols = HEADS * HEAD // N_TP
    chan_cols = CONV // N_TP
    taps = conv_taps.astype(jnp.float32)

    def one_sequence(normed):
        queries = project(normed, w_query)
        keys = project(normed, w_key)
        values = project(normed, w_value)
        inner = project(normed, w_conv_in)
        gate_b = project(normed, w_conv_b)
        gate_c = project(normed, w_conv_c)
        attended = window_attention(queries, keys, values, sink_logits)
        product = (gate_c.astype(jnp.float32) * inner.astype(jnp.float32)).astype(jnp.bfloat16)
        padded = jnp.concatenate([jnp.zeros((2, CONV), jnp.float32), product.astype(jnp.float32)], axis=0)
        length = product.shape[0]
        filtered = taps[0] * padded[0:length] + taps[1] * padded[1:length + 1] + taps[2] * padded[2:length + 2]
        conv_out = (gate_b.astype(jnp.float32) * filtered).astype(jnp.bfloat16)
        summed = jnp.zeros((length, D), jnp.float32)
        for group_id in range(N_TP):
            head_slice = slice(group_id * head_cols, (group_id + 1) * head_cols)
            chan_slice = slice(group_id * chan_cols, (group_id + 1) * chan_cols)
            partial_sum = jnp.dot(attended[:, head_slice], w_attn_out[head_slice], preferred_element_type=jnp.float32)
            partial_sum = partial_sum + jnp.dot(conv_out[:, chan_slice], w_conv_out[chan_slice], preferred_element_type=jnp.float32)
            summed = summed + partial_sum.astype(jnp.bfloat16).astype(jnp.float32)
        return summed.astype(jnp.bfloat16)
    return lax.map(one_sequence, normed_all)
```

```python
import functools

import jax
import jax.numpy as jnp
from jax import lax
from jax.experimental import pallas as pl
from jax.experimental.pallas import tpu as pltpu
from jax.sharding import PartitionSpec as P

HEADS = 16
HEAD = 64
WINDOW = 128
HALO = 16
MESH = pl.DeviceIdType.MESH
BF16, F32 = jnp.bfloat16, jnp.float32


def when(condition, body):
    if condition is True:
        body()
    else:
        pl.when(condition)(body)


class Part:
    def __init__(self, number, wide, place, base):
        self.number, self.wide, self.place, self.base = number, wide, place, base


def part_kinds(out_rows):
    kinds = [(False, None), (True, None), (False, None), (False, None), (False, None)]
    quarter, eighth = out_rows // 4, out_rows // 8
    kinds += [(False, (n * quarter, quarter)) for n in range(3)]
    kinds += [(True, (3 * quarter, eighth)), (False, (3 * quarter + eighth, eighth))]
    return kinds


def layer_kernel(sizes, *refs):
    n_sp, n_out, n_tp, n_proj, separate = sizes
    tok, gain, taps, sinks = refs[:4]
    n_in = 6 if separate else 5
    w_own = refs[4 : 4 + n_in]
    out_own = refs[4 + n_in : 6 + n_in]
    out = refs[6 + n_in]
    (tokf, w_all, wo_all, q_buf, kv_buf, inner, gate_b, product, m_att, m_conv, r_att, r_conv, bias,
     send_sem, recv_sem, own_sem, wo_send, wo_recv, tok_send, tok_recv, halo_send, halo_recv,
     mix_send, mix_recv) = refs[7 + n_in :]
    n_fs = 2 * n_out
    shards = n_sp * n_fs
    s, f, t = lax.axis_index("sp"), lax.axis_index("fs"), lax.axis_index("tp")
    o, i = f // 2, f % 2
    rows_total, width = tokf.shape
    cols = tok.shape[1]
    q_cols = q_buf.shape[1]
    kv_cols = kv_buf.shape[1] // 2
    k_rows = w_own[0].shape[0]
    out_rows, out_cols = out_own[0].shape
    owned = rows_total // n_tp
    chunks = 4
    step = rows_total // chunks
    order = [chunks - 1] + list(range(chunks - 1))
    me = s * n_fs + f

    right, left, core = (s + 1, f, t), (s - 1, f, t), (s, o * 2 + (1 - i), t)
    across = [(s, lax.rem(o + k, n_out) * 2 + i, t) for k in range(1, n_out)]
    peers = [(s, f, lax.rem(t + k, n_tp)) for k in range(1, n_tp)]
    has_right, has_left = s < n_sp - 1, s > 0

    local = []
    spots = [(0, 0), (1, 0), (1, kv_cols), (2, 0), (3, 0), (4, 0)] if separate else [(n, 0) for n in range(5)]
    for n, (number, col) in enumerate(spots):
        place = w_all.at[number, pl.ds(me * k_rows, k_rows), pl.ds(col, w_own[n].shape[1])]
        local.append(pltpu.make_async_copy(w_own[n], place, own_sem.at[n]))
    for a in range(2):
        local.append(pltpu.make_async_copy(out_own[a], wo_all.at[2 * t + a, me], own_sem.at[6 + a]))
    my_cols = pl.ds(pl.multiple_of(t * cols, cols), cols)
    local.append(pltpu.make_async_copy(tok, tokf.at[:, my_cols], own_sem.at[8]))
    for copy in local:
        copy.start()

    barrier = pltpu.get_barrier_semaphore()
    greet = lambda where: pl.semaphore_signal(barrier, inc=1, device_id=where, device_id_type=MESH)
    when(has_right, lambda: greet(right))
    when(has_left, lambda: greet(left))
    for where in across + [core] + peers:
        greet(where)
    count = len(across) + 1 + len(peers)
    pl.semaphore_wait(barrier, count + has_right.astype(jnp.int32) + has_left.astype(jnp.int32))

    wo_copies, tok_copies = [], {}
    for k, peer in enumerate(peers):
        for a in range(2):
            copy = pltpu.make_async_remote_copy(
                src_ref=out_own[a], dst_ref=wo_all.at[2 * t + a, me],
                send_sem=wo_send.at[k, a], recv_sem=wo_recv.at[k, a], device_id=peer, device_id_type=MESH,
            )
            copy.start()
            wo_copies.append(copy)
    for n in order:
        here = pl.ds(n * step, step)
        for k, peer in enumerate(peers):
            copy = pltpu.make_async_remote_copy(
                src_ref=tok.at[here], dst_ref=tokf.at[here, my_cols],
                send_sem=tok_send.at[k, n], recv_sem=tok_recv.at[k, n], device_id=peer, device_id_type=MESH,
            )
            copy.start()
            tok_copies[k, n] = copy

    parts, base = [], 0
    for number, (wide, rows) in enumerate(part_kinds(out_rows)):
        if rows is None:
            place = lambda src, number=number: w_all.at[number, pl.ds(src * k_rows, k_rows)]
        else:
            place = lambda src, rows=rows: wo_all.at[:, src, pl.ds(*rows)]
        parts.append(Part(number, wide, place, base))
        base += (5 if wide else 4) * n_sp * 2 if n_out > 1 else 2 * n_sp * 2

    def copy_of(part, src, where, lane, distance, side):
        spot = part.place(src)
        return pltpu.make_async_remote_copy(
            src_ref=spot, dst_ref=spot,
            send_sem=send_sem.at[part.base + lane * n_sp * 2 + distance * 2 + side],
            recv_sem=recv_sem.at[part.number * shards + src],
            device_id=where, device_id_type=MESH,
        )

    def deal(part, distance, k, drain):
        ys = [(2 + n, where) for n, where in enumerate(across)]
        lanes = 0 if k == 0 else 2 + (len(across) if part.wide else len(across) - 1) + 2 * (k - 1) + (0 if part.wide else 1)
        lane_z, lane_core = (0, 1) if k == 0 else (lanes, lanes + (1 if part.wide else 0))
        source_o = lax.rem(o + n_out - k, n_out)
        first = isinstance(distance, int) and distance == 0
        for side in (0,) if first else (0, 1):
            source_s = s if first else (s - distance if side == 0 else s + distance)
            there = True if first else (source_s >= 0 if side == 0 else source_s < n_sp)
            src = source_s * n_fs + source_o * 2 + i

            def body(side=side, src=src):
                def go(where, lane, at):
                    copy = copy_of(part, src, where, lane, distance, at)
                    copy.wait_send() if drain else copy.start()

                if not (first and k == 0) and not drain:
                    copy_of(part, src, core, 0, 0, 0).wait_recv()
                if k == 0 or part.wide:
                    if first or side == 0:
                        when(has_right, lambda: go(right, lane_z, 0))
                    if first or side == 1:
                        when(has_left, lambda: go(left, lane_z, 1))
                if k == 0 and (first or not part.wide):
                    for lane, where in ys:
                        go(where, lane, side)
                go(core, lane_core, side)

            when(there, body)

    def stage(number, n):
        part = parts[number]
        last = n_sp - 1
        if not (isinstance(n, int) and n > last):
            deal(part, n, 0, False)
        if isinstance(n, int) and n == 0:
            return
        for k in range(1, n_out):
            deal(part, n - 1, k, False)

    def partner(number, source_s):
        part = parts[number]
        for source_o in range(n_out):
            copy_of(part, source_s * n_fs + source_o * 2 + (1 - i), core, 0, 0, 0).wait_recv()

    def finish(number):
        for source_s in range(n_sp):
            partner(number, source_s)

    def tokens_in(n):
        for k in range(n_tp - 1):
            tok_copies[k, n].wait_recv()

    def norm(n):
        size = 32

        def body(r, carry):
            here = pl.ds(pl.multiple_of(n * step + r * size, size), size)
            values = tokf[here, :].astype(F32)
            centred = values - jnp.sum(values, axis=1, keepdims=True) * (1.0 / width)
            variance = jnp.sum(centred * centred, axis=1, keepdims=True) * (1.0 / width)
            tokf[here, :] = (centred * lax.rsqrt(variance + 1e-05) * gain[...]).astype(BF16)
            return carry

        lax.fori_loop(0, step // size, body, 0)

    def project(number, ns):
        def body(m, carry):
            n = m if len(ns) == chunks else ns[0] + m
            first = n * step if isinstance(n, int) else pl.multiple_of(n * step, step)
            here = pl.ds(first, step)
            result = jnp.dot(tokf[here, :], w_all[number], preferred_element_type=F32).astype(BF16)
            if number == 0:
                q_buf[here, :] = result
            elif number == 1:
                kv_buf[pl.ds(first + WINDOW, step), :] = result
            elif number == 2:
                inner[here, :] = result
            elif number == 3:
                gate_b[here, :] = result
            else:
                made = result.astype(F32) * inner[here, :].astype(F32)
                product[pl.ds(first + HALO, step), :] = made.astype(BF16)
            return carry

        if len(ns) == 1:
            body(0, 0)
        else:
            lax.fori_loop(0, len(ns), body, 0)

    def halo_copy(which):
        buffer, size = ((kv_buf, WINDOW), (product, HALO))[which]
        return pltpu.make_async_remote_copy(
            src_ref=buffer.at[pl.ds(rows_total, size)], dst_ref=buffer.at[pl.ds(0, size)],
            send_sem=halo_send.at[which], recv_sem=halo_recv.at[which], device_id=right, device_id_type=MESH,
        )

    def halo_out(which):
        when(has_right, lambda: halo_copy(which).start())

        def clear():
            buffer, size = ((kv_buf, WINDOW), (product, HALO))[which]
            buffer[0:size, :] = jnp.zeros((size, buffer.shape[1]), BF16)

        when(s == 0, clear)

    def halo_in(which):
        when(has_left, lambda: halo_copy(which).wait_recv())

    heads_here = q_cols // HEAD
    kv_here = kv_cols // HEAD
    group = heads_here // kv_here
    tall = group * WINDOW

    def make_bias():
        row = lax.broadcasted_iota(jnp.int32, (tall, 2 * WINDOW), 0)
        col = lax.broadcasted_iota(jnp.int32, (tall, 2 * WINDOW), 1)
        distance = WINDOW + row % WINDOW - col
        keep = (distance >= 0) & (distance < WINDOW)
        for h in range(kv_here):
            head = (t * heads_here + h * group + row // WINDOW + 1).astype(F32)
            slope = jnp.exp2(head * (-8.0 / HEADS))
            bias[h] = jnp.where(keep, -(slope * distance.astype(F32)), -jnp.inf)

    def attend(n):
        row = lax.broadcasted_iota(jnp.int32, (tall, 1), 0) // WINDOW
        col = lax.broadcasted_iota(jnp.int32, (1, 2 * WINDOW), 1)

        def body(b, carry):
            block = n * (step // WINDOW) + b
            first = pl.multiple_of(block * WINDOW, WINDOW)
            before = jnp.where(col >= WINDOW, 0.0, jnp.where((s == 0) & (block == 0), -jnp.inf, 0.0))
            queries = q_buf[pl.ds(first, WINDOW), :]
            band = kv_buf[pl.ds(first, 2 * WINDOW), :]
            outs = []
            for h in range(kv_here):
                query = jnp.concatenate(
                    [queries[:, (h * group + g) * HEAD : (h * group + g + 1) * HEAD] for g in range(group)], axis=0
                )
                key = band[:, h * HEAD : (h + 1) * HEAD]
                value = band[:, kv_cols + h * HEAD : kv_cols + (h + 1) * HEAD]
                scores = lax.dot_general(query, key, (((1,), (1,)), ((), ())), preferred_element_type=F32)
                scores = scores * HEAD ** (-0.5) + bias[h] + before
                sink = jnp.full((tall, 1), sinks[h * group], F32)
                for g in range(1, group):
                    sink = jnp.where(row == g, sinks[h * group + g], sink)
                top = jnp.maximum(jnp.max(scores, axis=1, keepdims=True), sink)
                raised = jnp.exp(scores - top)
                total = jnp.sum(raised, axis=1, keepdims=True) + jnp.exp(sink - top)
                weights = (raised * (1.0 / total)).astype(BF16)
                mixed = jnp.dot(weights, value, preferred_element_type=F32).astype(BF16)
                outs += [mixed[g * WINDOW : (g + 1) * WINDOW] for g in range(group)]
            m_att[pl.ds(first, WINDOW), :] = jnp.concatenate(outs, axis=1)
            return carry

        lax.fori_loop(0, step // WINDOW, body, 0)

    def convolve():
        size = 64

        def body(r, carry):
            first = pl.multiple_of(r * size, size)
            padded = product[pl.ds(first, size + HALO), :].astype(F32)
            tap = taps[...].astype(F32)
            filtered = (
                tap[0:1] * padded[HALO - 2 : HALO - 2 + size]
                + tap[1:2] * padded[HALO - 1 : HALO - 1 + size]
                + tap[2:3] * padded[HALO : HALO + size]
            )
            m_conv[pl.ds(first, size), :] = (gate_b[pl.ds(first, size), :].astype(F32) * filtered).astype(BF16)
            return carry

        lax.fori_loop(0, rows_total // size, body, 0)

    def mix_copy(which, k):
        source, target = ((m_att, r_att), (m_conv, r_conv))[which]
        return pltpu.make_async_remote_copy(
            src_ref=source.at[pl.ds(pl.multiple_of(peers[k][2] * owned, owned), owned)], dst_ref=target.at[k],
            send_sem=mix_send.at[which, k], recv_sem=mix_recv.at[which, k],
            device_id=peers[k], device_id_type=MESH,
        )

    def mix_out(which):
        for k in range(n_tp - 1):
            mix_copy(which, k).start()

    def mix_in():
        for which in range(2):
            for k in range(n_tp - 1):
                mix_copy(which, k).wait_recv()

    def project_out(source_s):
        for number in range(n_proj, len(parts)):
            partner(number, source_s)
        block = n_fs * out_cols
        tile = min(256, owned)

        def weights(row):
            blocks = [wo_all[row, source_s * n_fs + n] for n in range(n_fs)]
            return jnp.concatenate(blocks, axis=1)

        def body(r, carry):
            total = jnp.zeros((tile, block), F32)
            for k in range(n_tp):
                g = lax.rem(t + n_tp - k, n_tp)
                if k == 0:
                    here = pl.ds(pl.multiple_of(t * owned + r * tile, tile), tile)
                    att, conv = m_att[here, :], m_conv[here, :]
                else:
                    here = pl.ds(pl.multiple_of(r * tile, tile), tile)
                    att, conv = r_att[k - 1, here, :], r_conv[k - 1, here, :]
                partial = jnp.dot(att, weights(2 * g), preferred_element_type=F32)
                partial = partial + jnp.dot(conv, weights(2 * g + 1), preferred_element_type=F32)
                total = total + partial.astype(BF16).astype(F32)
            where = pl.ds(pl.multiple_of(source_s * block, block), block)
            out[pl.ds(pl.multiple_of(r * tile, tile), tile), where] = total.astype(BF16)
            return carry

        lax.fori_loop(0, owned // tile, body, 0)

    def first_chunk():
        tokens_in(order[0])
        norm(order[0])
        project(0, [order[0]])
        project(1, [order[0]])
        halo_out(0)

    def chunk(n):
        tokens_in(n)
        norm(n)
        project(0, [n])
        project(1, [n])

    def wo_ready():
        for copy in wo_copies:
            copy.wait_recv()

    for copy in local[:6] if separate else local[:5]:
        copy.wait()
    if n_sp <= 4:
        work = {
            (0, 1): [make_bias],
            (0, 2): [local[-3].wait, local[-2].wait, local[-1].wait, wo_ready],
            (2, 1): [first_chunk],
            (3, 1): [lambda: chunk(0)],
            (3, 2): [lambda: halo_in(0), lambda: attend(0)],
            (3, 3): [lambda: project(2, [3]), lambda: project(2, [0])],
            (4, 1): [lambda: chunk(1)],
            (4, 2): [lambda: attend(1)],
            (4, 3): [lambda: project(2, [1]), lambda: project(3, [0, 1]), lambda: project(3, [3])],
            (5, 1): [lambda: chunk(2)],
            (5, 2): [lambda: attend(2)],
            (5, 3): [lambda: attend(3), lambda: mix_out(0)],
            (6, 1): [lambda: project(2, [2]), lambda: project(3, [2]), lambda: project(4, [0, 1, 2, 3]), lambda: halo_out(1)],
            (6, 2): [lambda: halo_in(1), convolve, lambda: mix_out(1)],
        }
        total = len(parts)
        stage(0, 0)
        for number in range(total):
            for n in range(1, n_sp + 1):
                stage(number, n)
                if n == 1 and number + 1 < total:
                    stage(number + 1, 0)
                for job in work.get((number, n), []):
                    job()
                if number == total - 1:
                    if n == 1:
                        mix_in()
                        project_out(s)
                    if n > 1:
                        d = n - 1
                        when(s - d >= 0, lambda: project_out(s - d))
                        when(s + d < n_sp, lambda: project_out(s + d))
            if number < n_proj:
                finish(number)
    else:
        for copy in local[-3:]:
            copy.wait()
        wo_ready()

        def spread(number):
            stage(number, 0)
            stage(number, 1)
            lax.fori_loop(2, n_sp, lambda n, c: (stage(number, n), c)[1], 0)
            stage(number, n_sp)

        for number in range(n_proj):
            spread(number)
            finish(number)
        make_bias()
        first_chunk()
        for n in order[1:]:
            chunk(n)
        halo_in(0)
        for n in range(chunks):
            attend(n)
        mix_out(0)
        for number in (2, 3, 4):
            project(number, list(range(chunks)))
        halo_out(1)
        halo_in(1)
        convolve()
        mix_out(1)
        for number in range(n_proj, len(parts)):
            spread(number)
        mix_in()
        lax.fori_loop(0, n_sp, lambda n, c: (project_out(n), c)[1], 0)

    for part in parts:
        for k in range(n_out):
            deal(part, 0, k, True)
            if n_sp <= 4:
                for distance in range(1, n_sp):
                    deal(part, distance, k, True)
            else:
                lax.fori_loop(1, n_sp, lambda n, c, part=part, k=k: (deal(part, n, k, True), c)[1], 0)
    for which in range(2):
        when(has_right, lambda which=which: halo_copy(which).wait_send())
        for k in range(n_tp - 1):
            mix_copy(which, k).wait_send()
    for copy in wo_copies + list(tok_copies.values()):
        copy.wait_send()


def on_device(tokens, norm_gain, w_query, w_key, w_value, w_conv_in, w_conv_b, w_conv_c,
              conv_taps, sink_logits, w_attn_out, w_conv_out):
    n_sp, n_fs, n_tp = (lax.axis_size(axis) for axis in ("sp", "fs", "tp"))
    n_out = n_fs // 2
    shards = n_sp * n_fs
    rows, cols = tokens.shape[1:]
    width = cols * n_tp
    q_cols, kv_cols, channels = w_query.shape[1], w_key.shape[1], w_conv_in.shape[1]
    out_rows, out_cols = w_attn_out.shape
    separate = kv_cols % 128 == 0
    weights = [w_query]
    weights += [w_key, w_value] if separate else [jnp.concatenate([w_key, w_value], axis=1)]
    weights += [w_conv_in, w_conv_b, w_conv_c]
    owned = rows // n_tp
    kinds = part_kinds(out_rows)
    lanes = sum((5 if wide else 4) if n_out > 1 else 2 for wide, _ in kinds)
    kv_here = kv_cols // HEAD
    group = q_cols // kv_cols
    dma = pltpu.SemaphoreType.DMA
    vmem, anywhere = pl.BlockSpec(memory_space=pltpu.VMEM), pl.BlockSpec(memory_space=pl.ANY)
    summed = pl.pallas_call(
        functools.partial(layer_kernel, (n_sp, n_out, n_tp, 5, separate)),
        out_shape=jax.ShapeDtypeStruct((owned, width), BF16),
        in_specs=[anywhere, vmem, vmem, pl.BlockSpec(memory_space=pltpu.SMEM)] + [anywhere] * (len(weights) + 2),
        out_specs=vmem,
        scratch_shapes=[
            pltpu.VMEM((rows, width), BF16),
            pltpu.VMEM((5, width, q_cols), BF16),
            pltpu.VMEM((2 * n_tp, shards, out_rows, out_cols), BF16),
            pltpu.VMEM((rows, q_cols), BF16),
            pltpu.VMEM((WINDOW + rows, 2 * kv_cols), BF16),
            pltpu.VMEM((rows, channels), BF16),
            pltpu.VMEM((rows, channels), BF16),
            pltpu.VMEM((HALO + rows, channels), BF16),
            pltpu.VMEM((rows, q_cols), BF16),
            pltpu.VMEM((rows, channels), BF16),
            pltpu.VMEM((n_tp - 1, owned, q_cols), BF16),
            pltpu.VMEM((n_tp - 1, owned, channels), BF16),
            pltpu.VMEM((kv_here, group * WINDOW, 2 * WINDOW), F32),
            dma((lanes * n_sp * 2,)),
            dma((len(kinds) * shards,)),
            dma((9,)),
            dma((n_tp - 1, 2)),
            dma((n_tp - 1, 2)),
            dma((n_tp - 1, 4)),
            dma((n_tp - 1, 4)),
            dma((2,)),
            dma((2,)),
            dma((2, n_tp - 1)),
            dma((2, n_tp - 1)),
        ],
        compiler_params=pltpu.CompilerParams(
            collective_id=0, has_side_effects=True, vmem_limit_bytes=60 * 1024 * 1024
        ),
    )(tokens[0], norm_gain[None], conv_taps, sink_logits, *weights, w_attn_out, w_conv_out)
    return summed[None]


def solution(mesh):
    placed = (
        P("fs", "sp", "tp"),
        P(),
        P(("sp", "fs"), "tp"),
        P(("sp", "fs"), "tp"),
        P(("sp", "fs"), "tp"),
        P(("sp", "fs"), "tp"),
        P(("sp", "fs"), "tp"),
        P(("sp", "fs"), "tp"),
        P(None, "tp"),
        P("tp"),
        P("tp", ("sp", "fs")),
        P("tp", ("sp", "fs")),
    )
    return jax.shard_map(
        on_device,
        mesh=mesh,
        in_specs=placed,
        out_specs=P("fs", ("sp", "tp"), None),
        check_vma=False,
    )
```

```python
import functools

import jax
import jax.numpy as jnp
from jax import lax
from jax.experimental import pallas as pl
from jax.experimental.pallas import tpu as pltpu
from jax.sharding import PartitionSpec as P

HEADS = 16
HEAD = 64
WINDOW = 128
HALO = 16
MESH = pl.DeviceIdType.MESH
BF16, F32 = jnp.bfloat16, jnp.float32


TABLE_FOR = (4, 2, 2)
TABLE = (
    (0, 1, 0, 0, 0, 2), (0, 1, 0, 0, 0, 3), (0, 2, 0, 0, 0, 3), (0, 2, 0, 0, 0, 2), (0, 1, 1, 0, 0, 3),
    (0, 0, 0, 0, 0, 2), (0, 0, 0, 0, 0, 1), (0, 1, 0, 0, 0, 1), (0, 0, 0, 1, 0, 2), (0, 1, 0, 0, 0, 0),
    (0, 0, 0, 0, 0, 3), (0, 0, 0, 0, 0, 0), (0, 8, 0, 0, 0, 1), (0, 2, 0, 1, 1, 2), (0, 7, 0, 0, 0, 3),
    (0, 4, 0, 0, 0, 2), (0, 1, 1, 0, 0, 2), (0, 1, 0, 1, 0, 2), (0, 0, 0, 1, 0, 3), (0, 7, 0, 0, 0, 0),
    (0, 0, 0, 1, 1, 0), (0, 4, 0, 0, 0, 1), (0, 0, 0, 2, 0, 3), (0, 3, 0, 0, 0, 3), (0, 8, 0, 0, 0, 0),
    (0, 2, 0, 0, 0, 1), (0, 5, 0, 0, 0, 0), (0, 1, 0, 1, 0, 1), (0, 1, 1, 0, 0, 1), (0, 0, 0, 1, 1, 2),
    (0, 0, 0, 1, 1, 1), (0, 3, 0, 1, 1, 2), (0, 1, 1, 0, 0, 0), (0, 4, 0, 0, 0, 0), (0, 0, 1, 0, 0, 0),
    (0, 6, 0, 0, 0, 3), (0, 6, 0, 0, 0, 2), (0, 2, 0, 1, 0, 2), (0, 0, 0, 1, 0, 1), (0, 4, 0, 1, 1, 2),
    (0, 3, 0, 0, 0, 1), (0, 2, 0, 0, 0, 0), (0, 0, 1, 0, 0, 1), (0, 0, 0), (0, 4, 0, 0, 0, 3), (0, 1, 1, 1, 1, 0),
    (0, 2, 0, 1, 1, 0), (0, 0, 0, 2, 1, 1), (0, 1, 0, 2, 0, 3), (0, 2, 0, 1, 0, 1), (0, 8, 1, 0, 0, 1),
    (0, 3, 0, 2, 1, 1), (0, 2, 1, 0, 0, 0), (0, 1, 1, 1, 1, 2), (0, 0, 1, 0, 0, 3), (0, 1, 1, 1, 0, 2),
    (0, 1, 0, 1, 1, 2), (0, 2, 0, 2, 1, 1), (0, 5, 0, 0, 0, 3), (0, 7, 0, 0, 0, 1), (0, 1, 1, 1, 0, 3),
    (0, 6, 1, 0, 0, 3), (0, 0, 0, 3, 1, 0), (0, 3, 0, 0, 0, 0), (0, 8, 0, 0, 0, 2), (0, 3, 0, 3, 1, 0),
    (0, 5, 0, 1, 0, 1), (0, 2, 1, 1, 1, 2), (0, 0, 0, 2, 0, 2), (0, 1, 0, 2, 0, 2), (0, 4, 0, 1, 0, 3),
    (0, 6, 0, 0, 0, 0), (0, 0, 0, 2, 1, 0), (0, 1, 1, 1, 0, 1), (0, 4, 1, 1, 0, 3), (0, 8, 0, 1, 0, 2),
    (0, 8, 0, 0, 0, 3), (0, 2, 1, 0, 0, 2), (0, 0, 1, 3, 1, 0), (0, 1, 1, 2, 1, 1), (0, 1, 0, 1, 1, 0),
    (0, 4, 1, 0, 0, 2), (0, 2, 0, 2, 0, 2), (0, 4, 0, 1, 0, 1), (0, 0, 1, 2, 1, 1), (1, 3, 0), (1, 0, 0),
    (0, 1, 0, 2, 1, 1), (0, 3, 0, 0, 0, 2), (0, 6, 1, 0, 0, 0), (0, 2, 0, 2, 0, 3), (0, 8, 1, 0, 0, 2),
    (0, 8, 1, 1, 0, 3), (0, 8, 0, 2, 0, 3), (0, 8, 1, 0, 0, 0), (0, 0, 1, 2, 0, 2), (0, 3, 0, 1, 1, 1),
    (0, 8, 0, 1, 1, 2), (0, 1, 1, 2, 0, 2), (0, 1, 0, 1, 1, 1), (0, 3, 0, 1, 0, 1), (0, 7, 1, 0, 0, 0),
    (0, 5, 0, 0, 0, 2), (0, 8, 1, 0, 0, 3), (0, 7, 0, 1, 1, 2), (0, 0, 1, 1, 0, 2), (0, 2, 0, 3, 1, 0),
    (0, 1, 0, 3, 0, 3), (0, 4, 1, 0, 0, 0), (0, 3, 0, 2, 1, 0), (0, 8, 1, 1, 1, 1), (0, 3, 0, 2, 0, 2),
    (0, 2, 0, 1, 0, 3), (0, 2, 0, 1, 1, 1), (0, 5, 1, 1, 0, 1), (0, 1, 0, 1, 0, 3), (0, 0, 1, 2, 0, 3),
    (0, 4, 0, 2, 1, 1), (0, 1, 1, 1, 1, 1), (0, 2, 1, 3, 1, 0), (0, 8, 1, 1, 0, 1), (0, 0, 0, 3, 0, 3),
    (0, 2, 1, 1, 0, 1), (0, 0, 1, 1, 0, 3), (1, 1, 0), (0, 8, 0, 2, 0, 2), (0, 4, 1, 0, 0, 3), (0, 2, 0, 3, 0, 3),
    (0, 1, 0, 2, 1, 0), (0, 7, 1, 0, 0, 3), (0, 3, 0, 3, 0, 3), (0, 3, 1, 3, 1, 0), (0, 8, 1, 1, 0, 2),
    (1, 8, 1, 0, 0, 0), (0, 8, 0, 1, 0, 1), (0, 3, 0, 1, 1, 0), (0, 5, 1, 0, 0, 0), (0, 4, 0, 1, 1, 1),
    (0, 0, 1, 0, 0, 2), (0, 1, 1, 3, 0, 3), (0, 1, 0, 3, 1, 0), (0, 0, 1, 3, 0, 3), (0, 7, 0, 1, 0, 1),
    (0, 5, 1, 0, 0, 2), (0, 8, 1, 2, 0, 2), (0, 0, 1, 1, 1, 2), (0, 2, 1, 2, 0, 3), (0, 6, 0, 0, 0, 1),
    (0, 5, 0, 2, 0, 2), (0, 0, 1, 1, 1, 0), (0, 8, 0, 2, 1, 1), (0, 0, 1, 2, 1, 0), (0, 5, 0, 0, 0, 1),
    (0, 3, 1, 0, 0, 1), (0, 0, 1, 1, 1, 1), (0, 6, 0, 1, 1, 2), (0, 4, 1, 2, 1, 1), (0, 0, 1, 1, 0, 1),
    (0, 3, 1, 0, 0, 2), (0, 1, 1, 3, 1, 0), (0, 1, 1, 2, 0, 3), (1, 8, 0, 0, 0, 0), (1, 2, 0), (0, 5, 1, 0, 0, 3),
    (2, 0, 0), (0, 8, 0, 1, 0, 3), (0, 3, 1, 0, 0, 0), (0, 8, 0, 1, 1, 1), (0, 2, 0, 2, 1, 0), (0, 4, 1, 1, 1, 2),
    (0, 2, 1, 3, 0, 3), (0, 8, 1, 1, 1, 2), (0, 5, 0, 1, 0, 3), (0, 5, 0, 1, 1, 1), (0, 3, 1, 2, 0, 2),
    (0, 2, 1, 1, 1, 0), (0, 3, 0, 1, 0, 2), (0, 8, 0, 3, 0, 3), (0, 3, 1, 0, 0, 3), (0, 5, 0, 1, 1, 2), (2, 2, 0),
    (0, 4, 0, 3, 1, 0), (1, 8, 0, 1, 0, 1), (0, 4, 0, 2, 0, 2), (0, 8, 1, 2, 1, 1), (0, 8, 1, 3, 0, 3),
    (0, 6, 0, 1, 1, 1), (0, 1, 1, 2, 1, 0), (0, 3, 1, 3, 0, 3), (1, 8, 0, 2, 1, 1), (0, 4, 0, 1, 0, 2), (2, 1, 0),
    (2, 3, 0), (0, 4, 0, 1, 1, 0), (0, 5, 0, 3, 0, 3), (0, 2, 1, 0, 0, 1), (0, 6, 0, 1, 0, 1), (0, 3, 0, 1, 0, 3),
    (0, 7, 0, 2, 1, 1), (2, 2, 1), (2, 3, 1), (1, 8, 1, 0, 0, 2), (3, 3, 0), (0, 2, 1, 1, 0, 2), (2, 1, 1),
    (1, 8, 0, 1, 1, 1), (0, 3, 1, 1, 1, 1), (0, 6, 1, 1, 1, 2), (2, 0, 1), (0, 4, 0, 2, 1, 0), (0, 5, 1, 2, 0, 2),
    (0, 8, 0, 3, 1, 0), (0, 7, 0, 1, 0, 2), (0, 4, 1, 3, 1, 0), (0, 2, 1, 2, 0, 2), (0, 8, 1, 2, 1, 0),
    (0, 6, 0, 1, 1, 0), (1, 8, 0, 2, 0, 3), (0, 3, 1, 1, 0, 2), (0, 8, 0, 1, 1, 0), (0, 2, 1, 2, 1, 1),
    (0, 5, 0, 1, 1, 0), (0, 5, 1, 3, 0, 3), (1, 8, 1, 2, 1, 1), (0, 3, 1, 2, 1, 0), (0, 5, 1, 1, 0, 3),
    (1, 8, 0, 0, 0, 2), (1, 8, 0, 1, 1, 2), (0, 7, 1, 1, 1, 2), (0, 3, 1, 1, 0, 1), (0, 3, 0, 2, 0, 3),
    (0, 6, 0, 2, 0, 2), (0, 5, 1, 1, 1, 2), (0, 3, 1, 2, 1, 1), (0, 8, 1, 2, 0, 3), (1, 8, 1, 2, 0, 2),
    (1, 8, 0, 1, 0, 3), (1, 8, 1, 3, 0, 3), (0, 4, 0, 3, 0, 3), (0, 2, 1, 0, 0, 3), (0, 7, 0, 0, 0, 2), (3, 1, 0),
    (0, 4, 0, 2, 0, 3), (1, 8, 1, 0, 0, 3), (0, 3, 1, 1, 0, 3), (0, 3, 1, 1, 1, 2), (1, 8, 1, 0, 0, 1),
    (0, 3, 1, 1, 1, 0), (3, 2, 0), (0, 5, 1, 1, 1, 1), (0, 2, 1, 1, 0, 3), (1, 8, 0, 0, 0, 3), (0, 4, 1, 0, 0, 1),
    (0, 6, 0, 1, 0, 2), (0, 6, 1, 1, 1, 0), (0, 8, 1, 3, 1, 0), (0, 8, 0, 2, 1, 0), (3, 0, 0), (0, 3, 1, 2, 0, 3),
    (0, 7, 0, 1, 1, 0), (0, 6, 1, 0, 0, 2), (0, 4, 1, 1, 1, 0), (0, 2, 1, 1, 1, 1), (0, 4, 1, 1, 0, 1),
    (0, 4, 1, 1, 1, 1), (0, 4, 1, 1, 0, 2), (0, 2, 1, 2, 1, 0), (0, 6, 0, 1, 0, 3), (1, 8, 0, 3, 1, 0),
    (0, 5, 0, 2, 1, 1), (1, 8, 1, 2, 1, 0), (0, 4, 1, 2, 0, 2), (4, 0, 0), (0, 4, 1, 2, 1, 0), (2, 0, 3),
    (0, 7, 0, 2, 0, 3), (2, 3, 3), (2, 1, 2), (0, 7, 1, 2, 1, 1), (0, 5, 1, 0, 0, 1), (1, 8, 0, 2, 0, 2), (2, 3, 2),
    (0, 5, 0, 2, 1, 0), (0, 7, 0, 2, 0, 2), (0, 4, 1, 2, 0, 3), (2, 2, 3), (0, 4, 1, 3, 0, 3), (1, 8, 1, 1, 0, 1),
    (0, 6, 0, 3, 0, 3), (0, 7, 1, 0, 0, 1), (0, 5, 1, 2, 1, 1), (2, 1, 3), (0, 6, 0, 2, 1, 1), (2, 3, 4),
    (1, 8, 0, 1, 0, 2), (2, 0, 2), (0, 7, 1, 0, 0, 2), (0, 7, 0, 1, 0, 3), (0, 5, 0, 3, 1, 0), (1, 8, 1, 2, 0, 3),
    (2, 0, 4), (0, 7, 1, 1, 0, 2), (2, 1, 4), (0, 5, 0, 1, 0, 2), (1, 8, 1, 1, 0, 2), (2, 2, 2), (0, 7, 1, 2, 0, 2),
    (0, 7, 0, 3, 0, 3), (0, 6, 0, 2, 1, 0), (0, 6, 1, 1, 0, 3), (0, 5, 1, 2, 1, 0), (1, 8, 0, 0, 0, 1),
    (0, 6, 1, 1, 0, 1), (0, 6, 1, 0, 0, 1), (1, 8, 0, 1, 1, 0), (0, 7, 1, 1, 1, 0), (0, 7, 1, 1, 0, 1), (2, 2, 4),
    (5, 0, 0), (0, 6, 0, 3, 1, 0), (0, 6, 1, 2, 1, 0), (1, 8, 1, 1, 1, 1), (0, 7, 1, 2, 0, 3), (0, 5, 1, 1, 1, 0),
    (0, 6, 0, 2, 0, 3), (0, 5, 0, 2, 0, 3), (0, 6, 1, 2, 0, 2), (0, 6, 1, 1, 1, 1), (0, 7, 0, 3, 1, 0),
    (1, 8, 1, 1, 0, 3), (0, 7, 0, 2, 1, 0), (0, 6, 1, 2, 1, 1), (0, 8, 1, 1, 1, 0), (0, 7, 1, 3, 1, 0),
    (1, 8, 0, 2, 1, 0), (0, 6, 1, 3, 1, 0), (0, 7, 0, 1, 1, 1), (0, 6, 1, 3, 0, 3), (7, 0, 0), (0, 6, 1, 2, 0, 3),
    (0, 6, 1, 1, 0, 2), (0, 7, 1, 1, 0, 3), (0, 5, 1, 2, 0, 3), (0, 5, 1, 3, 1, 0), (1, 8, 1, 1, 1, 2),
    (0, 7, 1, 1, 1, 1), (1, 8, 1, 3, 1, 0), (0, 7, 1, 3, 0, 3), (0, 5, 1, 1, 0, 2), (7, 2, 0), (7, 1, 1), (7, 1, 0),
    (7, 3, 1), (7, 3, 0), (1, 8, 0, 3, 0, 3), (0, 7, 1, 2, 1, 0), (7, 2, 1), (6, 0, 0), (8, 2, 1), (1, 8, 1, 1, 1, 0),
    (8, 0, 0), (8, 3, 1), (8, 3, 0), (8, 1, 1), (8, 1, 0), (8, 2, 0),
)


def when(condition, body):
    if condition is True:
        body()
    elif condition is not False:
        pl.when(condition)(body)


class Part:
    def __init__(self, number, wide, crossing, place, base):
        self.number, self.wide, self.crossing, self.place, self.base = number, wide, crossing, place, base


def part_kinds(out_rows):
    kinds = [(False, False, None), (True, False, None)] + [(False, False, None)] * 3
    quarter = out_rows // 4
    kinds += [(False, False, (n * quarter, quarter)) for n in range(3)]
    return kinds + [(True, True, (3 * quarter, quarter))]


def lanes_of(wide, n_out):
    return 1 + n_out + (2 if wide else 1) * (n_out - 1)


def layer_kernel(sizes, *refs):
    n_sp, n_out, n_tp, n_proj, separate = sizes
    tok, gain, taps, sinks = refs[:4]
    n_in = 6 if separate else 5
    w_own = refs[4 : 4 + n_in]
    out_own = refs[4 + n_in : 6 + n_in]
    out = refs[6 + n_in]
    (tokf, w_all, wo_all, q_buf, kv_buf, inner, gate_b, product, m_att, m_conv, r_att, r_conv, bias,
     send_sem, recv_sem, own_sem, wo_send, wo_recv, tok_send, tok_recv, halo_send, halo_recv,
     mix_send, mix_recv, cross_send, cross_recv, pass_send, pass_recv) = refs[7 + n_in :]
    n_fs = 2 * n_out
    shards = n_sp * n_fs
    s, f, t = lax.axis_index("sp"), lax.axis_index("fs"), lax.axis_index("tp")
    o, i = f // 2, f % 2
    rows_total, width = tokf.shape
    cols = tok.shape[1]
    q_cols = q_buf.shape[1]
    kv_cols = kv_buf.shape[1] // 2
    k_rows = w_own[0].shape[0]
    out_rows, out_cols = out_own[0].shape
    owned = rows_total // n_tp
    chunks = 4
    step = rows_total // chunks
    order = [chunks - 1] + list(range(chunks - 1))
    me = s * n_fs + f

    right, left, core = (s + 1, f, t), (s - 1, f, t), (s, o * 2 + (1 - i), t)
    across = [(s, lax.rem(o + k, n_out) * 2 + i, t) for k in range(1, n_out)]
    peers = [(s, f, lax.rem(t + k, n_tp)) for k in range(1, n_tp)]
    has_right, has_left = s < n_sp - 1, s > 0

    local = []
    spots = [(0, 0), (1, 0), (1, kv_cols), (2, 0), (3, 0), (4, 0)] if separate else [(n, 0) for n in range(5)]
    for n, (number, col) in enumerate(spots):
        place = w_all.at[number, pl.ds(me * k_rows, k_rows), pl.ds(col, w_own[n].shape[1])]
        local.append(pltpu.make_async_copy(w_own[n], place, own_sem.at[n]))
    for a in range(2):
        local.append(pltpu.make_async_copy(out_own[a], wo_all.at[2 * t + a, me], own_sem.at[6 + a]))
    my_cols = pl.ds(pl.multiple_of(t * cols, cols), cols)
    local.append(pltpu.make_async_copy(tok, tokf.at[:, my_cols], own_sem.at[8]))
    for copy in local:
        copy.start()

    barrier = pltpu.get_barrier_semaphore()
    greet = lambda where: pl.semaphore_signal(barrier, inc=1, device_id=where, device_id_type=MESH)
    when(has_right, lambda: greet(right))
    when(has_left, lambda: greet(left))
    for where in across + [core] + peers:
        greet(where)
    count = len(across) + 1 + len(peers)
    pl.semaphore_wait(barrier, count + has_right.astype(jnp.int32) + has_left.astype(jnp.int32))

    wo_copies, tok_copies = [], {}
    direct = pl.ds(0, 3 * (out_rows // 4))
    for k, peer in enumerate(peers):
        for a in range(2):
            copy = pltpu.make_async_remote_copy(
                src_ref=out_own[a].at[direct], dst_ref=wo_all.at[2 * t + a, me, direct],
                send_sem=wo_send.at[k, a], recv_sem=wo_recv.at[k, a], device_id=peer, device_id_type=MESH,
            )
            copy.start()
            wo_copies.append(copy)
    for n in order:
        here = pl.ds(n * step, step)
        for k, peer in enumerate(peers):
            copy = pltpu.make_async_remote_copy(
                src_ref=tok.at[here], dst_ref=tokf.at[here, my_cols],
                send_sem=tok_send.at[k, n], recv_sem=tok_recv.at[k, n], device_id=peer, device_id_type=MESH,
            )
            copy.start()
            tok_copies[k, n] = copy

    parts, base = [], 0
    for number, (wide, crossing, rows) in enumerate(part_kinds(out_rows)):
        if rows is None:
            place = lambda src, g, number=number: w_all.at[number, pl.ds(src * k_rows, k_rows)]
        elif crossing:
            place = lambda src, g, rows=rows: wo_all.at[pl.ds(2 * g, 2), src, pl.ds(*rows)]
        else:
            place = lambda src, g, rows=rows: wo_all.at[:, src, pl.ds(*rows)]
        parts.append(Part(number, wide, crossing, place, base))
        base += lanes_of(wide, n_out) * n_sp * 2

    def copy_of(part, src, where, lane, distance, side):
        spot = part.place(src, t)
        return pltpu.make_async_remote_copy(
            src_ref=spot, dst_ref=spot,
            send_sem=send_sem.at[part.base + (lane * n_sp + distance) * 2 + side],
            recv_sem=recv_sem.at[part.number * shards + src],
            device_id=where, device_id_type=MESH,
        )

    def cross_copy(part, src, k):
        spot = part.place(src, t)
        return pltpu.make_async_remote_copy(
            src_ref=spot, dst_ref=spot, send_sem=cross_send.at[k, src], recv_sem=cross_recv.at[k, src],
            device_id=peers[k], device_id_type=MESH,
        )

    def pass_copy(part, src, k):
        spot = part.place(src, lax.rem(t + n_tp - k - 1, n_tp))
        return pltpu.make_async_remote_copy(
            src_ref=spot, dst_ref=spot, send_sem=pass_send.at[k, src], recv_sem=pass_recv.at[k, src],
            device_id=core, device_id_type=MESH,
        )

    def source(k, at):
        return at * n_fs + lax.rem(o + n_out - k, n_out) * 2 + i

    def handle(part, k, distance, side, at, drain):
        first = isinstance(distance, int) and distance == 0
        src = source(k, at)
        mine = (at + distance if side == 0 else at - distance) if isinstance(at, int) else s
        more_right, more_left = mine < n_sp - 1, mine > 0
        lane_z, lane_core = 0, 1
        if k > 0:
            lane_z = 2 + len(across) + 2 * (k - 1)
            lane_core = lane_z + 1
            if not part.wide:
                lane_core = 2 + len(across) + k - 1

        def go(where, lane, way):
            copy = copy_of(part, src, where, lane, distance, way)
            copy.wait_send() if drain else copy.start()

        if not (first and k == 0) and not drain:
            copy_of(part, src, core, 0, 0, 0).wait_recv()
        if k == 0 or part.wide:
            if first or side == 0:
                when(more_right, lambda: go(right, lane_z, 0))
            if first or side == 1:
                when(more_left, lambda: go(left, lane_z, 1))
        if k == 0 and (first or not part.wide):
            for n, where in enumerate(across):
                go(where, 2 + n, side)
        if part.crossing:
            for n in range(len(peers)):
                copy = cross_copy(part, src, n)
                copy.wait_send() if drain else copy.start()
        go(core, lane_core, side)

    def hand_over(part, src, drain):
        for k in range(len(peers)):
            if not drain:
                cross_copy(part, src, k).wait_recv()
            copy = pass_copy(part, src, k)
            copy.wait_send() if drain else copy.start()

    def deal(part, distance, k, drain):
        if isinstance(distance, int) and distance == 0:
            handle(part, k, 0, 0, s, drain)
            return
        when(s - distance >= 0, lambda: handle(part, k, distance, 0, s - distance, drain))
        when(s + distance < n_sp, lambda: handle(part, k, distance, 1, s + distance, drain))

    def partner(number, source_s):
        for source_o in range(n_out):
            copy_of(parts[number], source_s * n_fs + source_o * 2 + (1 - i), core, 0, 0, 0).wait_recv()

    def finish(number):
        for source_s in range(n_sp):
            partner(number, source_s)

    def norm(n):
        size = 32

        def body(r, carry):
            here = pl.ds(pl.multiple_of(n * step + r * size, size), size)
            values = tokf[here, :].astype(F32)
            centred = values - jnp.sum(values, axis=1, keepdims=True) * (1.0 / width)
            variance = jnp.sum(centred * centred, axis=1, keepdims=True) * (1.0 / width)
            tokf[here, :] = (centred * lax.rsqrt(variance + 1e-05) * gain[...]).astype(BF16)
            return carry

        lax.fori_loop(0, step // size, body, 0)

    def project(number, ns):
        def body(m, carry):
            n = m if len(ns) == chunks else ns[0] + m
            first = n * step if isinstance(n, int) else pl.multiple_of(n * step, step)
            here = pl.ds(first, step)
            result = jnp.dot(tokf[here, :], w_all[number], preferred_element_type=F32).astype(BF16)
            if number == 0:
                q_buf[here, :] = result
            elif number == 1:
                kv_buf[pl.ds(first + WINDOW, step), :] = result
            elif number == 2:
                inner[here, :] = result
            elif number == 3:
                gate_b[here, :] = result
            else:
                made = result.astype(F32) * inner[here, :].astype(F32)
                product[pl.ds(first + HALO, step), :] = made.astype(BF16)
            return carry

        if len(ns) == 1:
            body(0, 0)
        else:
            lax.fori_loop(0, len(ns), body, 0)

    def halo_copy(which):
        buffer, size = ((kv_buf, WINDOW), (product, HALO))[which]
        return pltpu.make_async_remote_copy(
            src_ref=buffer.at[pl.ds(rows_total, size)], dst_ref=buffer.at[pl.ds(0, size)],
            send_sem=halo_send.at[which], recv_sem=halo_recv.at[which], device_id=right, device_id_type=MESH,
        )

    def halo_out(which):
        when(has_right, lambda: halo_copy(which).start())

        def clear():
            buffer, size = ((kv_buf, WINDOW), (product, HALO))[which]
            buffer[0:size, :] = jnp.zeros((size, buffer.shape[1]), BF16)

        when(s == 0, clear)

    def halo_in(which):
        when(has_left, lambda: halo_copy(which).wait_recv())

    heads_here = q_cols // HEAD
    kv_here = kv_cols // HEAD
    group = heads_here // kv_here
    tall = group * WINDOW

    def make_bias():
        row = lax.broadcasted_iota(jnp.int32, (tall, 2 * WINDOW), 0)
        col = lax.broadcasted_iota(jnp.int32, (tall, 2 * WINDOW), 1)
        distance = WINDOW + row % WINDOW - col
        keep = (distance >= 0) & (distance < WINDOW)
        for h in range(kv_here):
            head = (t * heads_here + h * group + row // WINDOW + 1).astype(F32)
            slope = jnp.exp2(head * (-8.0 / HEADS))
            bias[h] = jnp.where(keep, -(slope * distance.astype(F32)), -jnp.inf)

    def attend(n):
        row = lax.broadcasted_iota(jnp.int32, (tall, 1), 0) // WINDOW
        col = lax.broadcasted_iota(jnp.int32, (1, 2 * WINDOW), 1)

        def body(b, carry):
            block = n * (step // WINDOW) + b
            first = pl.multiple_of(block * WINDOW, WINDOW)
            before = jnp.where(col >= WINDOW, 0.0, jnp.where((s == 0) & (block == 0), -jnp.inf, 0.0))
            queries = q_buf[pl.ds(first, WINDOW), :]
            band = kv_buf[pl.ds(first, 2 * WINDOW), :]
            outs = []
            for h in range(kv_here):
                query = jnp.concatenate(
                    [queries[:, (h * group + g) * HEAD : (h * group + g + 1) * HEAD] for g in range(group)], axis=0
                )
                key = band[:, h * HEAD : (h + 1) * HEAD]
                value = band[:, kv_cols + h * HEAD : kv_cols + (h + 1) * HEAD]
                scores = lax.dot_general(query, key, (((1,), (1,)), ((), ())), preferred_element_type=F32)
                scores = scores * HEAD ** (-0.5) + bias[h] + before
                sink = jnp.full((tall, 1), sinks[h * group], F32)
                for g in range(1, group):
                    sink = jnp.where(row == g, sinks[h * group + g], sink)
                top = jnp.maximum(jnp.max(scores, axis=1, keepdims=True), sink)
                raised = jnp.exp(scores - top)
                total = jnp.sum(raised, axis=1, keepdims=True) + jnp.exp(sink - top)
                weights = (raised * (1.0 / total)).astype(BF16)
                mixed = jnp.dot(weights, value, preferred_element_type=F32).astype(BF16)
                outs += [mixed[g * WINDOW : (g + 1) * WINDOW] for g in range(group)]
            m_att[pl.ds(first, WINDOW), :] = jnp.concatenate(outs, axis=1)
            return carry

        lax.fori_loop(0, step // WINDOW, body, 0)

    def convolve():
        size = 64

        def body(r, carry):
            first = pl.multiple_of(r * size, size)
            padded = product[pl.ds(first, size + HALO), :].astype(F32)
            tap = taps[...].astype(F32)
            filtered = (
                tap[0:1] * padded[HALO - 2 : HALO - 2 + size]
                + tap[1:2] * padded[HALO - 1 : HALO - 1 + size]
                + tap[2:3] * padded[HALO : HALO + size]
            )
            m_conv[pl.ds(first, size), :] = (gate_b[pl.ds(first, size), :].astype(F32) * filtered).astype(BF16)
            return carry

        lax.fori_loop(0, rows_total // size, body, 0)

    def mix_copy(which, k):
        source, target = ((m_att, r_att), (m_conv, r_conv))[which]
        return pltpu.make_async_remote_copy(
            src_ref=source.at[pl.ds(pl.multiple_of(peers[k][2] * owned, owned), owned)], dst_ref=target.at[k],
            send_sem=mix_send.at[which, k], recv_sem=mix_recv.at[which, k],
            device_id=peers[k], device_id_type=MESH,
        )

    def mix_out(which):
        for k in range(n_tp - 1):
            mix_copy(which, k).start()

    def mix_in():
        for which in range(2):
            for k in range(n_tp - 1):
                mix_copy(which, k).wait_recv()

    def project_out(source_s, own):
        for number in range(n_proj, len(parts)):
            if own:
                partner(number, source_s)
            elif parts[number].crossing:
                for source_o in range(n_out):
                    for k in range(n_tp - 1):
                        pass_copy(parts[number], source_s * n_fs + source_o * 2 + (1 - i), k).wait_recv()
        block = n_fs * out_cols
        tile = min(256, owned)

        def weights(row):
            blocks = [wo_all[row, source_s * n_fs + n] for n in range(n_fs)]
            return jnp.concatenate(blocks, axis=1)

        def body(r, carry):
            here = pl.ds(pl.multiple_of(r * tile, tile), tile)
            where = pl.ds(pl.multiple_of(source_s * block, block), block)
            total = None if own else out[here, where].astype(F32)
            for k in (0,) if own else range(1, n_tp):
                g = lax.rem(t + n_tp - k, n_tp)
                if own:
                    mine = pl.ds(pl.multiple_of(t * owned + r * tile, tile), tile)
                    att, conv = m_att[mine, :], m_conv[mine, :]
                else:
                    att, conv = r_att[k - 1, here, :], r_conv[k - 1, here, :]
                partial = jnp.dot(att, weights(2 * g), preferred_element_type=F32)
                partial = partial + jnp.dot(conv, weights(2 * g + 1), preferred_element_type=F32)
                total = partial if own else total + partial.astype(BF16).astype(F32)
            out[here, where] = total.astype(BF16)
            return carry

        lax.fori_loop(0, owned // tile, body, 0)

    own_weights, own_out, own_tokens = local[:-3], local[-3:-1], local[-1]
    waited = set()

    def once(key, body):
        if key not in waited:
            waited.add(key)
            body()

    def wait_all(copies):
        for copy in copies:
            copy.wait()

    def wo_ready():
        for copy in wo_copies:
            copy.wait_recv()

    def job(kind, n, side):
        if kind == 0:
            make_bias()
        elif kind == 1:
            once("tokens", own_tokens.wait)
            for k in range(n_tp - 1):
                tok_copies[k, n].wait_recv()
            norm(n)
        elif kind == 2:
            once(("part", side), lambda: finish(side))
            project(side, [n])
            if n == chunks - 1 and side in (1, 4):
                halo_out(0 if side == 1 else 1)
        elif kind == 3:
            if n == 0:
                halo_in(0)
            attend(n)
        elif kind == 4:
            mix_out(0)
        elif kind == 5:
            halo_in(1)
            convolve()
            mix_out(1)
        elif kind == 6:
            mix_in()
        elif n == 0:
            project_out(s, kind == 7)
        elif side == 0:
            when(s - n >= 0, lambda: project_out(s - n, kind == 7))
        else:
            when(s + n < n_sp, lambda: project_out(s + n, kind == 7))

    wait_all(own_weights)
    tabled = (n_sp, n_out, n_tp) == TABLE_FOR
    if tabled:
        events = []

        def flush():
            for mine in range(n_sp):
                turn = [entry for entry in events if entry[5] == mine]

                def body(mine=mine, turn=turn):
                    for passing, number, k, distance, side, _ in turn:
                        part = parts[number]
                        at = mine - distance if side == 0 else mine + distance
                        if passing:
                            hand_over(part, source(k, at), False)
                            continue
                        if distance == 0 and k == 0 and number >= n_proj:
                            once(("own", mine), lambda: wait_all(own_out))
                            if not part.crossing:
                                once(("direct", mine), wo_ready)
                        handle(part, k, distance, side, at, False)

                if turn:
                    pl.when(s == mine)(body)
            events.clear()

        for entry in TABLE:
            if len(entry) == 6:
                events.append(entry)
            else:
                flush()
                job(*entry)
        flush()
    else:
        wait_all(own_out)
        wo_ready()

        def spread(part):
            deal(part, 0, 0, False)
            for n in range(1, n_sp + 1):
                if n < n_sp:
                    deal(part, n, 0, False)
                for k in range(1, n_out):
                    deal(part, n - 1, k, False)

        for part in parts[:n_proj]:
            spread(part)
        job(0, 0, 0)
        for n in order:
            job(1, n, 0)
            job(2, n, 0)
            job(2, n, 1)
        for n in range(chunks):
            job(3, n, 0)
        job(4, 0, 0)
        for number in (2, 3, 4):
            for n in order:
                job(2, n, number)
        job(5, 0, 0)
        for part in parts[n_proj:]:
            spread(part)
        for at in range(n_sp):
            for k in range(n_out):
                hand_over(parts[-1], source(k, at), False)
        job(6, 0, 0)
        for own in (True, False):
            lax.fori_loop(0, n_sp, lambda n, c, own=own: (project_out(n, own), c)[1], 0)

    if tabled:
        events = [entry for entry in TABLE if len(entry) == 6]
        for mine in range(n_sp):

            def drain(mine=mine):
                for passing, number, k, distance, side, _ in [entry for entry in events if entry[5] == mine]:
                    at = mine - distance if side == 0 else mine + distance
                    if passing:
                        hand_over(parts[number], source(k, at), True)
                    else:
                        handle(parts[number], k, distance, side, at, True)

            pl.when(s == mine)(drain)
    else:
        for part in parts:
            for k in range(n_out):
                for distance in range(n_sp):
                    deal(part, distance, k, True)
        for at in range(n_sp):
            for k in range(n_out):
                hand_over(parts[-1], source(k, at), True)
    for which in range(2):
        when(has_right, lambda which=which: halo_copy(which).wait_send())
        for k in range(n_tp - 1):
            mix_copy(which, k).wait_send()
    for copy in wo_copies + list(tok_copies.values()):
        copy.wait_send()


def on_device(tokens, norm_gain, w_query, w_key, w_value, w_conv_in, w_conv_b, w_conv_c,
              conv_taps, sink_logits, w_attn_out, w_conv_out):
    n_sp, n_fs, n_tp = (lax.axis_size(axis) for axis in ("sp", "fs", "tp"))
    n_out = n_fs // 2
    shards = n_sp * n_fs
    rows, cols = tokens.shape[1:]
    width = cols * n_tp
    q_cols, kv_cols, channels = w_query.shape[1], w_key.shape[1], w_conv_in.shape[1]
    out_rows, out_cols = w_attn_out.shape
    separate = kv_cols % 128 == 0
    weights = [w_query]
    weights += [w_key, w_value] if separate else [jnp.concatenate([w_key, w_value], axis=1)]
    weights += [w_conv_in, w_conv_b, w_conv_c]
    owned = rows // n_tp
    kinds = part_kinds(out_rows)
    lanes = sum(lanes_of(wide, n_out) for wide, _, _ in kinds)
    kv_here = kv_cols // HEAD
    group = q_cols // kv_cols
    dma = pltpu.SemaphoreType.DMA
    vmem, anywhere = pl.BlockSpec(memory_space=pltpu.VMEM), pl.BlockSpec(memory_space=pl.ANY)
    summed = pl.pallas_call(
        functools.partial(layer_kernel, (n_sp, n_out, n_tp, 5, separate)),
        out_shape=jax.ShapeDtypeStruct((owned, width), BF16),
        in_specs=[anywhere, vmem, vmem, pl.BlockSpec(memory_space=pltpu.SMEM)] + [anywhere] * (len(weights) + 2),
        out_specs=vmem,
        scratch_shapes=[
            pltpu.VMEM((rows, width), BF16),
            pltpu.VMEM((5, width, q_cols), BF16),
            pltpu.VMEM((2 * n_tp, shards, out_rows, out_cols), BF16),
            pltpu.VMEM((rows, q_cols), BF16),
            pltpu.VMEM((WINDOW + rows, 2 * kv_cols), BF16),
            pltpu.VMEM((rows, channels), BF16),
            pltpu.VMEM((rows, channels), BF16),
            pltpu.VMEM((HALO + rows, channels), BF16),
            pltpu.VMEM((rows, q_cols), BF16),
            pltpu.VMEM((rows, channels), BF16),
            pltpu.VMEM((n_tp - 1, owned, q_cols), BF16),
            pltpu.VMEM((n_tp - 1, owned, channels), BF16),
            pltpu.VMEM((kv_here, group * WINDOW, 2 * WINDOW), F32),
            dma((lanes * n_sp * 2,)),
            dma((len(kinds) * shards,)),
            dma((9,)),
            dma((n_tp - 1, 2)),
            dma((n_tp - 1, 2)),
            dma((n_tp - 1, 4)),
            dma((n_tp - 1, 4)),
            dma((2,)),
            dma((2,)),
            dma((2, n_tp - 1)),
            dma((2, n_tp - 1)),
            dma((n_tp - 1, shards)),
            dma((n_tp - 1, shards)),
            dma((n_tp - 1, shards)),
            dma((n_tp - 1, shards)),
        ],
        compiler_params=pltpu.CompilerParams(
            collective_id=0, has_side_effects=True, vmem_limit_bytes=60 * 1024 * 1024
        ),
    )(tokens[0], norm_gain[None], conv_taps, sink_logits, *weights, w_attn_out, w_conv_out)
    return summed[None]


def solution(mesh):
    placed = (
        P("fs", "sp", "tp"),
        P(),
        P(("sp", "fs"), "tp"),
        P(("sp", "fs"), "tp"),
        P(("sp", "fs"), "tp"),
        P(("sp", "fs"), "tp"),
        P(("sp", "fs"), "tp"),
        P(("sp", "fs"), "tp"),
        P(None, "tp"),
        P("tp"),
        P("tp", ("sp", "fs")),
        P("tp", ("sp", "fs")),
    )
    return jax.shard_map(
        on_device,
        mesh=mesh,
        in_specs=placed,
        out_specs=P("fs", ("sp", "tp"), None),
        check_vma=False,
    )
```

```python
import functools

import jax
import jax.numpy as jnp
from jax import lax
from jax.experimental import pallas as pl
from jax.experimental.pallas import tpu as pltpu
from jax.sharding import PartitionSpec as P

HEADS = 16
HEAD = 64
WINDOW = 128
HALO = 16
MESH = pl.DeviceIdType.MESH
DIRECT_AFTER = 0
WAYS = RIGHT, LEFT, ACROSS, CROSS, CORE, HAND = range(6)
BF16, F32 = jnp.bfloat16, jnp.float32


TABLE_FOR = (4, 2, 2)
TABLE = (
    (0, 0, 0, 0, 0, 0), (2, 0, 0, 0, 0, 0), (3, 8, 0, 0, 0, 0), (4, 0, 0, 0, 0, 0), (0, 1, 0, 0, 0, 0),
    (2, 1, 0, 0, 0, 0), (4, 1, 0, 0, 0, 0), (4, 2, 0, 0, 0, 0), (4, 3, 0, 0, 0, 0), (4, 4, 0, 0, 0, 0),
    (4, 8, 0, 0, 0, 0), (0, 2, 0, 0, 0, 0), (2, 2, 0, 0, 0, 0), (4, 0, 1, 0, 0, 0), (4, 0, 0, 1, 1, 0),
    (0, 3, 0, 0, 0, 0), (2, 0, 0, 1, 1, 0), (4, 7, 0, 0, 0, 0), (4, 6, 0, 0, 0, 0), (4, 5, 0, 0, 0, 0),
    (4, 1, 1, 0, 0, 0), (4, 1, 0, 1, 1, 0), (0, 1, 1, 0, 0, 0), (2, 3, 0, 0, 0, 0), (4, 2, 1, 0, 0, 0),
    (4, 2, 0, 1, 1, 0), (0, 4, 0, 0, 0, 0), (2, 2, 0, 1, 1, 0), (4, 0, 1, 1, 1, 0), (4, 0, 0, 2, 1, 0),
    (0, 7, 0, 0, 0, 0), (2, 0, 0, 2, 1, 0), (4, 1, 1, 1, 1, 0), (4, 3, 1, 0, 0, 0), (0, 8, 0, 0, 0, 0),
    (2, 4, 0, 0, 0, 0), (0, 0, 0, 0, 0, 1), (1, 0, 0, 0, 0, 1), (2, 0, 0, 0, 0, 1), (3, 8, 0, 0, 0, 1),
    (0, 1, 0, 0, 0, 1), (1, 1, 0, 0, 0, 1), (2, 1, 0, 0, 0, 1), (4, 0, 0, 0, 0, 1), (4, 1, 0, 0, 0, 1),
    (4, 2, 0, 0, 0, 1), (4, 3, 0, 0, 0, 1), (4, 4, 0, 0, 0, 1), (4, 8, 0, 0, 0, 1), (0, 2, 0, 0, 0, 1),
    (1, 2, 0, 0, 0, 1), (2, 2, 0, 0, 0, 1), (4, 0, 0, 1, 0, 1), (4, 0, 0, 1, 1, 1), (4, 0, 1, 0, 0, 1),
    (0, 0, 0, 1, 0, 1), (1, 0, 0, 1, 1, 1), (2, 0, 0, 1, 0, 1), (4, 7, 0, 0, 0, 1), (4, 6, 0, 0, 0, 1),
    (4, 5, 0, 0, 0, 1), (4, 1, 0, 1, 0, 1), (4, 1, 0, 1, 1, 1), (4, 1, 1, 0, 0, 1), (0, 1, 0, 1, 0, 1),
    (1, 1, 1, 0, 0, 1), (2, 0, 0, 1, 1, 1), (4, 2, 0, 1, 0, 1), (4, 2, 0, 1, 1, 1), (4, 2, 1, 0, 0, 1),
    (0, 1, 1, 0, 0, 1), (1, 1, 0, 1, 1, 1), (2, 2, 0, 1, 0, 1), (4, 3, 0, 1, 0, 1), (4, 0, 0, 2, 1, 1),
    (4, 0, 1, 1, 0, 1), (0, 2, 0, 1, 0, 1), (1, 0, 0, 2, 1, 1), (2, 0, 0, 2, 1, 1), (4, 1, 1, 1, 0, 1),
    (4, 1, 1, 1, 1, 1), (4, 0, 1, 1, 1, 1), (0, 1, 1, 1, 0, 1), (1, 1, 1, 1, 1, 1), (2, 2, 0, 1, 1, 1),
    (0, 0, 0, 0, 0, 2), (1, 0, 0, 0, 0, 2), (2, 0, 0, 0, 0, 2), (3, 8, 0, 0, 0, 2), (0, 1, 0, 0, 0, 2),
    (1, 1, 0, 0, 0, 2), (2, 1, 0, 0, 0, 2), (4, 0, 0, 0, 0, 2), (4, 1, 0, 0, 0, 2), (4, 2, 0, 0, 0, 2),
    (4, 3, 0, 0, 0, 2), (4, 4, 0, 0, 0, 2), (4, 8, 0, 0, 0, 2), (0, 2, 0, 0, 0, 2), (1, 2, 0, 0, 0, 2),
    (2, 2, 0, 0, 0, 2), (4, 0, 0, 1, 0, 2), (4, 0, 0, 1, 1, 2), (4, 0, 1, 0, 0, 2), (0, 0, 0, 1, 0, 2),
    (1, 0, 0, 1, 1, 2), (2, 0, 0, 1, 0, 2), (4, 7, 0, 0, 0, 2), (4, 6, 0, 0, 0, 2), (4, 5, 0, 0, 0, 2),
    (4, 1, 0, 1, 0, 2), (4, 1, 0, 1, 1, 2), (4, 1, 1, 0, 0, 2), (0, 1, 0, 1, 0, 2), (1, 1, 1, 0, 0, 2),
    (2, 0, 0, 1, 1, 2), (4, 2, 0, 1, 0, 2), (4, 2, 0, 1, 1, 2), (4, 2, 1, 0, 0, 2), (0, 1, 1, 0, 0, 2),
    (1, 1, 0, 1, 1, 2), (2, 2, 0, 1, 0, 2), (4, 0, 0, 2, 0, 2), (4, 3, 0, 1, 1, 2), (4, 0, 1, 1, 0, 2),
    (0, 0, 0, 2, 0, 2), (1, 2, 0, 1, 1, 2), (2, 0, 0, 2, 0, 2), (4, 1, 0, 2, 0, 2), (4, 1, 1, 1, 1, 2),
    (4, 0, 1, 1, 1, 2), (0, 1, 0, 2, 0, 2), (1, 1, 1, 1, 1, 2), (2, 2, 0, 1, 1, 2), (1, 0, 0, 0, 0, 3),
    (2, 0, 0, 0, 0, 3), (3, 8, 0, 0, 0, 3), (4, 0, 0, 0, 0, 3), (1, 1, 0, 0, 0, 3), (2, 1, 0, 0, 0, 3),
    (4, 1, 0, 0, 0, 3), (4, 2, 0, 0, 0, 3), (4, 3, 0, 0, 0, 3), (4, 4, 0, 0, 0, 3), (4, 8, 0, 0, 0, 3),
    (1, 2, 0, 0, 0, 3), (2, 2, 0, 0, 0, 3), (4, 0, 0, 1, 0, 3), (4, 0, 1, 0, 0, 3), (1, 3, 0, 0, 0, 3),
    (2, 0, 0, 1, 0, 3), (4, 7, 0, 0, 0, 3), (4, 6, 0, 0, 0, 3), (4, 5, 0, 0, 0, 3), (4, 1, 0, 1, 0, 3),
    (4, 1, 1, 0, 0, 3), (1, 1, 1, 0, 0, 3), (2, 3, 0, 0, 0, 3), (4, 2, 0, 1, 0, 3), (4, 2, 1, 0, 0, 3),
    (1, 4, 0, 0, 0, 3), (2, 2, 0, 1, 0, 3), (4, 0, 0, 2, 0, 3), (4, 0, 1, 1, 0, 3), (1, 7, 0, 0, 0, 3),
    (2, 0, 0, 2, 0, 3), (4, 1, 0, 2, 0, 3), (4, 3, 1, 0, 0, 3), (1, 8, 0, 0, 0, 3), (2, 4, 0, 0, 0, 3), (1, 3, 0),
    (0, 6, 0, 0, 0, 0), (4, 1, 0, 2, 1, 0), (4, 2, 1, 1, 1, 0), (4, 1, 0, 2, 1, 1), (4, 2, 1, 1, 0, 1),
    (4, 4, 0, 1, 0, 1), (4, 1, 1, 1, 0, 2), (4, 2, 1, 1, 0, 2), (4, 4, 0, 1, 1, 2), (1, 6, 0, 0, 0, 3),
    (4, 1, 1, 1, 0, 3), (4, 2, 1, 1, 0, 3), (0, 0, 0), (2, 7, 0, 0, 0, 0), (0, 5, 0, 0, 0, 0), (4, 0, 1, 2, 1, 0),
    (4, 0, 0, 3, 1, 0), (2, 0, 0, 3, 1, 0), (4, 1, 1, 2, 1, 0), (4, 4, 1, 0, 0, 0), (2, 8, 0, 0, 0, 0),
    (2, 6, 0, 0, 0, 0), (4, 1, 0, 3, 1, 0), (4, 7, 1, 0, 0, 0), (0, 3, 0, 1, 0, 1), (1, 1, 0, 2, 1, 1),
    (2, 3, 0, 1, 0, 1), (4, 7, 0, 1, 0, 1), (4, 2, 0, 2, 1, 1), (4, 0, 1, 2, 1, 1), (0, 4, 0, 1, 0, 1),
    (1, 2, 0, 2, 1, 1), (2, 2, 0, 2, 1, 1), (3, 8, 0, 1, 0, 1), (4, 8, 0, 1, 0, 1), (4, 1, 1, 2, 1, 1),
    (4, 2, 1, 1, 1, 1), (0, 3, 0, 0, 0, 1), (1, 1, 1, 2, 1, 1), (2, 4, 0, 1, 0, 1), (4, 6, 0, 1, 0, 1),
    (4, 3, 0, 2, 1, 1), (4, 3, 1, 1, 0, 1), (0, 4, 0, 0, 0, 1), (1, 2, 0, 1, 1, 1), (2, 3, 0, 2, 1, 1),
    (4, 5, 0, 1, 0, 1), (0, 1, 1, 1, 0, 2), (1, 3, 0, 1, 1, 2), (2, 3, 0, 1, 1, 2), (4, 2, 0, 2, 0, 2),
    (4, 7, 0, 1, 1, 2), (4, 0, 1, 2, 0, 2), (0, 2, 0, 2, 0, 2), (1, 4, 0, 1, 1, 2), (2, 2, 0, 2, 0, 2),
    (3, 8, 0, 1, 1, 2), (4, 8, 0, 1, 1, 2), (4, 1, 1, 2, 0, 2), (4, 2, 1, 1, 1, 2), (0, 1, 1, 2, 0, 2),
    (1, 3, 0, 0, 0, 2), (2, 4, 0, 1, 1, 2), (4, 6, 0, 1, 1, 2), (4, 3, 0, 2, 0, 2), (4, 3, 1, 1, 1, 2),
    (0, 2, 0, 1, 0, 2), (1, 4, 0, 0, 0, 2), (2, 3, 0, 2, 0, 2), (4, 5, 0, 1, 1, 2), (2, 7, 0, 0, 0, 3),
    (1, 5, 0, 0, 0, 3), (4, 0, 0, 3, 0, 3), (4, 0, 1, 2, 0, 3), (2, 0, 0, 3, 0, 3), (4, 1, 0, 3, 0, 3),
    (4, 4, 1, 0, 0, 3), (2, 8, 0, 0, 0, 3), (2, 6, 0, 0, 0, 3), (4, 1, 1, 2, 0, 3), (4, 7, 1, 0, 0, 3), (1, 0, 0),
    (2, 2, 0, 3, 1, 0), (4, 0, 1, 3, 1, 0), (4, 2, 0, 3, 1, 0), (0, 8, 1, 0, 0, 0), (3, 8, 1, 0, 0, 0),
    (4, 8, 1, 0, 0, 0), (2, 5, 0, 0, 0, 0), (4, 1, 1, 3, 1, 0), (4, 6, 1, 0, 0, 0), (2, 2, 0, 2, 1, 0),
    (4, 2, 0, 2, 1, 0), (4, 2, 1, 3, 1, 0), (2, 3, 0, 3, 1, 0), (4, 3, 0, 3, 1, 0), (4, 2, 1, 2, 1, 1),
    (4, 4, 0, 2, 1, 1), (0, 7, 0, 1, 0, 1), (1, 3, 0, 2, 1, 1), (2, 4, 0, 2, 1, 1), (4, 3, 0, 1, 1, 1),
    (4, 4, 1, 1, 0, 1), (0, 8, 0, 1, 0, 1), (1, 4, 0, 2, 1, 1), (2, 3, 0, 1, 1, 1), (3, 8, 1, 1, 0, 1),
    (4, 8, 1, 1, 0, 1), (0, 8, 1, 1, 0, 1), (4, 4, 0, 1, 1, 1), (4, 3, 1, 2, 1, 1), (0, 6, 0, 1, 0, 1),
    (1, 3, 0, 1, 1, 1), (2, 4, 0, 1, 1, 1), (4, 7, 0, 2, 1, 1), (4, 4, 1, 2, 1, 1), (0, 5, 0, 1, 0, 1),
    (1, 4, 0, 1, 1, 1), (2, 3, 0, 0, 0, 1), (4, 2, 1, 2, 0, 2), (4, 4, 0, 2, 0, 2), (0, 3, 0, 2, 0, 2),
    (1, 7, 0, 1, 1, 2), (2, 4, 0, 2, 0, 2), (4, 3, 0, 1, 0, 2), (4, 4, 1, 1, 1, 2), (0, 4, 0, 2, 0, 2),
    (1, 8, 0, 1, 1, 2), (2, 3, 0, 1, 0, 2), (3, 8, 1, 1, 1, 2), (4, 8, 1, 1, 1, 2), (1, 8, 1, 1, 1, 2),
    (4, 4, 0, 1, 0, 2), (4, 3, 1, 2, 0, 2), (0, 3, 0, 1, 0, 2), (1, 6, 0, 1, 1, 2), (2, 4, 0, 1, 0, 2),
    (4, 7, 0, 2, 0, 2), (4, 4, 1, 2, 0, 2), (0, 4, 0, 1, 0, 2), (1, 5, 0, 1, 1, 2), (2, 3, 0, 0, 0, 2),
    (3, 8, 0, 2, 0, 2), (4, 8, 0, 2, 0, 2), (2, 2, 0, 3, 0, 3), (4, 0, 1, 3, 0, 3), (4, 2, 0, 3, 0, 3),
    (1, 8, 1, 0, 0, 3), (3, 8, 1, 0, 0, 3), (4, 8, 1, 0, 0, 3), (2, 5, 0, 0, 0, 3), (4, 1, 1, 3, 0, 3),
    (4, 6, 1, 0, 0, 3), (2, 2, 0, 2, 0, 3), (4, 2, 0, 2, 0, 3), (4, 2, 1, 3, 0, 3), (2, 3, 0, 3, 0, 3),
    (4, 3, 0, 3, 0, 3), (1, 1, 0), (2, 4, 0, 3, 1, 0), (4, 4, 0, 3, 1, 0), (4, 5, 1, 0, 0, 0), (3, 8, 1, 2, 1, 1),
    (3, 8, 0, 2, 1, 1), (4, 3, 1, 1, 1, 1), (4, 8, 1, 2, 1, 1), (4, 8, 0, 2, 1, 1), (3, 8, 1, 2, 0, 2),
    (4, 3, 1, 1, 0, 2), (4, 8, 1, 2, 0, 2), (2, 4, 0, 3, 0, 3), (4, 4, 0, 3, 0, 3), (4, 5, 1, 0, 0, 3), (2, 1, 1),
    (0, 7, 0, 0, 0, 1), (1, 3, 0, 0, 0, 1), (2, 4, 0, 0, 0, 1), (0, 3, 0, 0, 0, 2), (1, 7, 0, 0, 0, 2),
    (2, 4, 0, 0, 0, 2), (2, 1, 0), (4, 2, 1, 2, 1, 0), (4, 2, 1, 2, 0, 3), (2, 3, 1), (2, 3, 0, 2, 1, 0),
    (4, 3, 0, 2, 1, 0), (4, 4, 1, 1, 1, 1), (4, 6, 0, 2, 1, 1), (4, 4, 1, 1, 0, 2), (4, 6, 0, 2, 0, 2),
    (2, 3, 0, 2, 0, 3), (4, 3, 0, 2, 0, 3), (2, 0, 1), (2, 0, 0), (4, 3, 1, 3, 1, 0), (1, 4, 0, 0, 0, 1),
    (2, 7, 0, 2, 1, 1), (1, 8, 0, 0, 0, 2), (2, 7, 0, 2, 0, 2), (4, 3, 1, 3, 0, 3), (2, 3, 2), (1, 6, 0, 0, 0, 2),
    (2, 3, 0), (2, 4, 0, 2, 1, 0), (4, 4, 0, 2, 1, 0), (4, 3, 1, 0, 0, 1), (4, 5, 0, 2, 1, 1), (4, 3, 1, 0, 0, 2),
    (4, 5, 0, 2, 0, 2), (2, 4, 0, 2, 0, 3), (4, 4, 0, 2, 0, 3), (3, 1, 0), (2, 3, 0, 1, 1, 0), (4, 4, 1, 3, 1, 0),
    (4, 3, 0, 1, 1, 0), (0, 8, 0, 0, 0, 1), (0, 6, 0, 0, 0, 1), (1, 8, 1, 2, 1, 1), (1, 7, 0, 2, 1, 1),
    (2, 6, 0, 2, 1, 1), (4, 4, 1, 0, 0, 1), (4, 7, 0, 1, 1, 1), (0, 4, 0, 0, 0, 2), (1, 5, 0, 0, 0, 2),
    (2, 6, 0, 2, 0, 2), (4, 4, 1, 0, 0, 2), (4, 7, 0, 1, 0, 2), (2, 3, 0, 1, 0, 3), (4, 4, 1, 3, 0, 3),
    (4, 3, 0, 1, 0, 3), (2, 0, 2), (2, 5, 0, 2, 1, 1), (3, 8, 0, 1, 1, 1), (4, 8, 0, 1, 1, 1), (0, 8, 1, 2, 0, 2),
    (2, 5, 0, 2, 0, 2), (1, 2, 0), (2, 4, 0, 1, 1, 0), (4, 3, 1, 2, 1, 0), (4, 4, 0, 1, 1, 0), (0, 5, 0, 0, 0, 1),
    (1, 8, 0, 2, 1, 1), (4, 7, 1, 2, 1, 1), (0, 7, 0, 2, 0, 2), (4, 7, 1, 2, 0, 2), (4, 3, 1, 2, 0, 3), (2, 2, 1),
    (1, 6, 0, 2, 1, 1), (2, 7, 0, 1, 0, 1), (4, 6, 0, 1, 1, 1), (2, 7, 0, 1, 0, 2), (3, 8, 0, 1, 0, 2),
    (4, 8, 0, 1, 0, 2), (2, 2, 2), (3, 8, 1, 3, 1, 0), (4, 4, 1, 2, 1, 0), (4, 8, 1, 3, 1, 0), (4, 4, 1, 2, 0, 3),
    (2, 2, 0), (4, 6, 1, 2, 1, 1), (0, 8, 0, 2, 0, 2), (4, 6, 1, 2, 0, 2), (3, 2, 0), (2, 7, 0, 3, 1, 0),
    (3, 8, 0, 3, 1, 0), (4, 3, 1, 1, 1, 0), (4, 7, 0, 3, 1, 0), (4, 8, 0, 3, 1, 0), (1, 5, 0, 2, 1, 1),
    (2, 7, 0, 1, 1, 1), (4, 5, 1, 2, 1, 1), (4, 5, 0, 1, 1, 1), (0, 6, 0, 2, 0, 2), (2, 7, 0, 1, 1, 2),
    (4, 5, 1, 2, 0, 2), (4, 6, 0, 1, 0, 2), (2, 4, 0, 1, 0, 3), (3, 8, 1, 3, 0, 3), (4, 3, 1, 1, 0, 3),
    (4, 4, 0, 1, 0, 3), (4, 8, 1, 3, 0, 3), (3, 0, 0), (2, 6, 0, 3, 1, 0), (4, 4, 1, 1, 1, 0), (4, 6, 0, 3, 1, 0),
    (1, 7, 0, 1, 1, 1), (2, 6, 0, 1, 0, 1), (4, 7, 1, 1, 0, 1), (0, 5, 0, 2, 0, 2), (2, 6, 0, 1, 0, 2),
    (4, 7, 1, 1, 0, 2), (4, 5, 0, 1, 0, 2), (2, 7, 0, 3, 0, 3), (3, 8, 0, 3, 0, 3), (4, 7, 0, 3, 0, 3),
    (4, 8, 0, 3, 0, 3), (3, 3, 0), (2, 5, 0, 3, 1, 0), (4, 7, 1, 3, 1, 0), (4, 5, 0, 3, 1, 0), (1, 8, 0, 1, 1, 1),
    (1, 6, 0, 1, 1, 1), (2, 6, 0, 1, 1, 1), (4, 7, 1, 1, 1, 1), (0, 7, 0, 1, 0, 2), (2, 6, 0, 1, 1, 2),
    (4, 7, 1, 1, 1, 2), (2, 6, 0, 3, 0, 3), (4, 4, 1, 1, 0, 3), (4, 6, 0, 3, 0, 3), (4, 0, 0), (2, 3, 4),
    (2, 5, 0, 1, 0, 1), (0, 8, 0, 1, 0, 2), (2, 5, 0, 1, 0, 2), (4, 7, 1, 3, 0, 3), (2, 3, 3), (2, 5, 0, 3, 0, 3),
    (4, 5, 0, 3, 0, 3), (2, 1, 3), (4, 6, 1, 3, 1, 0), (1, 5, 0, 1, 1, 1), (4, 6, 1, 1, 0, 1), (0, 6, 0, 1, 0, 2),
    (4, 6, 1, 1, 0, 2), (2, 2, 3), (2, 7, 0, 2, 1, 0), (4, 7, 0, 2, 1, 0), (2, 5, 0, 1, 1, 1), (2, 5, 0, 1, 1, 2),
    (2, 1, 2), (3, 8, 0, 2, 1, 0), (4, 8, 0, 2, 1, 0), (4, 6, 1, 3, 0, 3), (2, 1, 4), (1, 7, 0, 0, 0, 1),
    (2, 7, 0, 2, 0, 3), (4, 7, 0, 2, 0, 3), (2, 0, 3), (4, 5, 1, 3, 1, 0), (4, 6, 1, 1, 1, 1), (0, 5, 0, 1, 0, 2),
    (4, 6, 1, 1, 1, 2), (2, 2, 4), (2, 7, 0, 0, 0, 1), (2, 7, 0, 0, 0, 2), (3, 8, 0, 2, 0, 3), (4, 8, 0, 2, 0, 3),
    (2, 0, 4), (2, 6, 0, 2, 1, 0), (4, 6, 0, 2, 1, 0), (4, 5, 1, 3, 0, 3), (5, 0, 0), (4, 7, 1, 2, 1, 0),
    (1, 8, 0, 0, 0, 1), (4, 5, 1, 1, 0, 1), (0, 7, 0, 0, 0, 2), (4, 5, 1, 1, 0, 2), (7, 3, 0), (1, 6, 0, 0, 0, 1),
    (2, 8, 0, 0, 0, 1), (2, 6, 0, 0, 0, 1), (4, 5, 1, 1, 1, 1), (1, 5, 0, 0, 0, 1), (2, 5, 0, 0, 0, 1),
    (4, 7, 1, 0, 0, 1), (0, 8, 1, 0, 0, 1), (1, 8, 1, 0, 0, 1), (3, 8, 1, 0, 0, 1), (4, 8, 1, 0, 0, 1),
    (4, 6, 1, 0, 0, 1), (1, 8, 1, 1, 1, 1), (3, 8, 1, 1, 1, 1), (4, 8, 1, 1, 1, 1), (4, 5, 1, 0, 0, 1),
    (2, 8, 0, 0, 0, 2), (2, 6, 0, 0, 0, 2), (0, 8, 0, 0, 0, 2), (4, 5, 1, 1, 1, 2), (0, 6, 0, 0, 0, 2),
    (2, 5, 0, 0, 0, 2), (4, 7, 1, 0, 0, 2), (0, 5, 0, 0, 0, 2), (1, 8, 1, 0, 0, 2), (3, 8, 1, 0, 0, 2),
    (4, 8, 1, 0, 0, 2), (0, 8, 1, 0, 0, 2), (4, 6, 1, 0, 0, 2), (3, 8, 1, 1, 0, 2), (4, 8, 1, 1, 0, 2),
    (0, 8, 1, 1, 0, 2), (4, 5, 1, 0, 0, 2), (2, 6, 0, 2, 0, 3), (4, 7, 1, 2, 0, 3), (4, 6, 0, 2, 0, 3), (7, 0, 0),
    (2, 5, 0, 2, 1, 0), (4, 5, 0, 2, 1, 0), (2, 5, 0, 2, 0, 3), (4, 5, 0, 2, 0, 3), (4, 6, 1, 2, 0, 3),
    (2, 7, 0, 1, 0, 3), (4, 7, 0, 1, 0, 3), (3, 8, 0, 1, 0, 3), (4, 8, 0, 1, 0, 3), (4, 5, 1, 2, 0, 3),
    (2, 6, 0, 1, 0, 3), (4, 6, 0, 1, 0, 3), (4, 7, 1, 1, 0, 3), (2, 5, 0, 1, 0, 3), (4, 5, 0, 1, 0, 3),
    (3, 8, 1, 1, 0, 3), (4, 8, 1, 1, 0, 3), (5, 8, 0, 0, 0, 3), (5, 8, 1, 0, 0, 3), (5, 8, 1, 3, 0, 3),
    (5, 8, 0, 3, 0, 3), (5, 8, 0, 2, 0, 3), (4, 6, 1, 1, 0, 3), (3, 8, 1, 2, 0, 3), (4, 8, 1, 2, 0, 3), (7, 2, 0),
    (4, 6, 1, 2, 1, 0), (2, 7, 0, 1, 1, 0), (4, 7, 0, 1, 1, 0), (3, 8, 0, 1, 1, 0), (4, 8, 0, 1, 1, 0),
    (4, 5, 1, 2, 1, 0), (2, 6, 0, 1, 1, 0), (4, 6, 0, 1, 1, 0), (4, 7, 1, 1, 1, 0), (2, 5, 0, 1, 1, 0),
    (4, 5, 0, 1, 1, 0), (3, 8, 1, 1, 1, 0), (4, 8, 1, 1, 1, 0), (4, 6, 1, 1, 1, 0), (3, 8, 1, 2, 1, 0),
    (4, 8, 1, 2, 1, 0), (5, 8, 0, 0, 0, 0), (4, 5, 1, 1, 1, 0), (5, 8, 1, 0, 0, 0), (5, 8, 1, 3, 1, 0),
    (5, 8, 0, 3, 1, 0), (5, 8, 0, 2, 1, 0), (5, 8, 0, 0, 0, 1), (5, 8, 0, 1, 0, 1), (5, 8, 1, 1, 0, 1),
    (5, 8, 1, 2, 1, 1), (5, 8, 0, 2, 1, 1), (5, 8, 0, 1, 1, 1), (5, 8, 0, 0, 0, 2), (5, 8, 0, 1, 1, 2),
    (5, 8, 1, 1, 1, 2), (5, 8, 0, 2, 0, 2), (5, 8, 1, 2, 0, 2), (5, 8, 0, 1, 0, 2), (4, 5, 1, 1, 0, 3),
    (5, 8, 0, 1, 0, 3), (6, 0, 0), (7, 3, 1), (7, 2, 1), (5, 8, 0, 1, 1, 0), (7, 1, 1), (5, 8, 1, 1, 1, 0),
    (5, 8, 1, 0, 0, 1), (5, 8, 1, 1, 1, 1), (5, 8, 1, 0, 0, 2), (8, 0, 0), (5, 8, 1, 1, 0, 2), (8, 1, 1),
    (5, 8, 1, 2, 1, 0), (8, 3, 1), (5, 8, 1, 1, 0, 3), (7, 1, 0), (8, 1, 0), (5, 8, 1, 2, 0, 3), (8, 3, 0), (8, 2, 1),
    (8, 2, 0),
)


def when(condition, body):
    if condition is True:
        body()
    elif condition is not False:
        pl.when(condition)(body)


class Part:
    def __init__(self, number, wide, crossing, place, base):
        self.number, self.wide, self.crossing, self.place, self.base = number, wide, crossing, place, base


def part_kinds(out_rows):
    kinds = [(False, False, None), (True, False, None)] + [(False, False, None)] * 3
    quarter = out_rows // 4
    kinds += [(False, False, (n * quarter, quarter)) for n in range(3)]
    return kinds + [(True, True, (3 * quarter, quarter))]


def lanes_of(wide, n_out):
    return 1 + n_out + (2 if wide else 1) * (n_out - 1)


def layer_kernel(sizes, *refs):
    n_sp, n_out, n_tp, n_proj, separate = sizes
    tok, gain, taps, sinks = refs[:4]
    n_in = 6 if separate else 5
    w_own = refs[4 : 4 + n_in]
    out_own = refs[4 + n_in : 6 + n_in]
    out = refs[6 + n_in]
    (tokf, w_all, wo_all, q_buf, kv_buf, inner, gate_b, product, m_att, m_conv, r_att, r_conv, bias,
     send_sem, recv_sem, own_sem, wo_send, wo_recv, tok_send, tok_recv, halo_send, halo_recv,
     mix_send, mix_recv, cross_send, cross_recv, pass_send, pass_recv) = refs[7 + n_in :]
    n_fs = 2 * n_out
    shards = n_sp * n_fs
    s, f, t = lax.axis_index("sp"), lax.axis_index("fs"), lax.axis_index("tp")
    o, i = f // 2, f % 2
    rows_total, width = tokf.shape
    cols = tok.shape[1]
    q_cols = q_buf.shape[1]
    kv_cols = kv_buf.shape[1] // 2
    k_rows = w_own[0].shape[0]
    out_rows, out_cols = out_own[0].shape
    owned = rows_total // n_tp
    chunks = 4
    step = rows_total // chunks
    order = [chunks - 1] + list(range(chunks - 1))
    me = s * n_fs + f

    right, left, core = (s + 1, f, t), (s - 1, f, t), (s, o * 2 + (1 - i), t)
    across = [(s, lax.rem(o + k, n_out) * 2 + i, t) for k in range(1, n_out)]
    peers = [(s, f, lax.rem(t + k, n_tp)) for k in range(1, n_tp)]
    has_right, has_left = s < n_sp - 1, s > 0

    local = []
    spots = [(0, 0), (1, 0), (1, kv_cols), (2, 0), (3, 0), (4, 0)] if separate else [(n, 0) for n in range(5)]
    for n, (number, col) in enumerate(spots):
        place = w_all.at[number, pl.ds(me * k_rows, k_rows), pl.ds(col, w_own[n].shape[1])]
        local.append(pltpu.make_async_copy(w_own[n], place, own_sem.at[n]))
    for a in range(2):
        local.append(pltpu.make_async_copy(out_own[a], wo_all.at[2 * t + a, me], own_sem.at[6 + a]))
    my_cols = pl.ds(pl.multiple_of(t * cols, cols), cols)
    local.append(pltpu.make_async_copy(tok, tokf.at[:, my_cols], own_sem.at[8]))
    for copy in local:
        copy.start()

    barrier = pltpu.get_barrier_semaphore()
    greet = lambda where: pl.semaphore_signal(barrier, inc=1, device_id=where, device_id_type=MESH)
    when(has_right, lambda: greet(right))
    when(has_left, lambda: greet(left))
    for where in across + [core] + peers:
        greet(where)
    count = len(across) + 1 + len(peers)
    pl.semaphore_wait(barrier, count + has_right.astype(jnp.int32) + has_left.astype(jnp.int32))

    wo_copies, tok_copies = [], {}
    direct = pl.ds(0, 3 * (out_rows // 4))
    def send_direct():
        for k, peer in enumerate(peers):
            for a in range(2):
                copy = pltpu.make_async_remote_copy(
                    src_ref=out_own[a].at[direct], dst_ref=wo_all.at[2 * t + a, me, direct],
                    send_sem=wo_send.at[k, a], recv_sem=wo_recv.at[k, a], device_id=peer, device_id_type=MESH,
                )
                copy.start()
                wo_copies.append(copy)

    for turn, n in enumerate(order):
        if turn == DIRECT_AFTER:
            send_direct()
        here = pl.ds(n * step, step)
        for k, peer in enumerate(peers):
            copy = pltpu.make_async_remote_copy(
                src_ref=tok.at[here], dst_ref=tokf.at[here, my_cols],
                send_sem=tok_send.at[k, n], recv_sem=tok_recv.at[k, n], device_id=peer, device_id_type=MESH,
            )
            copy.start()
            tok_copies[k, n] = copy

    parts, base = [], 0
    for number, (wide, crossing, rows) in enumerate(part_kinds(out_rows)):
        if rows is None:
            place = lambda src, g, number=number: w_all.at[number, pl.ds(src * k_rows, k_rows)]
        elif crossing:
            place = lambda src, g, rows=rows: wo_all.at[pl.ds(2 * g, 2), src, pl.ds(*rows)]
        else:
            place = lambda src, g, rows=rows: wo_all.at[:, src, pl.ds(*rows)]
        parts.append(Part(number, wide, crossing, place, base))
        base += lanes_of(wide, n_out) * n_sp * 2

    def copy_of(part, src, where, lane, distance, side):
        spot = part.place(src, t)
        return pltpu.make_async_remote_copy(
            src_ref=spot, dst_ref=spot,
            send_sem=send_sem.at[part.base + (lane * n_sp + distance) * 2 + side],
            recv_sem=recv_sem.at[part.number * shards + src],
            device_id=where, device_id_type=MESH,
        )

    def cross_copy(part, src, k):
        spot = part.place(src, t)
        return pltpu.make_async_remote_copy(
            src_ref=spot, dst_ref=spot, send_sem=cross_send.at[k, src], recv_sem=cross_recv.at[k, src],
            device_id=peers[k], device_id_type=MESH,
        )

    def pass_copy(part, src, k):
        spot = part.place(src, lax.rem(t + n_tp - k - 1, n_tp))
        return pltpu.make_async_remote_copy(
            src_ref=spot, dst_ref=spot, send_sem=pass_send.at[k, src], recv_sem=pass_recv.at[k, src],
            device_id=core, device_id_type=MESH,
        )

    def source(k, at):
        return at * n_fs + lax.rem(o + n_out - k, n_out) * 2 + i

    def handle(part, k, distance, side, at, drain, ways=WAYS, arrival=True):
        first = isinstance(distance, int) and distance == 0
        src = source(k, at)
        mine = (at + distance if side == 0 else at - distance) if isinstance(at, int) else s
        more_right, more_left = mine < n_sp - 1, mine > 0
        lane_z, lane_core = 0, 1
        if k > 0:
            lane_z = 2 + len(across) + 2 * (k - 1)
            lane_core = lane_z + 1
            if not part.wide:
                lane_core = 2 + len(across) + k - 1

        def go(where, lane, way):
            copy = copy_of(part, src, where, lane, distance, way)
            copy.wait_send() if drain else copy.start()

        if arrival and not (first and k == 0) and not drain:
            copy_of(part, src, core, 0, 0, 0).wait_recv()
        if k == 0 or part.wide:
            if RIGHT in ways and (first or side == 0):
                when(more_right, lambda: go(right, lane_z, 0))
            if LEFT in ways and (first or side == 1):
                when(more_left, lambda: go(left, lane_z, 1))
        if ACROSS in ways and k == 0 and (first or not part.wide):
            for n, where in enumerate(across):
                go(where, 2 + n, side)
        if CROSS in ways and part.crossing:
            for n in range(len(peers)):
                copy = cross_copy(part, src, n)
                copy.wait_send() if drain else copy.start()
        if CORE in ways:
            go(core, lane_core, side)

    def hand_over(part, src, drain):
        for k in range(len(peers)):
            if not drain:
                cross_copy(part, src, k).wait_recv()
            copy = pass_copy(part, src, k)
            copy.wait_send() if drain else copy.start()

    def deal(part, distance, k, drain):
        if isinstance(distance, int) and distance == 0:
            handle(part, k, 0, 0, s, drain)
            return
        when(s - distance >= 0, lambda: handle(part, k, distance, 0, s - distance, drain))
        when(s + distance < n_sp, lambda: handle(part, k, distance, 1, s + distance, drain))

    def partner(number, source_s):
        for source_o in range(n_out):
            copy_of(parts[number], source_s * n_fs + source_o * 2 + (1 - i), core, 0, 0, 0).wait_recv()

    def finish(number):
        for source_s in range(n_sp):
            partner(number, source_s)

    def norm(n):
        size = 32

        def body(r, carry):
            here = pl.ds(pl.multiple_of(n * step + r * size, size), size)
            values = tokf[here, :].astype(F32)
            centred = values - jnp.sum(values, axis=1, keepdims=True) * (1.0 / width)
            variance = jnp.sum(centred * centred, axis=1, keepdims=True) * (1.0 / width)
            tokf[here, :] = (centred * lax.rsqrt(variance + 1e-05) * gain[...]).astype(BF16)
            return carry

        lax.fori_loop(0, step // size, body, 0)

    def project(number, ns):
        def body(m, carry):
            n = m if len(ns) == chunks else ns[0] + m
            first = n * step if isinstance(n, int) else pl.multiple_of(n * step, step)
            here = pl.ds(first, step)
            result = jnp.dot(tokf[here, :], w_all[number], preferred_element_type=F32).astype(BF16)
            if number == 0:
                q_buf[here, :] = result
            elif number == 1:
                kv_buf[pl.ds(first + WINDOW, step), :] = result
            elif number == 2:
                inner[here, :] = result
            elif number == 3:
                gate_b[here, :] = result
            else:
                made = result.astype(F32) * inner[here, :].astype(F32)
                product[pl.ds(first + HALO, step), :] = made.astype(BF16)
            return carry

        if len(ns) == 1:
            body(0, 0)
        else:
            lax.fori_loop(0, len(ns), body, 0)

    def halo_copy(which):
        buffer, size = ((kv_buf, WINDOW), (product, HALO))[which]
        return pltpu.make_async_remote_copy(
            src_ref=buffer.at[pl.ds(rows_total, size)], dst_ref=buffer.at[pl.ds(0, size)],
            send_sem=halo_send.at[which], recv_sem=halo_recv.at[which], device_id=right, device_id_type=MESH,
        )

    def halo_out(which):
        when(has_right, lambda: halo_copy(which).start())

        def clear():
            buffer, size = ((kv_buf, WINDOW), (product, HALO))[which]
            buffer[0:size, :] = jnp.zeros((size, buffer.shape[1]), BF16)

        when(s == 0, clear)

    def halo_in(which):
        when(has_left, lambda: halo_copy(which).wait_recv())

    heads_here = q_cols // HEAD
    kv_here = kv_cols // HEAD
    group = heads_here // kv_here
    tall = group * WINDOW

    def make_bias():
        row = lax.broadcasted_iota(jnp.int32, (tall, 2 * WINDOW), 0)
        col = lax.broadcasted_iota(jnp.int32, (tall, 2 * WINDOW), 1)
        distance = WINDOW + row % WINDOW - col
        keep = (distance >= 0) & (distance < WINDOW)
        for h in range(kv_here):
            head = (t * heads_here + h * group + row // WINDOW + 1).astype(F32)
            slope = jnp.exp2(head * (-8.0 / HEADS))
            bias[h] = jnp.where(keep, -(slope * distance.astype(F32)), -jnp.inf)

    def attend(n):
        row = lax.broadcasted_iota(jnp.int32, (tall, 1), 0) // WINDOW
        col = lax.broadcasted_iota(jnp.int32, (1, 2 * WINDOW), 1)

        def body(b, carry):
            block = n * (step // WINDOW) + b
            first = pl.multiple_of(block * WINDOW, WINDOW)
            before = jnp.where(col >= WINDOW, 0.0, jnp.where((s == 0) & (block == 0), -jnp.inf, 0.0))
            queries = q_buf[pl.ds(first, WINDOW), :]
            band = kv_buf[pl.ds(first, 2 * WINDOW), :]
            outs = []
            for h in range(kv_here):
                query = jnp.concatenate(
                    [queries[:, (h * group + g) * HEAD : (h * group + g + 1) * HEAD] for g in range(group)], axis=0
                )
                key = band[:, h * HEAD : (h + 1) * HEAD]
                value = band[:, kv_cols + h * HEAD : kv_cols + (h + 1) * HEAD]
                scores = lax.dot_general(query, key, (((1,), (1,)), ((), ())), preferred_element_type=F32)
                scores = scores * HEAD ** (-0.5) + bias[h] + before
                sink = jnp.full((tall, 1), sinks[h * group], F32)
                for g in range(1, group):
                    sink = jnp.where(row == g, sinks[h * group + g], sink)
                top = jnp.maximum(jnp.max(scores, axis=1, keepdims=True), sink)
                raised = jnp.exp(scores - top)
                total = jnp.sum(raised, axis=1, keepdims=True) + jnp.exp(sink - top)
                weights = (raised * (1.0 / total)).astype(BF16)
                mixed = jnp.dot(weights, value, preferred_element_type=F32).astype(BF16)
                outs += [mixed[g * WINDOW : (g + 1) * WINDOW] for g in range(group)]
            m_att[pl.ds(first, WINDOW), :] = jnp.concatenate(outs, axis=1)
            return carry

        lax.fori_loop(0, step // WINDOW, body, 0)

    def convolve():
        size = 64

        def body(r, carry):
            first = pl.multiple_of(r * size, size)
            padded = product[pl.ds(first, size + HALO), :].astype(F32)
            tap = taps[...].astype(F32)
            filtered = (
                tap[0:1] * padded[HALO - 2 : HALO - 2 + size]
                + tap[1:2] * padded[HALO - 1 : HALO - 1 + size]
                + tap[2:3] * padded[HALO : HALO + size]
            )
            m_conv[pl.ds(first, size), :] = (gate_b[pl.ds(first, size), :].astype(F32) * filtered).astype(BF16)
            return carry

        lax.fori_loop(0, rows_total // size, body, 0)

    def mix_copy(which, k):
        source, target = ((m_att, r_att), (m_conv, r_conv))[which]
        return pltpu.make_async_remote_copy(
            src_ref=source.at[pl.ds(pl.multiple_of(peers[k][2] * owned, owned), owned)], dst_ref=target.at[k],
            send_sem=mix_send.at[which, k], recv_sem=mix_recv.at[which, k],
            device_id=peers[k], device_id_type=MESH,
        )

    def mix_out(which):
        for k in range(n_tp - 1):
            mix_copy(which, k).start()

    def mix_in():
        for which in range(2):
            for k in range(n_tp - 1):
                mix_copy(which, k).wait_recv()

    def project_out(source_s, own):
        for number in range(n_proj, len(parts)):
            if own:
                partner(number, source_s)
            elif parts[number].crossing:
                for source_o in range(n_out):
                    for k in range(n_tp - 1):
                        pass_copy(parts[number], source_s * n_fs + source_o * 2 + (1 - i), k).wait_recv()
        block = n_fs * out_cols
        tile = min(256, owned)

        def weights(row):
            blocks = [wo_all[row, source_s * n_fs + n] for n in range(n_fs)]
            return jnp.concatenate(blocks, axis=1)

        def body(r, carry):
            here = pl.ds(pl.multiple_of(r * tile, tile), tile)
            where = pl.ds(pl.multiple_of(source_s * block, block), block)
            total = None if own else out[here, where].astype(F32)
            for k in (0,) if own else range(1, n_tp):
                g = lax.rem(t + n_tp - k, n_tp)
                if own:
                    mine = pl.ds(pl.multiple_of(t * owned + r * tile, tile), tile)
                    att, conv = m_att[mine, :], m_conv[mine, :]
                else:
                    att, conv = r_att[k - 1, here, :], r_conv[k - 1, here, :]
                partial = jnp.dot(att, weights(2 * g), preferred_element_type=F32)
                partial = partial + jnp.dot(conv, weights(2 * g + 1), preferred_element_type=F32)
                total = partial if own else total + partial.astype(BF16).astype(F32)
            out[here, where] = total.astype(BF16)
            return carry

        lax.fori_loop(0, owned // tile, body, 0)

    own_weights, own_out, own_tokens = local[:-3], local[-3:-1], local[-1]
    waited = set()

    def once(key, body):
        if key not in waited:
            waited.add(key)
            body()

    def wait_all(copies):
        for copy in copies:
            copy.wait()

    def wo_ready():
        for copy in wo_copies:
            copy.wait_recv()

    def job(kind, n, side):
        if kind == 0:
            make_bias()
        elif kind == 1:
            once("tokens", own_tokens.wait)
            for k in range(n_tp - 1):
                tok_copies[k, n].wait_recv()
            norm(n)
        elif kind == 2:
            once(("part", side), lambda: finish(side))
            project(side, [n])
            if n == chunks - 1 and side in (1, 4):
                halo_out(0 if side == 1 else 1)
        elif kind == 3:
            if n == 0:
                halo_in(0)
            attend(n)
        elif kind == 4:
            mix_out(0)
        elif kind == 5:
            halo_in(1)
            convolve()
            mix_out(1)
        elif kind == 6:
            mix_in()
        elif n == 0:
            project_out(s, kind == 7)
        elif side == 0:
            when(s - n >= 0, lambda: project_out(s - n, kind == 7))
        else:
            when(s + n < n_sp, lambda: project_out(s + n, kind == 7))

    wait_all(own_weights)
    tabled = (n_sp, n_out, n_tp) == TABLE_FOR
    if tabled:
        events = []

        def flush():
            for mine in range(n_sp):
                turn = [entry for entry in events if entry[5] == mine]

                def body(mine=mine, turn=turn):
                    for way, number, k, distance, side, _ in turn:
                        part = parts[number]
                        at = mine - distance if side == 0 else mine + distance
                        if way == HAND:
                            hand_over(part, source(k, at), False)
                            continue
                        if distance == 0 and k == 0 and number >= n_proj:
                            once(("own", mine), lambda: wait_all(own_out))
                            if not part.crossing:
                                once(("direct", mine), wo_ready)
                        piece = (mine, number, k, distance, side)
                        handle(part, k, distance, side, at, False, (way,), piece not in waited)
                        waited.add(piece)

                if turn:
                    pl.when(s == mine)(body)
            events.clear()

        for entry in TABLE:
            if len(entry) == 6:
                events.append(entry)
            else:
                flush()
                job(*entry)
        flush()
    else:
        wait_all(own_out)
        wo_ready()

        def spread(part):
            deal(part, 0, 0, False)
            for n in range(1, n_sp + 1):
                if n < n_sp:
                    deal(part, n, 0, False)
                for k in range(1, n_out):
                    deal(part, n - 1, k, False)

        for part in parts[:n_proj]:
            spread(part)
        job(0, 0, 0)
        for n in order:
            job(1, n, 0)
            job(2, n, 0)
            job(2, n, 1)
        for n in range(chunks):
            job(3, n, 0)
        job(4, 0, 0)
        for number in (2, 3, 4):
            for n in order:
                job(2, n, number)
        job(5, 0, 0)
        for part in parts[n_proj:]:
            spread(part)
        for at in range(n_sp):
            for k in range(n_out):
                hand_over(parts[-1], source(k, at), False)
        job(6, 0, 0)
        for own in (True, False):
            lax.fori_loop(0, n_sp, lambda n, c, own=own: (project_out(n, own), c)[1], 0)

    if tabled:
        events = [entry for entry in TABLE if len(entry) == 6]
        for mine in range(n_sp):

            def drain(mine=mine):
                for way, number, k, distance, side, _ in [entry for entry in events if entry[5] == mine]:
                    at = mine - distance if side == 0 else mine + distance
                    if way == HAND:
                        hand_over(parts[number], source(k, at), True)
                    else:
                        handle(parts[number], k, distance, side, at, True, (way,))

            pl.when(s == mine)(drain)
    else:
        for part in parts:
            for k in range(n_out):
                for distance in range(n_sp):
                    deal(part, distance, k, True)
        for at in range(n_sp):
            for k in range(n_out):
                hand_over(parts[-1], source(k, at), True)
    for which in range(2):
        when(has_right, lambda which=which: halo_copy(which).wait_send())
        for k in range(n_tp - 1):
            mix_copy(which, k).wait_send()
    for copy in wo_copies + list(tok_copies.values()):
        copy.wait_send()


def on_device(tokens, norm_gain, w_query, w_key, w_value, w_conv_in, w_conv_b, w_conv_c,
              conv_taps, sink_logits, w_attn_out, w_conv_out):
    n_sp, n_fs, n_tp = (lax.axis_size(axis) for axis in ("sp", "fs", "tp"))
    n_out = n_fs // 2
    shards = n_sp * n_fs
    rows, cols = tokens.shape[1:]
    width = cols * n_tp
    q_cols, kv_cols, channels = w_query.shape[1], w_key.shape[1], w_conv_in.shape[1]
    out_rows, out_cols = w_attn_out.shape
    separate = kv_cols % 128 == 0
    weights = [w_query]
    weights += [w_key, w_value] if separate else [jnp.concatenate([w_key, w_value], axis=1)]
    weights += [w_conv_in, w_conv_b, w_conv_c]
    owned = rows // n_tp
    kinds = part_kinds(out_rows)
    lanes = sum(lanes_of(wide, n_out) for wide, _, _ in kinds)
    kv_here = kv_cols // HEAD
    group = q_cols // kv_cols
    dma = pltpu.SemaphoreType.DMA
    vmem, anywhere = pl.BlockSpec(memory_space=pltpu.VMEM), pl.BlockSpec(memory_space=pl.ANY)
    summed = pl.pallas_call(
        functools.partial(layer_kernel, (n_sp, n_out, n_tp, 5, separate)),
        out_shape=jax.ShapeDtypeStruct((owned, width), BF16),
        in_specs=[anywhere, vmem, vmem, pl.BlockSpec(memory_space=pltpu.SMEM)] + [anywhere] * (len(weights) + 2),
        out_specs=vmem,
        scratch_shapes=[
            pltpu.VMEM((rows, width), BF16),
            pltpu.VMEM((5, width, q_cols), BF16),
            pltpu.VMEM((2 * n_tp, shards, out_rows, out_cols), BF16),
            pltpu.VMEM((rows, q_cols), BF16),
            pltpu.VMEM((WINDOW + rows, 2 * kv_cols), BF16),
            pltpu.VMEM((rows, channels), BF16),
            pltpu.VMEM((rows, channels), BF16),
            pltpu.VMEM((HALO + rows, channels), BF16),
            pltpu.VMEM((rows, q_cols), BF16),
            pltpu.VMEM((rows, channels), BF16),
            pltpu.VMEM((n_tp - 1, owned, q_cols), BF16),
            pltpu.VMEM((n_tp - 1, owned, channels), BF16),
            pltpu.VMEM((kv_here, group * WINDOW, 2 * WINDOW), F32),
            dma((lanes * n_sp * 2,)),
            dma((len(kinds) * shards,)),
            dma((9,)),
            dma((n_tp - 1, 2)),
            dma((n_tp - 1, 2)),
            dma((n_tp - 1, 4)),
            dma((n_tp - 1, 4)),
            dma((2,)),
            dma((2,)),
            dma((2, n_tp - 1)),
            dma((2, n_tp - 1)),
            dma((n_tp - 1, shards)),
            dma((n_tp - 1, shards)),
            dma((n_tp - 1, shards)),
            dma((n_tp - 1, shards)),
        ],
        compiler_params=pltpu.CompilerParams(
            collective_id=0, has_side_effects=True, vmem_limit_bytes=60 * 1024 * 1024
        ),
    )(tokens[0], norm_gain[None], conv_taps, sink_logits, *weights, w_attn_out, w_conv_out)
    return summed[None]


def solution(mesh):
    placed = (
        P("fs", "sp", "tp"),
        P(),
        P(("sp", "fs"), "tp"),
        P(("sp", "fs"), "tp"),
        P(("sp", "fs"), "tp"),
        P(("sp", "fs"), "tp"),
        P(("sp", "fs"), "tp"),
        P(("sp", "fs"), "tp"),
        P(None, "tp"),
        P("tp"),
        P("tp", ("sp", "fs")),
        P("tp", ("sp", "fs")),
    )
    return jax.shard_map(
        on_device,
        mesh=mesh,
        in_specs=placed,
        out_specs=P("fs", ("sp", "tp"), None),
        check_vma=False,
    )
```

```python
import functools

import jax
import jax.numpy as jnp
from jax import lax
from jax.experimental import pallas as pl
from jax.experimental.pallas import tpu as pltpu
from jax.sharding import PartitionSpec as P

HEADS = 16
HEAD = 64
WINDOW = 128
HALO = 16
MESH = pl.DeviceIdType.MESH
DIRECT_AFTER = 2
WAYS = RIGHT, LEFT, ACROSS, CROSS, CORE, HAND = range(6)
BF16, F32 = jnp.bfloat16, jnp.float32


TABLE_FOR = (4, 2, 2)
TABLE = (
    (0, 1, 0, 0, 0, 0), (0, 0, 0, 0, 0, 0), (2, 1, 0, 0, 0, 0), (2, 0, 0, 0, 0, 0), (3, 8, 0, 0, 0, 0),
    (4, 1, 0, 0, 0, 0), (0, 2, 0, 0, 0, 0), (4, 0, 0, 0, 0, 0), (2, 2, 0, 0, 0, 0), (4, 2, 0, 0, 0, 0),
    (4, 3, 0, 0, 0, 0), (4, 4, 0, 0, 0, 0), (4, 8, 0, 0, 0, 0), (0, 3, 0, 0, 0, 0), (2, 3, 0, 0, 0, 0),
    (4, 1, 1, 0, 0, 0), (4, 1, 0, 1, 1, 0), (0, 1, 1, 0, 0, 0), (2, 4, 0, 0, 0, 0), (4, 0, 1, 0, 0, 0),
    (4, 0, 0, 1, 1, 0), (0, 4, 0, 0, 0, 0), (2, 0, 0, 1, 1, 0), (4, 2, 1, 0, 0, 0), (4, 2, 0, 1, 1, 0),
    (0, 8, 0, 0, 0, 0), (2, 2, 0, 1, 1, 0), (0, 1, 0, 0, 0, 1), (0, 0, 0, 0, 0, 1), (1, 1, 0, 0, 0, 1),
    (1, 0, 0, 0, 0, 1), (2, 1, 0, 0, 0, 1), (2, 0, 0, 0, 0, 1), (0, 2, 0, 0, 0, 1), (3, 8, 0, 0, 0, 1),
    (1, 2, 0, 0, 0, 1), (4, 1, 0, 0, 0, 1), (2, 2, 0, 0, 0, 1), (4, 0, 0, 0, 0, 1), (4, 2, 0, 0, 0, 1),
    (4, 3, 0, 0, 0, 1), (4, 4, 0, 0, 0, 1), (4, 8, 0, 0, 0, 1), (0, 3, 0, 0, 0, 1), (1, 3, 0, 0, 0, 1),
    (2, 3, 0, 0, 0, 1), (4, 1, 0, 1, 0, 1), (4, 1, 0, 1, 1, 1), (4, 1, 1, 0, 0, 1), (0, 1, 0, 1, 0, 1),
    (1, 1, 1, 0, 0, 1), (2, 4, 0, 0, 0, 1), (4, 0, 0, 1, 0, 1), (4, 0, 0, 1, 1, 1), (4, 0, 1, 0, 0, 1),
    (0, 1, 1, 0, 0, 1), (1, 1, 0, 1, 1, 1), (2, 0, 0, 1, 0, 1), (4, 2, 0, 1, 0, 1), (4, 2, 0, 1, 1, 1),
    (4, 2, 1, 0, 0, 1), (0, 0, 0, 1, 0, 1), (1, 0, 0, 1, 1, 1), (2, 0, 0, 1, 1, 1), (4, 3, 0, 1, 0, 1),
    (0, 1, 0, 0, 0, 2), (0, 0, 0, 0, 0, 2), (1, 1, 0, 0, 0, 2), (1, 0, 0, 0, 0, 2), (2, 1, 0, 0, 0, 2),
    (2, 0, 0, 0, 0, 2), (0, 2, 0, 0, 0, 2), (3, 8, 0, 0, 0, 2), (1, 2, 0, 0, 0, 2), (4, 1, 0, 0, 0, 2),
    (2, 2, 0, 0, 0, 2), (4, 0, 0, 0, 0, 2), (4, 2, 0, 0, 0, 2), (4, 3, 0, 0, 0, 2), (4, 4, 0, 0, 0, 2),
    (4, 8, 0, 0, 0, 2), (0, 3, 0, 0, 0, 2), (1, 3, 0, 0, 0, 2), (2, 3, 0, 0, 0, 2), (4, 1, 0, 1, 0, 2),
    (4, 1, 0, 1, 1, 2), (4, 1, 1, 0, 0, 2), (0, 1, 0, 1, 0, 2), (1, 1, 1, 0, 0, 2), (2, 4, 0, 0, 0, 2),
    (4, 0, 0, 1, 0, 2), (4, 0, 0, 1, 1, 2), (4, 0, 1, 0, 0, 2), (0, 1, 1, 0, 0, 2), (1, 1, 0, 1, 1, 2),
    (2, 0, 0, 1, 0, 2), (4, 2, 0, 1, 0, 2), (4, 2, 0, 1, 1, 2), (4, 2, 1, 0, 0, 2), (0, 0, 0, 1, 0, 2),
    (1, 0, 0, 1, 1, 2), (2, 0, 0, 1, 1, 2), (4, 3, 0, 1, 0, 2), (4, 3, 0, 1, 1, 2), (1, 1, 0, 0, 0, 3),
    (1, 0, 0, 0, 0, 3), (2, 1, 0, 0, 0, 3), (2, 0, 0, 0, 0, 3), (3, 8, 0, 0, 0, 3), (4, 1, 0, 0, 0, 3),
    (1, 2, 0, 0, 0, 3), (4, 0, 0, 0, 0, 3), (2, 2, 0, 0, 0, 3), (4, 2, 0, 0, 0, 3), (4, 3, 0, 0, 0, 3),
    (4, 4, 0, 0, 0, 3), (4, 8, 0, 0, 0, 3), (1, 3, 0, 0, 0, 3), (2, 3, 0, 0, 0, 3), (4, 1, 0, 1, 0, 3),
    (4, 1, 1, 0, 0, 3), (1, 1, 1, 0, 0, 3), (2, 4, 0, 0, 0, 3), (4, 0, 0, 1, 0, 3), (4, 0, 1, 0, 0, 3),
    (1, 4, 0, 0, 0, 3), (2, 0, 0, 1, 0, 3), (4, 2, 0, 1, 0, 3), (4, 2, 1, 0, 0, 3), (1, 8, 0, 0, 0, 3),
    (2, 2, 0, 1, 0, 3), (4, 3, 0, 1, 0, 3), (1, 0, 0), (2, 3, 0, 1, 1, 0), (4, 3, 1, 0, 0, 0), (4, 3, 0, 1, 1, 0),
    (4, 1, 1, 1, 1, 0), (4, 4, 1, 0, 0, 0), (2, 8, 0, 0, 0, 0), (4, 1, 0, 2, 1, 0), (4, 0, 1, 1, 1, 0),
    (2, 0, 0, 2, 1, 0), (4, 0, 0, 2, 1, 0), (4, 2, 1, 1, 1, 0), (0, 2, 0, 1, 0, 1), (1, 2, 0, 1, 1, 1),
    (2, 2, 0, 1, 0, 1), (4, 3, 1, 0, 0, 1), (4, 3, 0, 1, 1, 1), (4, 1, 1, 1, 0, 1), (4, 1, 1, 1, 1, 1),
    (4, 4, 1, 0, 0, 1), (0, 1, 1, 1, 0, 1), (1, 1, 1, 1, 1, 1), (2, 2, 0, 1, 1, 1), (4, 4, 0, 1, 0, 1),
    (4, 1, 0, 2, 1, 1), (4, 0, 1, 1, 0, 1), (0, 3, 0, 1, 0, 1), (1, 1, 0, 2, 1, 1), (3, 8, 0, 1, 0, 1),
    (2, 3, 0, 1, 0, 1), (4, 8, 0, 1, 0, 1), (4, 0, 0, 2, 1, 1), (4, 0, 1, 1, 1, 1), (0, 4, 0, 1, 0, 1),
    (1, 0, 0, 2, 1, 1), (2, 0, 0, 2, 1, 1), (0, 2, 0, 1, 0, 2), (1, 2, 0, 1, 1, 2), (2, 2, 0, 1, 0, 2),
    (4, 3, 1, 0, 0, 2), (4, 1, 0, 2, 0, 2), (4, 1, 1, 1, 1, 2), (4, 4, 1, 0, 0, 2), (0, 1, 0, 2, 0, 2),
    (1, 1, 1, 1, 1, 2), (2, 2, 0, 1, 1, 2), (4, 1, 1, 1, 0, 2), (4, 4, 0, 1, 1, 2), (4, 0, 1, 1, 0, 2),
    (0, 1, 1, 1, 0, 2), (1, 3, 0, 1, 1, 2), (3, 8, 0, 1, 1, 2), (2, 3, 0, 1, 0, 2), (4, 8, 0, 1, 1, 2),
    (4, 0, 0, 2, 0, 2), (4, 0, 1, 1, 1, 2), (0, 0, 0, 2, 0, 2), (1, 4, 0, 1, 1, 2), (2, 0, 0, 2, 0, 2),
    (2, 3, 0, 1, 0, 3), (4, 3, 1, 0, 0, 3), (4, 1, 0, 2, 0, 3), (4, 4, 1, 0, 0, 3), (2, 8, 0, 0, 0, 3),
    (4, 1, 1, 1, 0, 3), (4, 0, 1, 1, 0, 3), (2, 0, 0, 2, 0, 3), (4, 0, 0, 2, 0, 3), (4, 2, 1, 1, 0, 3), (1, 1, 0),
    (0, 8, 1, 0, 0, 0), (2, 2, 0, 2, 1, 0), (3, 8, 1, 0, 0, 0), (4, 2, 0, 2, 1, 0), (4, 3, 1, 1, 1, 0),
    (4, 8, 1, 0, 0, 0), (0, 4, 0, 0, 0, 1), (1, 2, 0, 2, 1, 1), (2, 2, 0, 2, 1, 1), (4, 2, 1, 1, 0, 1),
    (4, 2, 0, 2, 1, 1), (0, 2, 0, 2, 0, 2), (1, 4, 0, 0, 0, 2), (2, 2, 0, 2, 0, 2), (4, 2, 0, 2, 0, 2),
    (4, 2, 1, 1, 0, 2), (1, 8, 1, 0, 0, 3), (2, 2, 0, 2, 0, 3), (3, 8, 1, 0, 0, 3), (4, 2, 0, 2, 0, 3),
    (4, 3, 1, 1, 0, 3), (4, 8, 1, 0, 0, 3), (0, 0, 0), (4, 1, 1, 2, 1, 0), (0, 6, 0, 0, 0, 0), (0, 7, 0, 0, 0, 0),
    (2, 6, 0, 0, 0, 0), (2, 7, 0, 0, 0, 0), (4, 0, 1, 2, 1, 0), (4, 6, 0, 0, 0, 0), (0, 5, 0, 0, 0, 0),
    (4, 7, 0, 0, 0, 0), (4, 5, 0, 0, 0, 0), (2, 5, 0, 0, 0, 0), (4, 1, 0, 3, 1, 0), (4, 2, 1, 2, 1, 0),
    (2, 0, 0, 3, 1, 0), (4, 0, 0, 3, 1, 0), (4, 6, 1, 0, 0, 0), (2, 2, 0, 3, 1, 0), (4, 2, 0, 3, 1, 0),
    (4, 7, 1, 0, 0, 0), (4, 1, 1, 3, 1, 0), (4, 1, 1, 2, 1, 1), (4, 2, 1, 1, 1, 1), (0, 8, 0, 0, 0, 1),
    (4, 1, 1, 2, 0, 2), (4, 2, 1, 1, 1, 2), (4, 1, 0, 3, 0, 3), (1, 6, 0, 0, 0, 3), (1, 7, 0, 0, 0, 3),
    (2, 6, 0, 0, 0, 3), (2, 7, 0, 0, 0, 3), (4, 0, 1, 2, 0, 3), (4, 6, 0, 0, 0, 3), (1, 5, 0, 0, 0, 3),
    (4, 7, 0, 0, 0, 3), (4, 5, 0, 0, 0, 3), (2, 5, 0, 0, 0, 3), (4, 1, 1, 2, 0, 3), (4, 2, 1, 2, 0, 3),
    (2, 0, 0, 3, 0, 3), (4, 0, 0, 3, 0, 3), (4, 6, 1, 0, 0, 3), (2, 2, 0, 3, 0, 3), (4, 2, 0, 3, 0, 3),
    (4, 7, 1, 0, 0, 3), (4, 5, 1, 0, 0, 3), (4, 1, 1, 3, 0, 3), (2, 0, 1), (4, 5, 1, 0, 0, 0), (1, 1, 1, 2, 1, 1),
    (2, 3, 0, 1, 1, 1), (4, 6, 0, 0, 0, 1), (4, 7, 0, 0, 0, 1), (4, 5, 0, 0, 0, 1), (3, 8, 1, 1, 0, 1),
    (4, 8, 1, 1, 0, 1), (1, 6, 0, 0, 0, 2), (2, 3, 0, 1, 1, 2), (4, 6, 0, 0, 0, 2), (4, 7, 0, 0, 0, 2),
    (4, 5, 0, 0, 0, 2), (4, 0, 1, 3, 0, 3), (2, 1, 1), (4, 3, 1, 1, 0, 1), (4, 3, 0, 2, 1, 1), (1, 3, 0, 2, 1, 1),
    (2, 3, 0, 2, 1, 1), (0, 6, 0, 0, 0, 1), (4, 4, 0, 2, 1, 1), (4, 0, 1, 2, 1, 1), (4, 6, 0, 1, 0, 1),
    (1, 4, 0, 2, 1, 1), (2, 4, 0, 2, 1, 1), (0, 7, 0, 0, 0, 1), (4, 4, 0, 1, 1, 1), (4, 2, 1, 2, 1, 1),
    (4, 7, 0, 1, 0, 1), (1, 3, 0, 1, 1, 1), (2, 4, 0, 1, 0, 1), (0, 5, 0, 0, 0, 1), (4, 6, 0, 1, 1, 1),
    (4, 3, 1, 1, 1, 1), (4, 5, 0, 1, 0, 1), (1, 4, 0, 1, 1, 1), (3, 8, 1, 1, 1, 2), (4, 3, 0, 2, 0, 2),
    (4, 8, 1, 1, 1, 2), (4, 3, 1, 1, 0, 2), (0, 1, 1, 2, 0, 2), (1, 7, 0, 0, 0, 2), (2, 3, 0, 2, 0, 2),
    (4, 4, 0, 2, 0, 2), (4, 0, 1, 2, 0, 2), (4, 6, 0, 1, 1, 2), (0, 3, 0, 2, 0, 2), (1, 5, 0, 0, 0, 2),
    (2, 4, 0, 2, 0, 2), (4, 4, 0, 1, 0, 2), (4, 2, 1, 2, 0, 2), (4, 7, 0, 1, 1, 2), (0, 4, 0, 2, 0, 2),
    (1, 8, 0, 0, 0, 2), (3, 8, 0, 1, 0, 2), (2, 4, 0, 1, 0, 2), (4, 8, 0, 1, 0, 2), (1, 6, 0, 1, 1, 2),
    (4, 3, 1, 1, 1, 2), (4, 5, 0, 1, 1, 2), (0, 3, 0, 1, 0, 2), (1, 2, 0), (2, 3, 0, 3, 1, 0), (4, 0, 1, 3, 1, 0),
    (4, 3, 0, 3, 1, 0), (2, 4, 0, 3, 1, 0), (4, 4, 0, 3, 1, 0), (0, 6, 0, 1, 0, 1), (2, 4, 0, 1, 1, 1),
    (4, 3, 1, 2, 1, 1), (4, 7, 0, 1, 1, 1), (1, 7, 0, 1, 1, 2), (2, 4, 0, 1, 1, 2), (4, 3, 1, 2, 0, 2),
    (2, 3, 0, 3, 0, 3), (4, 2, 1, 3, 0, 3), (4, 3, 0, 3, 0, 3), (2, 1, 0), (2, 0, 0), (4, 2, 1, 3, 1, 0),
    (1, 4, 0, 0, 0, 1), (2, 6, 0, 0, 0, 1), (0, 4, 0, 1, 0, 2), (2, 6, 0, 0, 0, 2), (4, 6, 0, 1, 0, 2),
    (2, 4, 0, 3, 0, 3), (4, 4, 0, 3, 0, 3), (2, 2, 0), (0, 7, 0, 1, 0, 1), (2, 2, 1), (2, 3, 0, 2, 1, 0),
    (4, 3, 0, 2, 1, 0), (4, 4, 1, 2, 1, 1), (4, 5, 0, 1, 1, 1), (1, 5, 0, 1, 1, 2), (4, 4, 1, 2, 0, 2), (2, 1, 2),
    (1, 6, 0, 0, 0, 1), (0, 4, 0, 0, 0, 2), (3, 0, 0), (2, 4, 0, 2, 1, 0), (4, 3, 1, 3, 1, 0), (4, 4, 0, 2, 1, 0),
    (0, 5, 0, 1, 0, 1), (2, 7, 0, 0, 0, 1), (3, 8, 0, 1, 1, 1), (4, 4, 1, 1, 0, 1), (1, 7, 0, 0, 0, 1),
    (4, 8, 0, 1, 1, 1), (2, 5, 0, 0, 0, 1), (4, 6, 0, 2, 1, 1), (1, 8, 0, 1, 1, 2), (2, 7, 0, 0, 0, 2),
    (4, 4, 1, 1, 0, 2), (0, 6, 0, 0, 0, 2), (4, 7, 0, 1, 0, 2), (1, 8, 1, 1, 1, 2), (4, 5, 0, 1, 0, 2),
    (2, 5, 0, 0, 0, 2), (2, 3, 0, 2, 0, 3), (4, 3, 1, 3, 0, 3), (4, 3, 0, 2, 0, 3), (3, 1, 0), (2, 4, 0, 1, 1, 0),
    (4, 4, 1, 3, 1, 0), (4, 4, 0, 1, 1, 0), (5, 8, 0, 0, 0, 0), (0, 8, 0, 1, 0, 1), (0, 8, 1, 1, 0, 1),
    (1, 5, 0, 0, 0, 1), (2, 8, 0, 0, 0, 1), (4, 4, 1, 1, 1, 1), (4, 7, 0, 2, 1, 1), (0, 7, 0, 0, 0, 2),
    (4, 4, 1, 1, 1, 2), (4, 6, 0, 2, 0, 2), (2, 8, 0, 0, 0, 2), (2, 4, 0, 2, 0, 3), (4, 4, 1, 3, 0, 3),
    (4, 4, 0, 2, 0, 3), (5, 8, 0, 0, 0, 3), (5, 8, 1, 0, 0, 3), (4, 0, 0), (2, 2, 2), (4, 3, 1, 2, 1, 0),
    (5, 8, 1, 0, 0, 0), (2, 4, 0, 1, 0, 3), (4, 4, 0, 1, 0, 3), (1, 3, 0), (2, 6, 0, 1, 1, 0), (4, 6, 0, 1, 1, 0),
    (4, 4, 1, 2, 1, 0), (2, 7, 0, 1, 1, 0), (4, 7, 0, 1, 1, 0), (4, 4, 1, 1, 1, 0), (2, 6, 0, 1, 0, 1),
    (1, 8, 0, 0, 0, 1), (4, 6, 1, 0, 0, 1), (5, 8, 0, 0, 0, 1), (4, 5, 0, 2, 1, 1), (5, 8, 0, 1, 0, 1),
    (2, 6, 0, 1, 0, 2), (4, 6, 1, 0, 0, 2), (0, 5, 0, 0, 0, 2), (5, 8, 0, 0, 0, 2), (4, 3, 1, 2, 0, 3),
    (2, 6, 0, 1, 0, 3), (4, 6, 0, 1, 0, 3), (4, 4, 1, 2, 0, 3), (2, 7, 0, 1, 0, 3), (4, 7, 0, 1, 0, 3),
    (4, 4, 1, 1, 0, 3), (2, 2, 4), (2, 5, 0, 1, 1, 0), (4, 5, 0, 1, 1, 0), (4, 7, 0, 2, 0, 2), (5, 8, 0, 1, 1, 2),
    (2, 5, 0, 1, 0, 3), (4, 5, 0, 1, 0, 3), (2, 3, 1), (1, 6, 0, 1, 1, 1), (2, 6, 0, 1, 1, 1), (3, 8, 0, 2, 1, 1),
    (4, 7, 1, 0, 0, 1), (4, 8, 0, 2, 1, 1), (5, 8, 1, 1, 0, 1), (2, 1, 4), (3, 8, 0, 1, 1, 0), (4, 8, 0, 1, 1, 0),
    (4, 6, 1, 1, 1, 0), (2, 6, 0, 1, 1, 2), (4, 7, 1, 0, 0, 2), (5, 8, 1, 1, 1, 2), (3, 8, 0, 1, 0, 3),
    (4, 8, 0, 1, 0, 3), (4, 6, 1, 1, 0, 3), (2, 0, 2), (3, 8, 1, 2, 1, 1), (4, 8, 1, 2, 1, 1), (5, 8, 0, 1, 1, 1),
    (0, 8, 0, 0, 0, 2), (4, 5, 0, 2, 0, 2), (5, 8, 0, 1, 0, 2), (2, 0, 4), (2, 0, 3), (1, 7, 0, 1, 1, 1),
    (2, 7, 0, 1, 0, 1), (4, 5, 1, 0, 0, 1), (0, 6, 0, 1, 0, 2), (2, 7, 0, 1, 0, 2), (3, 8, 0, 2, 0, 2),
    (4, 5, 1, 0, 0, 2), (4, 8, 0, 2, 0, 2), (2, 2, 3), (2, 6, 0, 2, 1, 0), (4, 6, 0, 2, 1, 0), (4, 7, 1, 1, 1, 0),
    (4, 7, 1, 1, 0, 3), (2, 1, 3), (0, 8, 1, 0, 0, 1), (3, 8, 1, 0, 0, 1), (4, 8, 1, 0, 0, 1), (1, 8, 1, 0, 0, 2),
    (3, 8, 1, 0, 0, 2), (3, 8, 1, 2, 0, 2), (4, 8, 1, 0, 0, 2), (4, 8, 1, 2, 0, 2), (2, 6, 0, 2, 0, 3),
    (4, 6, 0, 2, 0, 3), (2, 3, 2), (1, 5, 0, 1, 1, 1), (2, 7, 0, 1, 1, 1), (5, 8, 0, 1, 0, 3), (2, 3, 3),
    (5, 8, 0, 1, 1, 0), (4, 6, 1, 1, 0, 1), (3, 8, 1, 1, 1, 1), (4, 8, 1, 1, 1, 1), (1, 8, 1, 0, 0, 1),
    (2, 5, 0, 1, 0, 1), (1, 8, 0, 1, 1, 1), (4, 6, 1, 1, 1, 1), (1, 6, 0, 2, 1, 1), (2, 5, 0, 1, 1, 1),
    (0, 7, 0, 1, 0, 2), (2, 7, 0, 1, 1, 2), (5, 0, 0), (2, 7, 0, 2, 1, 0), (4, 7, 0, 2, 1, 0), (4, 5, 1, 1, 1, 0),
    (2, 7, 0, 2, 0, 3), (4, 7, 0, 2, 0, 3), (4, 5, 1, 1, 0, 3), (2, 3, 0), (4, 6, 1, 1, 0, 2), (2, 3, 4),
    (4, 7, 1, 1, 0, 1), (3, 8, 1, 1, 0, 2), (2, 5, 0, 1, 0, 2), (4, 8, 1, 1, 0, 2), (3, 2, 0), (2, 5, 0, 2, 1, 0),
    (3, 8, 1, 1, 1, 0), (4, 5, 0, 2, 1, 0), (4, 8, 1, 1, 1, 0), (4, 6, 1, 2, 1, 0), (1, 7, 0, 2, 1, 1),
    (2, 6, 0, 2, 1, 1), (4, 7, 1, 1, 1, 1), (5, 8, 0, 2, 1, 1), (5, 8, 1, 2, 1, 1), (0, 5, 0, 1, 0, 2),
    (4, 6, 1, 1, 1, 2), (2, 5, 0, 1, 1, 2), (2, 5, 0, 2, 0, 3), (3, 8, 0, 2, 0, 3), (4, 5, 0, 2, 0, 3),
    (4, 8, 0, 2, 0, 3), (4, 6, 1, 2, 0, 3), (3, 3, 0), (3, 8, 0, 2, 1, 0), (4, 8, 0, 2, 1, 0), (4, 7, 1, 2, 1, 0),
    (1, 5, 0, 2, 1, 1), (2, 7, 0, 2, 1, 1), (4, 5, 1, 1, 0, 1), (5, 8, 1, 0, 0, 1), (5, 8, 1, 1, 1, 1),
    (0, 8, 0, 1, 0, 2), (0, 8, 1, 0, 0, 2), (4, 7, 1, 1, 0, 2), (2, 6, 0, 2, 0, 2), (5, 8, 0, 2, 0, 2),
    (3, 8, 1, 1, 0, 3), (4, 8, 1, 1, 0, 3), (4, 7, 1, 2, 0, 3), (5, 1, 0), (2, 6, 0, 3, 1, 0), (4, 6, 0, 3, 1, 0),
    (4, 5, 1, 2, 1, 0), (2, 7, 0, 3, 1, 0), (4, 7, 0, 3, 1, 0), (4, 6, 1, 3, 1, 0), (1, 8, 1, 1, 1, 1),
    (2, 5, 0, 2, 1, 1), (1, 8, 0, 2, 1, 1), (4, 5, 1, 1, 1, 1), (1, 8, 1, 2, 1, 1), (4, 6, 1, 2, 1, 1),
    (4, 7, 1, 2, 1, 1), (0, 6, 0, 2, 0, 2), (5, 8, 1, 0, 0, 2), (4, 7, 1, 1, 1, 2), (5, 8, 1, 2, 0, 2),
    (2, 7, 0, 2, 0, 2), (0, 7, 0, 2, 0, 2), (4, 5, 1, 1, 0, 2), (2, 5, 0, 2, 0, 2), (0, 5, 0, 2, 0, 2),
    (4, 5, 1, 1, 1, 2), (0, 8, 0, 2, 0, 2), (0, 8, 1, 1, 0, 2), (4, 6, 1, 2, 0, 2), (0, 8, 1, 2, 0, 2),
    (4, 7, 1, 2, 0, 2), (2, 6, 0, 3, 0, 3), (4, 6, 0, 3, 0, 3), (4, 5, 1, 2, 0, 3), (2, 7, 0, 3, 0, 3),
    (4, 7, 0, 3, 0, 3), (4, 6, 1, 3, 0, 3), (6, 0, 0), (7, 1, 1), (2, 5, 0, 3, 1, 0), (4, 5, 0, 3, 1, 0),
    (4, 5, 1, 2, 1, 1), (7, 0, 0), (3, 8, 1, 2, 1, 0), (4, 8, 1, 2, 1, 0), (5, 8, 1, 1, 1, 0), (4, 7, 1, 3, 1, 0),
    (5, 8, 0, 2, 1, 0), (3, 8, 0, 3, 1, 0), (4, 8, 0, 3, 1, 0), (3, 8, 1, 3, 1, 0), (4, 8, 1, 3, 1, 0),
    (5, 8, 1, 2, 1, 0), (4, 5, 1, 3, 1, 0), (5, 8, 0, 3, 1, 0), (4, 5, 1, 2, 0, 2), (5, 8, 1, 1, 0, 2),
    (2, 5, 0, 3, 0, 3), (4, 5, 0, 3, 0, 3), (7, 3, 1), (8, 0, 0), (5, 8, 1, 3, 1, 0), (5, 8, 0, 2, 0, 3), (8, 1, 1),
    (7, 1, 0), (3, 8, 0, 3, 0, 3), (4, 8, 0, 3, 0, 3), (4, 7, 1, 3, 0, 3), (5, 8, 1, 1, 0, 3), (7, 2, 1), (8, 3, 1),
    (3, 8, 1, 2, 0, 3), (4, 8, 1, 2, 0, 3), (7, 2, 0), (3, 8, 1, 3, 0, 3), (4, 5, 1, 3, 0, 3), (4, 8, 1, 3, 0, 3),
    (8, 2, 1), (5, 8, 0, 3, 0, 3), (7, 3, 0), (5, 8, 1, 2, 0, 3), (8, 1, 0), (5, 8, 1, 3, 0, 3), (8, 2, 0), (8, 3, 0),
)


def when(condition, body):
    if condition is True:
        body()
    elif condition is not False:
        pl.when(condition)(body)


def aligned(at, size):
    return at if isinstance(at, int) else pl.multiple_of(at, size)


class Part:
    def __init__(self, number, wide, crossing, place, base):
        self.number, self.wide, self.crossing, self.place, self.base = number, wide, crossing, place, base


def part_kinds(out_rows):
    kinds = [(False, False, None), (True, False, None)] + [(False, False, None)] * 3
    quarter = out_rows // 4
    kinds += [(False, False, (n * quarter, quarter)) for n in range(3)]
    return kinds + [(True, True, (3 * quarter, quarter))]


def lanes_of(wide, n_out):
    return 1 + n_out + (2 if wide else 1) * (n_out - 1)


def layer_kernel(sizes, *refs):
    n_sp, n_out, n_tp, n_proj, separate = sizes
    tok = refs[0]
    n_in = 6 if separate else 5
    w_own = refs[4 : 4 + n_in]
    out_own = refs[4 + n_in : 6 + n_in]
    out = refs[6 + n_in]
    (tokf, w_all, wo_all, q_buf, kv_buf, inner, gate_b, product, m_att, m_conv, r_att, r_conv, bias,
     send_sem, recv_sem, own_sem, wo_send, wo_recv, tok_send, tok_recv, halo_send, halo_recv,
     mix_send, mix_recv, cross_send, cross_recv, pass_send, pass_recv,
     out_buf, out_sem, gain, taps, sinks) = refs[7 + n_in :]
    out_hbm, out = out, out_buf
    n_fs = 2 * n_out
    shards = n_sp * n_fs
    s, f, t = lax.axis_index("sp"), lax.axis_index("fs"), lax.axis_index("tp")
    o, i = f // 2, f % 2
    rows_total, width = tokf.shape
    cols = tok.shape[1]
    q_cols = q_buf.shape[1]
    kv_cols = kv_buf.shape[1] // 2
    k_rows = w_own[0].shape[0]
    out_rows, out_cols = out_own[0].shape
    owned = rows_total // n_tp
    chunks = 4
    step = rows_total // chunks
    tabled = (n_sp, n_out, n_tp) == TABLE_FOR
    order = [3, 0, 1, 2]
    attended = [0, 1, 2, 3]
    if tabled:
        order = [3, 2 - 2 * t, 1, 2 * t]
        attended = [3 - 3 * t, 2 - t, 1 + t, 3 * t]
    me = s * n_fs + f

    right, left, core = (s + 1, f, t), (s - 1, f, t), (s, o * 2 + (1 - i), t)
    across = [(s, lax.rem(o + k, n_out) * 2 + i, t) for k in range(1, n_out)]
    peers = [(s, f, lax.rem(t + k, n_tp)) for k in range(1, n_tp)]
    has_right, has_left = s < n_sp - 1, s > 0

    local = []
    spots = [(0, 0), (1, 0), (1, kv_cols), (2, 0), (3, 0), (4, 0)] if separate else [(n, 0) for n in range(5)]
    for n, (number, col) in enumerate(spots):
        place = w_all.at[number, pl.ds(me * k_rows, k_rows), pl.ds(col, w_own[n].shape[1])]
        local.append(pltpu.make_async_copy(w_own[n], place, own_sem.at[n]))
    for a in range(2):
        local.append(pltpu.make_async_copy(out_own[a], wo_all.at[2 * t + a, me], own_sem.at[6 + a]))
    for n, (source_ref, spot) in enumerate(zip(refs[1:4], (gain, taps, sinks))):
        local.append(pltpu.make_async_copy(source_ref, spot, own_sem.at[9 + n]))
    my_cols = pl.ds(pl.multiple_of(t * cols, cols), cols)
    local.append(pltpu.make_async_copy(tok, tokf.at[:, my_cols], own_sem.at[8]))
    for copy in local:
        copy.start()

    barrier = pltpu.get_barrier_semaphore()
    greet = lambda where: pl.semaphore_signal(barrier, inc=1, device_id=where, device_id_type=MESH)
    when(has_right, lambda: greet(right))
    when(has_left, lambda: greet(left))
    for where in across + [core] + peers:
        greet(where)
    count = len(across) + 1 + len(peers)
    pl.semaphore_wait(barrier, count + has_right.astype(jnp.int32) + has_left.astype(jnp.int32))

    wo_copies, tok_copies = [], {}
    direct = pl.ds(0, 3 * (out_rows // 4))
    def send_direct():
        for k, peer in enumerate(peers):
            for a in range(2):
                copy = pltpu.make_async_remote_copy(
                    src_ref=out_own[a].at[direct], dst_ref=wo_all.at[2 * t + a, me, direct],
                    send_sem=wo_send.at[k, a], recv_sem=wo_recv.at[k, a], device_id=peer, device_id_type=MESH,
                )
                copy.start()
                wo_copies.append(copy)

    wanted = [3, 2 * t, 1, 2 - 2 * t] if tabled else order
    for turn, n in enumerate(wanted):
        if turn == DIRECT_AFTER:
            send_direct()
        here = pl.ds(aligned(n * step, step), step)
        for k, peer in enumerate(peers):
            copy = pltpu.make_async_remote_copy(
                src_ref=tok.at[here], dst_ref=tokf.at[here, my_cols],
                send_sem=tok_send.at[k, turn], recv_sem=tok_recv.at[k, turn], device_id=peer, device_id_type=MESH,
            )
            copy.start()
            tok_copies[k, turn] = copy

    parts, base = [], 0
    for number, (wide, crossing, rows) in enumerate(part_kinds(out_rows)):
        if rows is None:
            place = lambda src, g, number=number: w_all.at[number, pl.ds(src * k_rows, k_rows)]
        elif crossing:
            place = lambda src, g, rows=rows: wo_all.at[pl.ds(2 * g, 2), src, pl.ds(*rows)]
        else:
            place = lambda src, g, rows=rows: wo_all.at[:, src, pl.ds(*rows)]
        parts.append(Part(number, wide, crossing, place, base))
        base += lanes_of(wide, n_out) * n_sp * 2

    def copy_of(part, src, where, lane, distance, side):
        spot = part.place(src, t)
        return pltpu.make_async_remote_copy(
            src_ref=spot, dst_ref=spot,
            send_sem=send_sem.at[part.base + (lane * n_sp + distance) * 2 + side],
            recv_sem=recv_sem.at[part.number * shards + src],
            device_id=where, device_id_type=MESH,
        )

    def cross_copy(part, src, k):
        spot = part.place(src, t)
        return pltpu.make_async_remote_copy(
            src_ref=spot, dst_ref=spot, send_sem=cross_send.at[k, src], recv_sem=cross_recv.at[k, src],
            device_id=peers[k], device_id_type=MESH,
        )

    def pass_copy(part, src, k):
        spot = part.place(src, lax.rem(t + n_tp - k - 1, n_tp))
        return pltpu.make_async_remote_copy(
            src_ref=spot, dst_ref=spot, send_sem=pass_send.at[k, src], recv_sem=pass_recv.at[k, src],
            device_id=core, device_id_type=MESH,
        )

    def source(k, at):
        return at * n_fs + lax.rem(o + n_out - k, n_out) * 2 + i

    def handle(part, k, distance, side, at, drain, ways=WAYS, arrival=True):
        first = isinstance(distance, int) and distance == 0
        src = source(k, at)
        mine = (at + distance if side == 0 else at - distance) if isinstance(at, int) else s
        more_right, more_left = mine < n_sp - 1, mine > 0
        lane_z, lane_core = 0, 1
        if k > 0:
            lane_z = 2 + len(across) + 2 * (k - 1)
            lane_core = lane_z + 1
            if not part.wide:
                lane_core = 2 + len(across) + k - 1

        def go(where, lane, way):
            copy = copy_of(part, src, where, lane, distance, way)
            copy.wait_send() if drain else copy.start()

        if arrival and not (first and k == 0) and not drain:
            copy_of(part, src, core, 0, 0, 0).wait_recv()
        if k == 0 or part.wide:
            if RIGHT in ways and (first or side == 0):
                when(more_right, lambda: go(right, lane_z, 0))
            if LEFT in ways and (first or side == 1):
                when(more_left, lambda: go(left, lane_z, 1))
        if ACROSS in ways and k == 0 and (first or not part.wide):
            for n, where in enumerate(across):
                go(where, 2 + n, side)
        if CROSS in ways and part.crossing:
            for n in range(len(peers)):
                copy = cross_copy(part, src, n)
                copy.wait_send() if drain else copy.start()
        if CORE in ways:
            go(core, lane_core, side)

    def hand_over(part, src, drain):
        for k in range(len(peers)):
            if not drain:
                cross_copy(part, src, k).wait_recv()
            copy = pass_copy(part, src, k)
            copy.wait_send() if drain else copy.start()

    def deal(part, distance, k, drain):
        if isinstance(distance, int) and distance == 0:
            handle(part, k, 0, 0, s, drain)
            return
        when(s - distance >= 0, lambda: handle(part, k, distance, 0, s - distance, drain))
        when(s + distance < n_sp, lambda: handle(part, k, distance, 1, s + distance, drain))

    def partner(number, source_s):
        for source_o in range(n_out):
            copy_of(parts[number], source_s * n_fs + source_o * 2 + (1 - i), core, 0, 0, 0).wait_recv()

    def finish(number):
        for source_s in range(n_sp):
            partner(number, source_s)

    def norm(n):
        size = 32

        def body(r, carry):
            here = pl.ds(pl.multiple_of(n * step + r * size, size), size)
            values = tokf[here, :].astype(F32)
            centred = values - jnp.sum(values, axis=1, keepdims=True) * (1.0 / width)
            variance = jnp.sum(centred * centred, axis=1, keepdims=True) * (1.0 / width)
            tokf[here, :] = (centred * lax.rsqrt(variance + 1e-05) * gain[...]).astype(BF16)
            return carry

        lax.fori_loop(0, step // size, body, 0)

    def project(number, n):
        first = aligned(n * step, step)
        here = pl.ds(first, step)
        result = jnp.dot(tokf[here, :], w_all[number], preferred_element_type=F32).astype(BF16)
        if number == 0:
            q_buf[here, :] = result
        elif number == 1:
            kv_buf[pl.ds(first + WINDOW, step), :] = result
        elif number == 2:
            inner[here, :] = result
        elif number == 3:
            gate_b[here, :] = result
        else:
            made = result.astype(F32) * inner[here, :].astype(F32)
            product[pl.ds(first + HALO, step), :] = made.astype(BF16)

    def halo_copy(which):
        buffer, size = ((kv_buf, WINDOW), (product, HALO))[which]
        return pltpu.make_async_remote_copy(
            src_ref=buffer.at[pl.ds(rows_total, size)], dst_ref=buffer.at[pl.ds(0, size)],
            send_sem=halo_send.at[which], recv_sem=halo_recv.at[which], device_id=right, device_id_type=MESH,
        )

    def halo_out(which):
        when(has_right, lambda: halo_copy(which).start())

        def clear():
            buffer, size = ((kv_buf, WINDOW), (product, HALO))[which]
            buffer[0:size, :] = jnp.zeros((size, buffer.shape[1]), BF16)

        when(s == 0, clear)

    def halo_in(which):
        when(has_left, lambda: halo_copy(which).wait_recv())

    heads_here = q_cols // HEAD
    kv_here = kv_cols // HEAD
    group = heads_here // kv_here
    tall = group * WINDOW

    def make_bias():
        row = lax.broadcasted_iota(jnp.int32, (tall, 2 * WINDOW), 0)
        col = lax.broadcasted_iota(jnp.int32, (tall, 2 * WINDOW), 1)
        distance = WINDOW + row % WINDOW - col
        keep = (distance >= 0) & (distance < WINDOW)
        for h in range(kv_here):
            head = (t * heads_here + h * group + row // WINDOW + 1).astype(F32)
            slope = jnp.exp2(head * (-8.0 / HEADS))
            bias[h] = jnp.where(keep, -(slope * distance.astype(F32)), -jnp.inf)

    def attend(n):
        row = lax.broadcasted_iota(jnp.int32, (tall, 1), 0) // WINDOW
        col = lax.broadcasted_iota(jnp.int32, (1, 2 * WINDOW), 1)

        def body(b, carry):
            block = n * (step // WINDOW) + b
            first = pl.multiple_of(block * WINDOW, WINDOW)
            before = jnp.where(col >= WINDOW, 0.0, jnp.where((s == 0) & (block == 0), -jnp.inf, 0.0))
            queries = q_buf[pl.ds(first, WINDOW), :]
            band = kv_buf[pl.ds(first, 2 * WINDOW), :]
            outs = []
            for h in range(kv_here):
                query = jnp.concatenate(
                    [queries[:, (h * group + g) * HEAD : (h * group + g + 1) * HEAD] for g in range(group)], axis=0
                )
                key = band[:, h * HEAD : (h + 1) * HEAD]
                value = band[:, kv_cols + h * HEAD : kv_cols + (h + 1) * HEAD]
                scores = lax.dot_general(query, key, (((1,), (1,)), ((), ())), preferred_element_type=F32)
                scores = scores * HEAD ** (-0.5) + bias[h] + before
                sink = jnp.full((tall, 1), sinks[h * group], F32)
                for g in range(1, group):
                    sink = jnp.where(row == g, sinks[h * group + g], sink)
                top = jnp.maximum(jnp.max(scores, axis=1, keepdims=True), sink)
                raised = jnp.exp(scores - top)
                total = jnp.sum(raised, axis=1, keepdims=True) + jnp.exp(sink - top)
                weights = (raised * (1.0 / total)).astype(BF16)
                mixed = jnp.dot(weights, value, preferred_element_type=F32).astype(BF16)
                outs += [mixed[g * WINDOW : (g + 1) * WINDOW] for g in range(group)]
            m_att[pl.ds(first, WINDOW), :] = jnp.concatenate(outs, axis=1)
            return carry

        lax.fori_loop(0, step // WINDOW, body, 0)

    def convolve(start, count):
        size = 64

        def body(r, carry):
            first = pl.multiple_of(start + r * size, size)
            padded = product[pl.ds(first, size + HALO), :].astype(F32)
            tap = taps[...].astype(F32)
            filtered = (
                tap[0:1] * padded[HALO - 2 : HALO - 2 + size]
                + tap[1:2] * padded[HALO - 1 : HALO - 1 + size]
                + tap[2:3] * padded[HALO : HALO + size]
            )
            m_conv[pl.ds(first, size), :] = (gate_b[pl.ds(first, size), :].astype(F32) * filtered).astype(BF16)
            return carry

        lax.fori_loop(0, count // size, body, 0)

    def mix_copy(which, k):
        source, target = ((m_att, r_att), (m_conv, r_conv))[which]
        return pltpu.make_async_remote_copy(
            src_ref=source.at[pl.ds(pl.multiple_of(peers[k][2] * owned, owned), owned)], dst_ref=target.at[k],
            send_sem=mix_send.at[which, k], recv_sem=mix_recv.at[which, k],
            device_id=peers[k], device_id_type=MESH,
        )

    def mix_out(which):
        for k in range(n_tp - 1):
            mix_copy(which, k).start()

    def mix_in():
        for which in range(2):
            for k in range(n_tp - 1):
                mix_copy(which, k).wait_recv()

    def project_out(source_s, own):
        for number in range(n_proj, len(parts)):
            if own:
                partner(number, source_s)
            elif parts[number].crossing:
                for source_o in range(n_out):
                    for k in range(n_tp - 1):
                        pass_copy(parts[number], source_s * n_fs + source_o * 2 + (1 - i), k).wait_recv()
        block = n_fs * out_cols
        tile = min(256, owned)

        def weights(row):
            blocks = [wo_all[row, source_s * n_fs + n] for n in range(n_fs)]
            return jnp.concatenate(blocks, axis=1)

        def body(r, carry):
            here = pl.ds(pl.multiple_of(r * tile, tile), tile)
            where = pl.ds(pl.multiple_of(source_s * block, block), block)
            total = None if own else out[here, where].astype(F32)
            for k in (0,) if own else range(1, n_tp):
                g = lax.rem(t + n_tp - k, n_tp)
                if own:
                    mine = pl.ds(pl.multiple_of(t * owned + r * tile, tile), tile)
                    att, conv = m_att[mine, :], m_conv[mine, :]
                else:
                    att, conv = r_att[k - 1, here, :], r_conv[k - 1, here, :]
                partial = jnp.dot(att, weights(2 * g), preferred_element_type=F32)
                partial = partial + jnp.dot(conv, weights(2 * g + 1), preferred_element_type=F32)
                total = partial if own else total + partial.astype(BF16).astype(F32)
            out[here, where] = total.astype(BF16)
            return carry

        lax.fori_loop(0, owned // tile, body, 0)
        if not own:
            out_copy(source_s).start()

    def out_copy(source_s):
        block = n_fs * out_cols
        where = pl.ds(pl.multiple_of(source_s * block, block), block)
        return pltpu.make_async_copy(out.at[:, where], out_hbm.at[:, where], out_sem.at[source_s])

    own_weights, own_out, small, own_tokens = local[:-6], local[-6:-4], local[-4:-1], local[-1]
    waited = set()

    def once(key, body):
        if key not in waited:
            waited.add(key)
            body()

    def wait_all(copies):
        for copy in copies:
            copy.wait()

    def wo_ready():
        for copy in wo_copies:
            copy.wait_recv()

    def job(kind, n, side):
        if kind == 0:
            make_bias()
        elif kind == 1:
            once("tokens", lambda: wait_all(small + [own_tokens]))
            for k in range(n_tp - 1):
                tok_copies[k, n].wait_recv()
            norm(order[n])
        elif kind == 2:
            once(("part", side), lambda: finish(side))
            project(side, order[n])
            if n == 0 and side in (1, 4):
                halo_out(0 if side == 1 else 1)
        elif kind == 3:
            once("halo", lambda: halo_in(0))
            attend(attended[n])
        elif kind == 4:
            mix_out(0)
        elif kind == 5:
            once("product", lambda: halo_in(1))
            if not tabled:
                convolve(0, rows_total)
            else:
                convolve((t if n == 1 else 1 - t) * owned, owned)
            if n == 0:
                mix_out(1)
        elif kind == 6:
            mix_in()
        elif n == 0:
            project_out(s, kind == 7)
        elif side == 0:
            when(s - n >= 0, lambda: project_out(s - n, kind == 7))
        else:
            when(s + n < n_sp, lambda: project_out(s + n, kind == 7))

    wait_all(own_weights)
    if tabled:
        events = []

        def flush():
            for mine in range(n_sp):
                turn = [entry for entry in events if entry[5] == mine]

                def body(mine=mine, turn=turn):
                    for way, number, k, distance, side, _ in turn:
                        part = parts[number]
                        at = mine - distance if side == 0 else mine + distance
                        if way == HAND:
                            hand_over(part, source(k, at), False)
                            continue
                        if distance == 0 and k == 0 and number >= n_proj:
                            once(("own", mine), lambda: wait_all(own_out))
                            if not part.crossing:
                                once(("direct", mine), wo_ready)
                        piece = (mine, number, k, distance, side)
                        handle(part, k, distance, side, at, False, (way,), piece not in waited)
                        waited.add(piece)

                if turn:
                    pl.when(s == mine)(body)
            events.clear()

        for entry in TABLE:
            if len(entry) == 6:
                events.append(entry)
            else:
                flush()
                job(*entry)
        flush()
    else:
        wait_all(own_out)
        wo_ready()

        def spread(part):
            deal(part, 0, 0, False)
            for n in range(1, n_sp + 1):
                if n < n_sp:
                    deal(part, n, 0, False)
                for k in range(1, n_out):
                    deal(part, n - 1, k, False)

        for part in parts[:n_proj]:
            spread(part)
        job(0, 0, 0)
        for n in range(chunks):
            job(1, n, 0)
            job(2, n, 0)
            job(2, n, 1)
        for n in range(chunks):
            job(3, n, 0)
        job(4, 0, 0)
        for number in (2, 3, 4):
            for n in range(chunks):
                job(2, n, number)
        job(5, 0, 0)
        for part in parts[n_proj:]:
            spread(part)
        for at in range(n_sp):
            for k in range(n_out):
                hand_over(parts[-1], source(k, at), False)
        job(6, 0, 0)
        for own in (True, False):
            lax.fori_loop(0, n_sp, lambda n, c, own=own: (project_out(n, own), c)[1], 0)

    for source_s in range(n_sp):
        out_copy(source_s).wait()
    if tabled:
        events = [entry for entry in TABLE if len(entry) == 6]
        for mine in range(n_sp):

            def drain(mine=mine):
                for way, number, k, distance, side, _ in [entry for entry in events if entry[5] == mine]:
                    at = mine - distance if side == 0 else mine + distance
                    if way == HAND:
                        hand_over(parts[number], source(k, at), True)
                    else:
                        handle(parts[number], k, distance, side, at, True, (way,))

            pl.when(s == mine)(drain)
    else:
        for part in parts:
            for k in range(n_out):
                for distance in range(n_sp):
                    deal(part, distance, k, True)
        for at in range(n_sp):
            for k in range(n_out):
                hand_over(parts[-1], source(k, at), True)
    for which in range(2):
        when(has_right, lambda which=which: halo_copy(which).wait_send())
        for k in range(n_tp - 1):
            mix_copy(which, k).wait_send()
    for copy in wo_copies + list(tok_copies.values()):
        copy.wait_send()


def on_device(tokens, norm_gain, w_query, w_key, w_value, w_conv_in, w_conv_b, w_conv_c,
              conv_taps, sink_logits, w_attn_out, w_conv_out):
    n_sp, n_fs, n_tp = (lax.axis_size(axis) for axis in ("sp", "fs", "tp"))
    n_out = n_fs // 2
    shards = n_sp * n_fs
    rows, cols = tokens.shape[1:]
    width = cols * n_tp
    q_cols, kv_cols, channels = w_query.shape[1], w_key.shape[1], w_conv_in.shape[1]
    out_rows, out_cols = w_attn_out.shape
    separate = kv_cols % 128 == 0
    weights = [w_query]
    weights += [w_key, w_value] if separate else [jnp.concatenate([w_key, w_value], axis=1)]
    weights += [w_conv_in, w_conv_b, w_conv_c]
    owned = rows // n_tp
    kinds = part_kinds(out_rows)
    lanes = sum(lanes_of(wide, n_out) for wide, _, _ in kinds)
    kv_here = kv_cols // HEAD
    group = q_cols // kv_cols
    dma = pltpu.SemaphoreType.DMA
    summed = pl.pallas_call(
        functools.partial(layer_kernel, (n_sp, n_out, n_tp, 5, separate)),
        out_shape=jax.ShapeDtypeStruct((owned, width), BF16),
        in_specs=[pl.BlockSpec(memory_space=pltpu.HBM)] * (len(weights) + 6),
        out_specs=pl.BlockSpec(memory_space=pl.ANY),
        scratch_shapes=[
            pltpu.VMEM((rows, width), BF16),
            pltpu.VMEM((5, width, q_cols), BF16),
            pltpu.VMEM((2 * n_tp, shards, out_rows, out_cols), BF16),
            pltpu.VMEM((rows, q_cols), BF16),
            pltpu.VMEM((WINDOW + rows, 2 * kv_cols), BF16),
            pltpu.VMEM((rows, channels), BF16),
            pltpu.VMEM((rows, channels), BF16),
            pltpu.VMEM((HALO + rows, channels), BF16),
            pltpu.VMEM((rows, q_cols), BF16),
            pltpu.VMEM((rows, channels), BF16),
            pltpu.VMEM((n_tp - 1, owned, q_cols), BF16),
            pltpu.VMEM((n_tp - 1, owned, channels), BF16),
            pltpu.VMEM((kv_here, group * WINDOW, 2 * WINDOW), F32),
            dma((lanes * n_sp * 2,)),
            dma((len(kinds) * shards,)),
            dma((12,)),
            dma((n_tp - 1, 2)),
            dma((n_tp - 1, 2)),
            dma((n_tp - 1, 4)),
            dma((n_tp - 1, 4)),
            dma((2,)),
            dma((2,)),
            dma((2, n_tp - 1)),
            dma((2, n_tp - 1)),
            dma((n_tp - 1, shards)),
            dma((n_tp - 1, shards)),
            dma((n_tp - 1, shards)),
            dma((n_tp - 1, shards)),
            pltpu.VMEM((owned, width), BF16),
            dma((n_sp,)),
            pltpu.VMEM((1, width), F32),
            pltpu.VMEM(conv_taps.shape, BF16),
            pltpu.SMEM(sink_logits.shape, F32),
        ],
        compiler_params=pltpu.CompilerParams(
            collective_id=0, has_side_effects=True, vmem_limit_bytes=60 * 1024 * 1024
        ),
    )(tokens[0], norm_gain[None], conv_taps, sink_logits, *weights, w_attn_out, w_conv_out)
    return copy_out(summed)[None]


def copy_out(array):
    rows, width = array.shape
    count = 8
    step = rows // count

    def kernel(source, target, held, sem):
        cut = lambda n: pl.ds(n * step, step)
        reads = [pltpu.make_async_copy(source.at[cut(n)], held.at[cut(n)], sem.at[0, n]) for n in range(count)]
        writes = [pltpu.make_async_copy(held.at[cut(n)], target.at[cut(n)], sem.at[1, n]) for n in range(count)]
        for copy in reads:
            copy.start()
        for read, write in zip(reads, writes):
            read.wait()
            write.start()
        for copy in writes:
            copy.wait()

    anywhere = pl.BlockSpec(memory_space=pl.ANY)
    return pl.pallas_call(
        kernel,
        out_shape=jax.ShapeDtypeStruct(array.shape, array.dtype),
        in_specs=[anywhere],
        out_specs=anywhere,
        scratch_shapes=[pltpu.VMEM(array.shape, array.dtype), pltpu.SemaphoreType.DMA((2, count))],
        compiler_params=pltpu.CompilerParams(vmem_limit_bytes=60 * 1024 * 1024),
    )(array)


def solution(mesh):
    placed = (
        P("fs", "sp", "tp"),
        P(),
        P(("sp", "fs"), "tp"),
        P(("sp", "fs"), "tp"),
        P(("sp", "fs"), "tp"),
        P(("sp", "fs"), "tp"),
        P(("sp", "fs"), "tp"),
        P(("sp", "fs"), "tp"),
        P(None, "tp"),
        P("tp"),
        P("tp", ("sp", "fs")),
        P("tp", ("sp", "fs")),
    )
    return jax.shard_map(
        on_device,
        mesh=mesh,
        in_specs=placed,
        out_specs=P("fs", ("sp", "tp"), None),
        check_vma=False,
    )
```

```python
import functools

import jax
import jax.numpy as jnp
from jax import lax
from jax.experimental import pallas as pl
from jax.experimental.pallas import tpu as pltpu
from jax.sharding import PartitionSpec as P

HEADS = 16
HEAD = 64
WINDOW = 128
HALO = 16
MESH = pl.DeviceIdType.MESH
DIRECT_AFTER = 2
WAYS = RIGHT, LEFT, ACROSS, CROSS, CORE, HAND = range(6)
BF16, F32 = jnp.bfloat16, jnp.float32


TABLE_FOR = (4, 2, 2)
TABLE = (
    (0, 1, 0, 0, 0, 0), (0, 0, 0, 0, 0, 0), (2, 1, 0, 0, 0, 0), (2, 0, 0, 0, 0, 0), (3, 8, 0, 0, 0, 0),
    (4, 1, 0, 0, 0, 0), (0, 2, 0, 0, 0, 0), (4, 0, 0, 0, 0, 0), (2, 2, 0, 0, 0, 0), (4, 2, 0, 0, 0, 0),
    (4, 3, 0, 0, 0, 0), (4, 4, 0, 0, 0, 0), (4, 8, 0, 0, 0, 0), (0, 3, 0, 0, 0, 0), (2, 3, 0, 0, 0, 0),
    (4, 1, 1, 0, 0, 0), (4, 1, 0, 1, 1, 0), (0, 1, 1, 0, 0, 0), (2, 4, 0, 0, 0, 0), (4, 0, 1, 0, 0, 0),
    (4, 0, 0, 1, 1, 0), (0, 4, 0, 0, 0, 0), (2, 0, 0, 1, 1, 0), (4, 2, 1, 0, 0, 0), (4, 2, 0, 1, 1, 0),
    (0, 8, 0, 0, 0, 0), (2, 2, 0, 1, 1, 0), (0, 1, 0, 0, 0, 1), (0, 0, 0, 0, 0, 1), (1, 1, 0, 0, 0, 1),
    (1, 0, 0, 0, 0, 1), (2, 1, 0, 0, 0, 1), (2, 0, 0, 0, 0, 1), (0, 2, 0, 0, 0, 1), (3, 8, 0, 0, 0, 1),
    (1, 2, 0, 0, 0, 1), (4, 1, 0, 0, 0, 1), (2, 2, 0, 0, 0, 1), (4, 0, 0, 0, 0, 1), (4, 2, 0, 0, 0, 1),
    (4, 3, 0, 0, 0, 1), (4, 4, 0, 0, 0, 1), (4, 8, 0, 0, 0, 1), (0, 3, 0, 0, 0, 1), (1, 3, 0, 0, 0, 1),
    (2, 3, 0, 0, 0, 1), (4, 1, 0, 1, 0, 1), (4, 1, 0, 1, 1, 1), (4, 1, 1, 0, 0, 1), (0, 1, 0, 1, 0, 1),
    (1, 1, 1, 0, 0, 1), (2, 4, 0, 0, 0, 1), (4, 0, 0, 1, 0, 1), (4, 0, 0, 1, 1, 1), (4, 0, 1, 0, 0, 1),
    (0, 1, 1, 0, 0, 1), (1, 1, 0, 1, 1, 1), (2, 0, 0, 1, 0, 1), (4, 2, 0, 1, 0, 1), (4, 2, 0, 1, 1, 1),
    (4, 2, 1, 0, 0, 1), (0, 0, 0, 1, 0, 1), (1, 0, 0, 1, 1, 1), (2, 0, 0, 1, 1, 1), (4, 3, 0, 1, 0, 1),
    (0, 1, 0, 0, 0, 2), (0, 0, 0, 0, 0, 2), (1, 1, 0, 0, 0, 2), (1, 0, 0, 0, 0, 2), (2, 1, 0, 0, 0, 2),
    (2, 0, 0, 0, 0, 2), (0, 2, 0, 0, 0, 2), (3, 8, 0, 0, 0, 2), (1, 2, 0, 0, 0, 2), (4, 1, 0, 0, 0, 2),
    (2, 2, 0, 0, 0, 2), (4, 0, 0, 0, 0, 2), (4, 2, 0, 0, 0, 2), (4, 3, 0, 0, 0, 2), (4, 4, 0, 0, 0, 2),
    (4, 8, 0, 0, 0, 2), (0, 3, 0, 0, 0, 2), (1, 3, 0, 0, 0, 2), (2, 3, 0, 0, 0, 2), (4, 1, 0, 1, 0, 2),
    (4, 1, 0, 1, 1, 2), (4, 1, 1, 0, 0, 2), (0, 1, 0, 1, 0, 2), (1, 1, 1, 0, 0, 2), (2, 4, 0, 0, 0, 2),
    (4, 0, 0, 1, 0, 2), (4, 0, 0, 1, 1, 2), (4, 0, 1, 0, 0, 2), (0, 1, 1, 0, 0, 2), (1, 1, 0, 1, 1, 2),
    (2, 0, 0, 1, 0, 2), (4, 2, 0, 1, 0, 2), (4, 2, 0, 1, 1, 2), (4, 2, 1, 0, 0, 2), (0, 0, 0, 1, 0, 2),
    (1, 0, 0, 1, 1, 2), (2, 0, 0, 1, 1, 2), (4, 3, 0, 1, 0, 2), (4, 3, 0, 1, 1, 2), (1, 1, 0, 0, 0, 3),
    (1, 0, 0, 0, 0, 3), (2, 1, 0, 0, 0, 3), (2, 0, 0, 0, 0, 3), (3, 8, 0, 0, 0, 3), (4, 1, 0, 0, 0, 3),
    (1, 2, 0, 0, 0, 3), (4, 0, 0, 0, 0, 3), (2, 2, 0, 0, 0, 3), (4, 2, 0, 0, 0, 3), (4, 3, 0, 0, 0, 3),
    (4, 4, 0, 0, 0, 3), (4, 8, 0, 0, 0, 3), (1, 3, 0, 0, 0, 3), (2, 3, 0, 0, 0, 3), (4, 1, 0, 1, 0, 3),
    (4, 1, 1, 0, 0, 3), (1, 1, 1, 0, 0, 3), (2, 4, 0, 0, 0, 3), (4, 0, 0, 1, 0, 3), (4, 0, 1, 0, 0, 3),
    (1, 4, 0, 0, 0, 3), (2, 0, 0, 1, 0, 3), (4, 2, 0, 1, 0, 3), (4, 2, 1, 0, 0, 3), (1, 8, 0, 0, 0, 3),
    (2, 2, 0, 1, 0, 3), (4, 3, 0, 1, 0, 3), (1, 0, 0), (2, 3, 0, 1, 1, 0), (4, 3, 1, 0, 0, 0), (4, 3, 0, 1, 1, 0),
    (4, 1, 1, 1, 1, 0), (4, 4, 1, 0, 0, 0), (2, 8, 0, 0, 0, 0), (4, 1, 0, 2, 1, 0), (4, 0, 1, 1, 1, 0),
    (2, 0, 0, 2, 1, 0), (4, 0, 0, 2, 1, 0), (4, 2, 1, 1, 1, 0), (0, 2, 0, 1, 0, 1), (1, 2, 0, 1, 1, 1),
    (2, 2, 0, 1, 0, 1), (4, 3, 1, 0, 0, 1), (4, 3, 0, 1, 1, 1), (4, 1, 1, 1, 0, 1), (4, 1, 1, 1, 1, 1),
    (4, 4, 1, 0, 0, 1), (0, 1, 1, 1, 0, 1), (1, 1, 1, 1, 1, 1), (2, 2, 0, 1, 1, 1), (4, 4, 0, 1, 0, 1),
    (4, 1, 0, 2, 1, 1), (4, 0, 1, 1, 0, 1), (0, 3, 0, 1, 0, 1), (1, 1, 0, 2, 1, 1), (3, 8, 0, 1, 0, 1),
    (2, 3, 0, 1, 0, 1), (4, 8, 0, 1, 0, 1), (4, 0, 0, 2, 1, 1), (4, 0, 1, 1, 1, 1), (0, 4, 0, 1, 0, 1),
    (1, 0, 0, 2, 1, 1), (2, 0, 0, 2, 1, 1), (0, 2, 0, 1, 0, 2), (1, 2, 0, 1, 1, 2), (2, 2, 0, 1, 0, 2),
    (4, 3, 1, 0, 0, 2), (4, 1, 0, 2, 0, 2), (4, 1, 1, 1, 1, 2), (4, 4, 1, 0, 0, 2), (0, 1, 0, 2, 0, 2),
    (1, 1, 1, 1, 1, 2), (2, 2, 0, 1, 1, 2), (4, 1, 1, 1, 0, 2), (4, 4, 0, 1, 1, 2), (4, 0, 1, 1, 0, 2),
    (0, 1, 1, 1, 0, 2), (1, 3, 0, 1, 1, 2), (3, 8, 0, 1, 1, 2), (2, 3, 0, 1, 0, 2), (4, 8, 0, 1, 1, 2),
    (4, 0, 0, 2, 0, 2), (4, 0, 1, 1, 1, 2), (0, 0, 0, 2, 0, 2), (1, 4, 0, 1, 1, 2), (2, 0, 0, 2, 0, 2),
    (2, 3, 0, 1, 0, 3), (4, 3, 1, 0, 0, 3), (4, 1, 0, 2, 0, 3), (4, 4, 1, 0, 0, 3), (2, 8, 0, 0, 0, 3),
    (4, 1, 1, 1, 0, 3), (4, 0, 1, 1, 0, 3), (2, 0, 0, 2, 0, 3), (4, 0, 0, 2, 0, 3), (4, 2, 1, 1, 0, 3), (1, 1, 0),
    (0, 8, 1, 0, 0, 0), (2, 2, 0, 2, 1, 0), (3, 8, 1, 0, 0, 0), (4, 2, 0, 2, 1, 0), (4, 3, 1, 1, 1, 0),
    (4, 8, 1, 0, 0, 0), (0, 4, 0, 0, 0, 1), (1, 2, 0, 2, 1, 1), (2, 2, 0, 2, 1, 1), (4, 2, 1, 1, 0, 1),
    (4, 2, 0, 2, 1, 1), (0, 2, 0, 2, 0, 2), (1, 4, 0, 0, 0, 2), (2, 2, 0, 2, 0, 2), (4, 2, 0, 2, 0, 2),
    (4, 2, 1, 1, 0, 2), (1, 8, 1, 0, 0, 3), (2, 2, 0, 2, 0, 3), (3, 8, 1, 0, 0, 3), (4, 2, 0, 2, 0, 3),
    (4, 3, 1, 1, 0, 3), (4, 8, 1, 0, 0, 3), (0, 0, 0), (4, 1, 1, 2, 1, 0), (0, 6, 0, 0, 0, 0), (0, 7, 0, 0, 0, 0),
    (2, 6, 0, 0, 0, 0), (2, 7, 0, 0, 0, 0), (4, 0, 1, 2, 1, 0), (4, 6, 0, 0, 0, 0), (0, 5, 0, 0, 0, 0),
    (4, 7, 0, 0, 0, 0), (4, 5, 0, 0, 0, 0), (2, 5, 0, 0, 0, 0), (4, 1, 0, 3, 1, 0), (4, 2, 1, 2, 1, 0),
    (2, 0, 0, 3, 1, 0), (4, 0, 0, 3, 1, 0), (4, 6, 1, 0, 0, 0), (2, 2, 0, 3, 1, 0), (4, 2, 0, 3, 1, 0),
    (4, 7, 1, 0, 0, 0), (4, 1, 1, 3, 1, 0), (4, 1, 1, 2, 1, 1), (4, 2, 1, 1, 1, 1), (0, 8, 0, 0, 0, 1),
    (4, 1, 1, 2, 0, 2), (4, 2, 1, 1, 1, 2), (4, 1, 0, 3, 0, 3), (1, 6, 0, 0, 0, 3), (1, 7, 0, 0, 0, 3),
    (2, 6, 0, 0, 0, 3), (2, 7, 0, 0, 0, 3), (4, 0, 1, 2, 0, 3), (4, 6, 0, 0, 0, 3), (1, 5, 0, 0, 0, 3),
    (4, 7, 0, 0, 0, 3), (4, 5, 0, 0, 0, 3), (2, 5, 0, 0, 0, 3), (4, 1, 1, 2, 0, 3), (4, 2, 1, 2, 0, 3),
    (2, 0, 0, 3, 0, 3), (4, 0, 0, 3, 0, 3), (4, 6, 1, 0, 0, 3), (2, 2, 0, 3, 0, 3), (4, 2, 0, 3, 0, 3),
    (4, 7, 1, 0, 0, 3), (4, 5, 1, 0, 0, 3), (4, 1, 1, 3, 0, 3), (2, 0, 1), (4, 5, 1, 0, 0, 0), (1, 1, 1, 2, 1, 1),
    (2, 3, 0, 1, 1, 1), (4, 6, 0, 0, 0, 1), (4, 7, 0, 0, 0, 1), (4, 5, 0, 0, 0, 1), (3, 8, 1, 1, 0, 1),
    (4, 8, 1, 1, 0, 1), (1, 6, 0, 0, 0, 2), (2, 3, 0, 1, 1, 2), (4, 6, 0, 0, 0, 2), (4, 7, 0, 0, 0, 2),
    (4, 5, 0, 0, 0, 2), (4, 0, 1, 3, 0, 3), (2, 1, 1), (4, 3, 1, 1, 0, 1), (4, 3, 0, 2, 1, 1), (1, 3, 0, 2, 1, 1),
    (2, 3, 0, 2, 1, 1), (0, 6, 0, 0, 0, 1), (4, 4, 0, 2, 1, 1), (4, 0, 1, 2, 1, 1), (4, 6, 0, 1, 0, 1),
    (1, 4, 0, 2, 1, 1), (2, 4, 0, 2, 1, 1), (0, 7, 0, 0, 0, 1), (4, 4, 0, 1, 1, 1), (4, 2, 1, 2, 1, 1),
    (4, 7, 0, 1, 0, 1), (1, 3, 0, 1, 1, 1), (2, 4, 0, 1, 0, 1), (0, 5, 0, 0, 0, 1), (4, 6, 0, 1, 1, 1),
    (4, 3, 1, 1, 1, 1), (4, 5, 0, 1, 0, 1), (1, 4, 0, 1, 1, 1), (3, 8, 1, 1, 1, 2), (4, 3, 0, 2, 0, 2),
    (4, 8, 1, 1, 1, 2), (4, 3, 1, 1, 0, 2), (0, 1, 1, 2, 0, 2), (1, 7, 0, 0, 0, 2), (2, 3, 0, 2, 0, 2),
    (4, 4, 0, 2, 0, 2), (4, 0, 1, 2, 0, 2), (4, 6, 0, 1, 1, 2), (0, 3, 0, 2, 0, 2), (1, 5, 0, 0, 0, 2),
    (2, 4, 0, 2, 0, 2), (4, 4, 0, 1, 0, 2), (4, 2, 1, 2, 0, 2), (4, 7, 0, 1, 1, 2), (0, 4, 0, 2, 0, 2),
    (1, 8, 0, 0, 0, 2), (3, 8, 0, 1, 0, 2), (2, 4, 0, 1, 0, 2), (4, 8, 0, 1, 0, 2), (1, 6, 0, 1, 1, 2),
    (4, 3, 1, 1, 1, 2), (4, 5, 0, 1, 1, 2), (0, 3, 0, 1, 0, 2), (1, 2, 0), (2, 3, 0, 3, 1, 0), (4, 0, 1, 3, 1, 0),
    (4, 3, 0, 3, 1, 0), (2, 4, 0, 3, 1, 0), (4, 4, 0, 3, 1, 0), (0, 6, 0, 1, 0, 1), (2, 4, 0, 1, 1, 1),
    (4, 3, 1, 2, 1, 1), (4, 7, 0, 1, 1, 1), (1, 7, 0, 1, 1, 2), (2, 4, 0, 1, 1, 2), (4, 3, 1, 2, 0, 2),
    (2, 3, 0, 3, 0, 3), (4, 2, 1, 3, 0, 3), (4, 3, 0, 3, 0, 3), (2, 1, 0), (2, 0, 0), (4, 2, 1, 3, 1, 0),
    (1, 4, 0, 0, 0, 1), (2, 6, 0, 0, 0, 1), (0, 4, 0, 1, 0, 2), (2, 6, 0, 0, 0, 2), (4, 6, 0, 1, 0, 2),
    (2, 4, 0, 3, 0, 3), (4, 4, 0, 3, 0, 3), (2, 2, 0), (0, 7, 0, 1, 0, 1), (2, 2, 1), (2, 3, 0, 2, 1, 0),
    (4, 3, 0, 2, 1, 0), (4, 4, 1, 2, 1, 1), (4, 5, 0, 1, 1, 1), (1, 5, 0, 1, 1, 2), (4, 4, 1, 2, 0, 2), (2, 1, 2),
    (1, 6, 0, 0, 0, 1), (0, 4, 0, 0, 0, 2), (3, 0, 0), (2, 4, 0, 2, 1, 0), (4, 3, 1, 3, 1, 0), (4, 4, 0, 2, 1, 0),
    (0, 5, 0, 1, 0, 1), (2, 7, 0, 0, 0, 1), (3, 8, 0, 1, 1, 1), (4, 4, 1, 1, 0, 1), (1, 7, 0, 0, 0, 1),
    (4, 8, 0, 1, 1, 1), (2, 5, 0, 0, 0, 1), (4, 6, 0, 2, 1, 1), (1, 8, 0, 1, 1, 2), (2, 7, 0, 0, 0, 2),
    (4, 4, 1, 1, 0, 2), (0, 6, 0, 0, 0, 2), (4, 7, 0, 1, 0, 2), (1, 8, 1, 1, 1, 2), (4, 5, 0, 1, 0, 2),
    (2, 5, 0, 0, 0, 2), (2, 3, 0, 2, 0, 3), (4, 3, 1, 3, 0, 3), (4, 3, 0, 2, 0, 3), (3, 1, 0), (2, 4, 0, 1, 1, 0),
    (4, 4, 1, 3, 1, 0), (4, 4, 0, 1, 1, 0), (5, 8, 0, 0, 0, 0), (0, 8, 0, 1, 0, 1), (0, 8, 1, 1, 0, 1),
    (1, 5, 0, 0, 0, 1), (2, 8, 0, 0, 0, 1), (4, 4, 1, 1, 1, 1), (4, 7, 0, 2, 1, 1), (0, 7, 0, 0, 0, 2),
    (4, 4, 1, 1, 1, 2), (4, 6, 0, 2, 0, 2), (2, 8, 0, 0, 0, 2), (2, 4, 0, 2, 0, 3), (4, 4, 1, 3, 0, 3),
    (4, 4, 0, 2, 0, 3), (5, 8, 0, 0, 0, 3), (5, 8, 1, 0, 0, 3), (4, 0, 0), (2, 2, 2), (4, 3, 1, 2, 1, 0),
    (5, 8, 1, 0, 0, 0), (2, 4, 0, 1, 0, 3), (4, 4, 0, 1, 0, 3), (1, 3, 0), (2, 6, 0, 1, 1, 0), (4, 6, 0, 1, 1, 0),
    (4, 4, 1, 2, 1, 0), (2, 7, 0, 1, 1, 0), (4, 7, 0, 1, 1, 0), (4, 4, 1, 1, 1, 0), (2, 6, 0, 1, 0, 1),
    (1, 8, 0, 0, 0, 1), (4, 6, 1, 0, 0, 1), (5, 8, 0, 0, 0, 1), (4, 5, 0, 2, 1, 1), (5, 8, 0, 1, 0, 1),
    (2, 6, 0, 1, 0, 2), (4, 6, 1, 0, 0, 2), (0, 5, 0, 0, 0, 2), (5, 8, 0, 0, 0, 2), (4, 3, 1, 2, 0, 3),
    (2, 6, 0, 1, 0, 3), (4, 6, 0, 1, 0, 3), (4, 4, 1, 2, 0, 3), (2, 7, 0, 1, 0, 3), (4, 7, 0, 1, 0, 3),
    (4, 4, 1, 1, 0, 3), (2, 2, 4), (2, 5, 0, 1, 1, 0), (4, 5, 0, 1, 1, 0), (4, 7, 0, 2, 0, 2), (5, 8, 0, 1, 1, 2),
    (2, 5, 0, 1, 0, 3), (4, 5, 0, 1, 0, 3), (2, 3, 1), (1, 6, 0, 1, 1, 1), (2, 6, 0, 1, 1, 1), (3, 8, 0, 2, 1, 1),
    (4, 7, 1, 0, 0, 1), (4, 8, 0, 2, 1, 1), (5, 8, 1, 1, 0, 1), (2, 1, 4), (3, 8, 0, 1, 1, 0), (4, 8, 0, 1, 1, 0),
    (4, 6, 1, 1, 1, 0), (2, 6, 0, 1, 1, 2), (4, 7, 1, 0, 0, 2), (5, 8, 1, 1, 1, 2), (3, 8, 0, 1, 0, 3),
    (4, 8, 0, 1, 0, 3), (4, 6, 1, 1, 0, 3), (2, 0, 2), (3, 8, 1, 2, 1, 1), (4, 8, 1, 2, 1, 1), (5, 8, 0, 1, 1, 1),
    (0, 8, 0, 0, 0, 2), (4, 5, 0, 2, 0, 2), (5, 8, 0, 1, 0, 2), (2, 0, 4), (2, 0, 3), (1, 7, 0, 1, 1, 1),
    (2, 7, 0, 1, 0, 1), (4, 5, 1, 0, 0, 1), (0, 6, 0, 1, 0, 2), (2, 7, 0, 1, 0, 2), (3, 8, 0, 2, 0, 2),
    (4, 5, 1, 0, 0, 2), (4, 8, 0, 2, 0, 2), (2, 2, 3), (2, 6, 0, 2, 1, 0), (4, 6, 0, 2, 1, 0), (4, 7, 1, 1, 1, 0),
    (4, 7, 1, 1, 0, 3), (2, 1, 3), (0, 8, 1, 0, 0, 1), (3, 8, 1, 0, 0, 1), (4, 8, 1, 0, 0, 1), (1, 8, 1, 0, 0, 2),
    (3, 8, 1, 0, 0, 2), (3, 8, 1, 2, 0, 2), (4, 8, 1, 0, 0, 2), (4, 8, 1, 2, 0, 2), (2, 6, 0, 2, 0, 3),
    (4, 6, 0, 2, 0, 3), (2, 3, 2), (1, 5, 0, 1, 1, 1), (2, 7, 0, 1, 1, 1), (5, 8, 0, 1, 0, 3), (2, 3, 3),
    (5, 8, 0, 1, 1, 0), (4, 6, 1, 1, 0, 1), (3, 8, 1, 1, 1, 1), (4, 8, 1, 1, 1, 1), (1, 8, 1, 0, 0, 1),
    (2, 5, 0, 1, 0, 1), (1, 8, 0, 1, 1, 1), (4, 6, 1, 1, 1, 1), (1, 6, 0, 2, 1, 1), (2, 5, 0, 1, 1, 1),
    (0, 7, 0, 1, 0, 2), (2, 7, 0, 1, 1, 2), (5, 0, 0), (2, 7, 0, 2, 1, 0), (4, 7, 0, 2, 1, 0), (4, 5, 1, 1, 1, 0),
    (2, 7, 0, 2, 0, 3), (4, 7, 0, 2, 0, 3), (4, 5, 1, 1, 0, 3), (2, 3, 0), (4, 6, 1, 1, 0, 2), (2, 3, 4),
    (4, 7, 1, 1, 0, 1), (3, 8, 1, 1, 0, 2), (2, 5, 0, 1, 0, 2), (4, 8, 1, 1, 0, 2), (3, 2, 0), (2, 5, 0, 2, 1, 0),
    (3, 8, 1, 1, 1, 0), (4, 5, 0, 2, 1, 0), (4, 8, 1, 1, 1, 0), (4, 6, 1, 2, 1, 0), (1, 7, 0, 2, 1, 1),
    (2, 6, 0, 2, 1, 1), (4, 7, 1, 1, 1, 1), (5, 8, 0, 2, 1, 1), (5, 8, 1, 2, 1, 1), (0, 5, 0, 1, 0, 2),
    (4, 6, 1, 1, 1, 2), (2, 5, 0, 1, 1, 2), (2, 5, 0, 2, 0, 3), (3, 8, 0, 2, 0, 3), (4, 5, 0, 2, 0, 3),
    (4, 8, 0, 2, 0, 3), (4, 6, 1, 2, 0, 3), (3, 3, 0), (3, 8, 0, 2, 1, 0), (4, 8, 0, 2, 1, 0), (4, 7, 1, 2, 1, 0),
    (1, 5, 0, 2, 1, 1), (2, 7, 0, 2, 1, 1), (4, 5, 1, 1, 0, 1), (5, 8, 1, 0, 0, 1), (5, 8, 1, 1, 1, 1),
    (0, 8, 0, 1, 0, 2), (0, 8, 1, 0, 0, 2), (4, 7, 1, 1, 0, 2), (2, 6, 0, 2, 0, 2), (5, 8, 0, 2, 0, 2),
    (3, 8, 1, 1, 0, 3), (4, 8, 1, 1, 0, 3), (4, 7, 1, 2, 0, 3), (5, 1, 0), (2, 6, 0, 3, 1, 0), (4, 6, 0, 3, 1, 0),
    (4, 5, 1, 2, 1, 0), (2, 7, 0, 3, 1, 0), (4, 7, 0, 3, 1, 0), (4, 6, 1, 3, 1, 0), (1, 8, 1, 1, 1, 1),
    (2, 5, 0, 2, 1, 1), (1, 8, 0, 2, 1, 1), (4, 5, 1, 1, 1, 1), (1, 8, 1, 2, 1, 1), (4, 6, 1, 2, 1, 1),
    (4, 7, 1, 2, 1, 1), (0, 6, 0, 2, 0, 2), (5, 8, 1, 0, 0, 2), (4, 7, 1, 1, 1, 2), (5, 8, 1, 2, 0, 2),
    (2, 7, 0, 2, 0, 2), (0, 7, 0, 2, 0, 2), (4, 5, 1, 1, 0, 2), (2, 5, 0, 2, 0, 2), (0, 5, 0, 2, 0, 2),
    (4, 5, 1, 1, 1, 2), (0, 8, 0, 2, 0, 2), (0, 8, 1, 1, 0, 2), (4, 6, 1, 2, 0, 2), (0, 8, 1, 2, 0, 2),
    (4, 7, 1, 2, 0, 2), (2, 6, 0, 3, 0, 3), (4, 6, 0, 3, 0, 3), (4, 5, 1, 2, 0, 3), (2, 7, 0, 3, 0, 3),
    (4, 7, 0, 3, 0, 3), (4, 6, 1, 3, 0, 3), (6, 0, 0), (7, 1, 1), (2, 5, 0, 3, 1, 0), (4, 5, 0, 3, 1, 0),
    (4, 5, 1, 2, 1, 1), (7, 0, 0), (3, 8, 1, 2, 1, 0), (4, 8, 1, 2, 1, 0), (5, 8, 1, 1, 1, 0), (4, 7, 1, 3, 1, 0),
    (5, 8, 0, 2, 1, 0), (3, 8, 0, 3, 1, 0), (4, 8, 0, 3, 1, 0), (3, 8, 1, 3, 1, 0), (4, 8, 1, 3, 1, 0),
    (5, 8, 1, 2, 1, 0), (4, 5, 1, 3, 1, 0), (5, 8, 0, 3, 1, 0), (4, 5, 1, 2, 0, 2), (5, 8, 1, 1, 0, 2),
    (2, 5, 0, 3, 0, 3), (4, 5, 0, 3, 0, 3), (7, 3, 1), (8, 0, 0), (5, 8, 1, 3, 1, 0), (5, 8, 0, 2, 0, 3), (8, 1, 1),
    (7, 1, 0), (3, 8, 0, 3, 0, 3), (4, 8, 0, 3, 0, 3), (4, 7, 1, 3, 0, 3), (5, 8, 1, 1, 0, 3), (7, 2, 1), (8, 3, 1),
    (3, 8, 1, 2, 0, 3), (4, 8, 1, 2, 0, 3), (7, 2, 0), (3, 8, 1, 3, 0, 3), (4, 5, 1, 3, 0, 3), (4, 8, 1, 3, 0, 3),
    (8, 2, 1), (5, 8, 0, 3, 0, 3), (7, 3, 0), (5, 8, 1, 2, 0, 3), (8, 1, 0), (5, 8, 1, 3, 0, 3), (8, 2, 0), (8, 3, 0),
)


def when(condition, body):
    if condition is True:
        body()
    elif condition is not False:
        pl.when(condition)(body)


def aligned(at, size):
    return at if isinstance(at, int) else pl.multiple_of(at, size)


class Part:
    def __init__(self, number, wide, crossing, place, base):
        self.number, self.wide, self.crossing, self.place, self.base = number, wide, crossing, place, base


def part_kinds(out_rows):
    kinds = [(False, False, None), (True, False, None)] + [(False, False, None)] * 3
    quarter = out_rows // 4
    kinds += [(False, False, (n * quarter, quarter)) for n in range(3)]
    return kinds + [(True, True, (3 * quarter, quarter))]


def lanes_of(wide, n_out):
    return 1 + n_out + (2 if wide else 1) * (n_out - 1)


def layer_kernel(sizes, *refs):
    n_sp, n_out, n_tp, n_proj, separate = sizes
    tok = refs[0]
    n_in = 6 if separate else 5
    w_own = refs[4 : 4 + n_in]
    out_own = refs[4 + n_in : 6 + n_in]
    out = refs[6 + n_in]
    (tokf, w_all, wo_all, q_buf, kv_buf, inner, gate_b, product, m_att, m_conv, r_att, r_conv, bias,
     send_sem, recv_sem, own_sem, wo_send, wo_recv, tok_send, tok_recv, halo_send, halo_recv,
     mix_send, mix_recv, cross_send, cross_recv, pass_send, pass_recv,
     out_buf, out_sem, gain, taps, sinks) = refs[7 + n_in :]
    out_hbm, out = out, out_buf
    n_fs = 2 * n_out
    shards = n_sp * n_fs
    s, f, t = lax.axis_index("sp"), lax.axis_index("fs"), lax.axis_index("tp")
    o, i = f // 2, f % 2
    rows_total, width = tokf.shape
    cols = tok.shape[1]
    q_cols = q_buf.shape[1]
    kv_cols = kv_buf.shape[1] // 2
    k_rows = w_own[0].shape[0]
    out_rows, out_cols = out_own[0].shape
    owned = rows_total // n_tp
    chunks = 4
    step = rows_total // chunks
    tabled = (n_sp, n_out, n_tp) == TABLE_FOR
    order = [3, 0, 1, 2]
    attended = [0, 1, 2, 3]
    if tabled:
        order = [3, 2 - 2 * t, 1, 2 * t]
        attended = [3 - 3 * t, 2 - t, 1 + t, 3 * t]
    me = s * n_fs + f

    right, left, core = (s + 1, f, t), (s - 1, f, t), (s, o * 2 + (1 - i), t)
    across = [(s, lax.rem(o + k, n_out) * 2 + i, t) for k in range(1, n_out)]
    peers = [(s, f, lax.rem(t + k, n_tp)) for k in range(1, n_tp)]
    has_right, has_left = s < n_sp - 1, s > 0

    local = []
    spots = [(0, 0), (1, 0), (1, kv_cols), (2, 0), (3, 0), (4, 0)] if separate else [(n, 0) for n in range(5)]
    for n, (number, col) in enumerate(spots):
        place = w_all.at[number, pl.ds(me * k_rows, k_rows), pl.ds(col, w_own[n].shape[1])]
        local.append(pltpu.make_async_copy(w_own[n], place, own_sem.at[n]))
    for a in range(2):
        local.append(pltpu.make_async_copy(out_own[a], wo_all.at[2 * t + a, me], own_sem.at[6 + a]))
    for n, (source_ref, spot) in enumerate(zip(refs[1:4], (gain, taps, sinks))):
        local.append(pltpu.make_async_copy(source_ref, spot, own_sem.at[9 + n]))
    my_cols = pl.ds(pl.multiple_of(t * cols, cols), cols)
    local.append(pltpu.make_async_copy(tok, tokf.at[:, my_cols], own_sem.at[8]))
    for copy in local:
        copy.start()

    barrier = pltpu.get_barrier_semaphore()
    greet = lambda where: pl.semaphore_signal(barrier, inc=1, device_id=where, device_id_type=MESH)
    when(has_right, lambda: greet(right))
    when(has_left, lambda: greet(left))
    for where in across + [core] + peers:
        greet(where)
    count = len(across) + 1 + len(peers)
    pl.semaphore_wait(barrier, count + has_right.astype(jnp.int32) + has_left.astype(jnp.int32))

    wo_copies, tok_copies = [], {}
    direct = pl.ds(0, 3 * (out_rows // 4))
    def send_direct():
        for k, peer in enumerate(peers):
            for a in range(2):
                copy = pltpu.make_async_remote_copy(
                    src_ref=out_own[a].at[direct], dst_ref=wo_all.at[2 * t + a, me, direct],
                    send_sem=wo_send.at[k, a], recv_sem=wo_recv.at[k, a], device_id=peer, device_id_type=MESH,
                )
                copy.start()
                wo_copies.append(copy)

    wanted = [3, 2 * t, 1, 2 - 2 * t] if tabled else order
    for turn, n in enumerate(wanted):
        if turn == DIRECT_AFTER:
            send_direct()
        here = pl.ds(aligned(n * step, step), step)
        for k, peer in enumerate(peers):
            copy = pltpu.make_async_remote_copy(
                src_ref=tok.at[here], dst_ref=tokf.at[here, my_cols],
                send_sem=tok_send.at[k, turn], recv_sem=tok_recv.at[k, turn], device_id=peer, device_id_type=MESH,
            )
            copy.start()
            tok_copies[k, turn] = copy

    parts, base = [], 0
    for number, (wide, crossing, rows) in enumerate(part_kinds(out_rows)):
        if rows is None:
            place = lambda src, g, number=number: w_all.at[number, pl.ds(src * k_rows, k_rows)]
        elif crossing:
            place = lambda src, g, rows=rows: wo_all.at[pl.ds(2 * g, 2), src, pl.ds(*rows)]
        else:
            place = lambda src, g, rows=rows: wo_all.at[:, src, pl.ds(*rows)]
        parts.append(Part(number, wide, crossing, place, base))
        base += lanes_of(wide, n_out) * n_sp * 2

    def copy_of(part, src, where, lane, distance, side):
        spot = part.place(src, t)
        return pltpu.make_async_remote_copy(
            src_ref=spot, dst_ref=spot,
            send_sem=send_sem.at[part.base + (lane * n_sp + distance) * 2 + side],
            recv_sem=recv_sem.at[part.number * shards + src],
            device_id=where, device_id_type=MESH,
        )

    def cross_copy(part, src, k):
        spot = part.place(src, t)
        return pltpu.make_async_remote_copy(
            src_ref=spot, dst_ref=spot, send_sem=cross_send.at[k, src], recv_sem=cross_recv.at[k, src],
            device_id=peers[k], device_id_type=MESH,
        )

    def pass_copy(part, src, k):
        spot = part.place(src, lax.rem(t + n_tp - k - 1, n_tp))
        return pltpu.make_async_remote_copy(
            src_ref=spot, dst_ref=spot, send_sem=pass_send.at[k, src], recv_sem=pass_recv.at[k, src],
            device_id=core, device_id_type=MESH,
        )

    def source(k, at):
        return at * n_fs + lax.rem(o + n_out - k, n_out) * 2 + i

    def handle(part, k, distance, side, at, drain, ways=WAYS, arrival=True):
        first = isinstance(distance, int) and distance == 0
        src = source(k, at)
        mine = (at + distance if side == 0 else at - distance) if isinstance(at, int) else s
        more_right, more_left = mine < n_sp - 1, mine > 0
        lane_z, lane_core = 0, 1
        if k > 0:
            lane_z = 2 + len(across) + 2 * (k - 1)
            lane_core = lane_z + 1
            if not part.wide:
                lane_core = 2 + len(across) + k - 1

        def go(where, lane, way):
            copy = copy_of(part, src, where, lane, distance, way)
            copy.wait_send() if drain else copy.start()

        if arrival and not (first and k == 0) and not drain:
            copy_of(part, src, core, 0, 0, 0).wait_recv()
        if k == 0 or part.wide:
            if RIGHT in ways and (first or side == 0):
                when(more_right, lambda: go(right, lane_z, 0))
            if LEFT in ways and (first or side == 1):
                when(more_left, lambda: go(left, lane_z, 1))
        if ACROSS in ways and k == 0 and (first or not part.wide):
            for n, where in enumerate(across):
                go(where, 2 + n, side)
        if CROSS in ways and part.crossing:
            for n in range(len(peers)):
                copy = cross_copy(part, src, n)
                copy.wait_send() if drain else copy.start()
        if CORE in ways:
            go(core, lane_core, side)

    def hand_over(part, src, drain):
        for k in range(len(peers)):
            if not drain:
                cross_copy(part, src, k).wait_recv()
            copy = pass_copy(part, src, k)
            copy.wait_send() if drain else copy.start()

    def deal(part, distance, k, drain):
        if isinstance(distance, int) and distance == 0:
            handle(part, k, 0, 0, s, drain)
            return
        when(s - distance >= 0, lambda: handle(part, k, distance, 0, s - distance, drain))
        when(s + distance < n_sp, lambda: handle(part, k, distance, 1, s + distance, drain))

    def partner(number, source_s):
        for source_o in range(n_out):
            copy_of(parts[number], source_s * n_fs + source_o * 2 + (1 - i), core, 0, 0, 0).wait_recv()

    def finish(number):
        for source_s in range(n_sp):
            partner(number, source_s)

    def norm(n):
        size = 32

        def body(r, carry):
            here = pl.ds(pl.multiple_of(n * step + r * size, size), size)
            values = tokf[here, :].astype(F32)
            centred = values - jnp.sum(values, axis=1, keepdims=True) * (1.0 / width)
            variance = jnp.sum(centred * centred, axis=1, keepdims=True) * (1.0 / width)
            tokf[here, :] = (centred * lax.rsqrt(variance + 1e-05) * gain[...]).astype(BF16)
            return carry

        lax.fori_loop(0, step // size, body, 0)

    def project(number, n):
        first = aligned(n * step, step)
        here = pl.ds(first, step)
        result = jnp.dot(tokf[here, :], w_all[number], preferred_element_type=F32).astype(BF16)
        if number == 0:
            q_buf[here, :] = result
        elif number == 1:
            kv_buf[pl.ds(first + WINDOW, step), :] = result
        elif number == 2:
            inner[here, :] = result
        elif number == 3:
            gate_b[here, :] = result
        else:
            made = result.astype(F32) * inner[here, :].astype(F32)
            product[pl.ds(first + HALO, step), :] = made.astype(BF16)

    def halo_copy(which):
        buffer, size = ((kv_buf, WINDOW), (product, HALO))[which]
        return pltpu.make_async_remote_copy(
            src_ref=buffer.at[pl.ds(rows_total, size)], dst_ref=buffer.at[pl.ds(0, size)],
            send_sem=halo_send.at[which], recv_sem=halo_recv.at[which], device_id=right, device_id_type=MESH,
        )

    def halo_out(which):
        when(has_right, lambda: halo_copy(which).start())

        def clear():
            buffer, size = ((kv_buf, WINDOW), (product, HALO))[which]
            buffer[0:size, :] = jnp.zeros((size, buffer.shape[1]), BF16)

        when(s == 0, clear)

    def halo_in(which):
        when(has_left, lambda: halo_copy(which).wait_recv())

    heads_here = q_cols // HEAD
    kv_here = kv_cols // HEAD
    group = heads_here // kv_here
    tall = group * WINDOW

    def make_bias():
        row = lax.broadcasted_iota(jnp.int32, (tall, 2 * WINDOW), 0)
        col = lax.broadcasted_iota(jnp.int32, (tall, 2 * WINDOW), 1)
        distance = WINDOW + row % WINDOW - col
        keep = (distance >= 0) & (distance < WINDOW)
        for h in range(kv_here):
            head = (t * heads_here + h * group + row // WINDOW + 1).astype(F32)
            slope = jnp.exp2(head * (-8.0 / HEADS))
            bias[h] = jnp.where(keep, -(slope * distance.astype(F32)), -jnp.inf)

    def attend(n):
        row = lax.broadcasted_iota(jnp.int32, (tall, 1), 0) // WINDOW
        col = lax.broadcasted_iota(jnp.int32, (1, 2 * WINDOW), 1)

        def body(b, carry):
            block = n * (step // WINDOW) + b
            first = pl.multiple_of(block * WINDOW, WINDOW)
            before = jnp.where(col >= WINDOW, 0.0, jnp.where((s == 0) & (block == 0), -jnp.inf, 0.0))
            queries = q_buf[pl.ds(first, WINDOW), :]
            band = kv_buf[pl.ds(first, 2 * WINDOW), :]
            outs = []
            for h in range(kv_here):
                query = jnp.concatenate(
                    [queries[:, (h * group + g) * HEAD : (h * group + g + 1) * HEAD] for g in range(group)], axis=0
                )
                key = band[:, h * HEAD : (h + 1) * HEAD]
                value = band[:, kv_cols + h * HEAD : kv_cols + (h + 1) * HEAD]
                scores = lax.dot_general(query, key, (((1,), (1,)), ((), ())), preferred_element_type=F32)
                scores = scores * HEAD ** (-0.5) + bias[h] + before
                sink = jnp.full((tall, 1), sinks[h * group], F32)
                for g in range(1, group):
                    sink = jnp.where(row == g, sinks[h * group + g], sink)
                top = jnp.maximum(jnp.max(scores, axis=1, keepdims=True), sink)
                raised = jnp.exp(scores - top)
                total = jnp.sum(raised, axis=1, keepdims=True) + jnp.exp(sink - top)
                weights = (raised * (1.0 / total)).astype(BF16)
                mixed = jnp.dot(weights, value, preferred_element_type=F32).astype(BF16)
                outs += [mixed[g * WINDOW : (g + 1) * WINDOW] for g in range(group)]
            m_att[pl.ds(first, WINDOW), :] = jnp.concatenate(outs, axis=1)
            return carry

        lax.fori_loop(0, step // WINDOW, body, 0)

    def convolve(start, count):
        size = 64

        def body(r, carry):
            first = pl.multiple_of(start + r * size, size)
            padded = product[pl.ds(first, size + HALO), :].astype(F32)
            tap = taps[...].astype(F32)
            filtered = (
                tap[0:1] * padded[HALO - 2 : HALO - 2 + size]
                + tap[1:2] * padded[HALO - 1 : HALO - 1 + size]
                + tap[2:3] * padded[HALO : HALO + size]
            )
            m_conv[pl.ds(first, size), :] = (gate_b[pl.ds(first, size), :].astype(F32) * filtered).astype(BF16)
            return carry

        lax.fori_loop(0, count // size, body, 0)

    def mix_copy(which, k):
        source, target = ((m_att, r_att), (m_conv, r_conv))[which]
        return pltpu.make_async_remote_copy(
            src_ref=source.at[pl.ds(pl.multiple_of(peers[k][2] * owned, owned), owned)], dst_ref=target.at[k],
            send_sem=mix_send.at[which, k], recv_sem=mix_recv.at[which, k],
            device_id=peers[k], device_id_type=MESH,
        )

    def mix_out(which):
        for k in range(n_tp - 1):
            mix_copy(which, k).start()

    def mix_in():
        for which in range(2):
            for k in range(n_tp - 1):
                mix_copy(which, k).wait_recv()

    def project_out(source_s, own):
        for number in range(n_proj, len(parts)):
            if own:
                partner(number, source_s)
            elif parts[number].crossing:
                for source_o in range(n_out):
                    for k in range(n_tp - 1):
                        pass_copy(parts[number], source_s * n_fs + source_o * 2 + (1 - i), k).wait_recv()
        block = n_fs * out_cols
        tile = min(512, owned)

        def weights(row):
            blocks = [wo_all[row, source_s * n_fs + n] for n in range(n_fs)]
            return jnp.concatenate(blocks, axis=1)

        def body(r, carry):
            here = pl.ds(pl.multiple_of(r * tile, tile), tile)
            where = pl.ds(pl.multiple_of(source_s * block, block), block)
            total = None if own else out[here, where].astype(F32)
            for k in (0,) if own else range(1, n_tp):
                g = lax.rem(t + n_tp - k, n_tp)
                if own:
                    mine = pl.ds(pl.multiple_of(t * owned + r * tile, tile), tile)
                    att, conv = m_att[mine, :], m_conv[mine, :]
                else:
                    att, conv = r_att[k - 1, here, :], r_conv[k - 1, here, :]
                partial = jnp.dot(att, weights(2 * g), preferred_element_type=F32)
                partial = partial + jnp.dot(conv, weights(2 * g + 1), preferred_element_type=F32)
                total = partial if own else total + partial.astype(BF16).astype(F32)
            out[here, where] = total.astype(BF16)
            return carry

        lax.fori_loop(0, owned // tile, body, 0)
        if not own:
            out_copy(source_s).start()

    def out_copy(source_s):
        block = n_fs * out_cols
        where = pl.ds(pl.multiple_of(source_s * block, block), block)
        return pltpu.make_async_copy(out.at[:, where], out_hbm.at[:, where], out_sem.at[source_s])

    own_weights, own_out, small, own_tokens = local[:-6], local[-6:-4], local[-4:-1], local[-1]
    waited = set()

    def once(key, body):
        if key not in waited:
            waited.add(key)
            body()

    def wait_all(copies):
        for copy in copies:
            copy.wait()

    def wo_ready():
        for copy in wo_copies:
            copy.wait_recv()

    def job(kind, n, side):
        if kind == 0:
            make_bias()
        elif kind == 1:
            once("tokens", lambda: wait_all(small + [own_tokens]))
            for k in range(n_tp - 1):
                tok_copies[k, n].wait_recv()
            norm(order[n])
        elif kind == 2:
            once(("part", side), lambda: finish(side))
            project(side, order[n])
            if n == 0 and side in (1, 4):
                halo_out(0 if side == 1 else 1)
        elif kind == 3:
            once("halo", lambda: halo_in(0))
            attend(attended[n])
        elif kind == 4:
            mix_out(0)
        elif kind == 5:
            once("product", lambda: halo_in(1))
            if not tabled:
                convolve(0, rows_total)
            else:
                convolve((t if n == 1 else 1 - t) * owned, owned)
            if n == 0:
                mix_out(1)
        elif kind == 6:
            mix_in()
        elif n == 0:
            project_out(s, kind == 7)
        elif side == 0:
            when(s - n >= 0, lambda: project_out(s - n, kind == 7))
        else:
            when(s + n < n_sp, lambda: project_out(s + n, kind == 7))

    wait_all(own_weights)
    if tabled:
        events = []

        def flush():
            for mine in range(n_sp):
                turn = [entry for entry in events if entry[5] == mine]

                def body(mine=mine, turn=turn):
                    for way, number, k, distance, side, _ in turn:
                        part = parts[number]
                        at = mine - distance if side == 0 else mine + distance
                        if way == HAND:
                            hand_over(part, source(k, at), False)
                            continue
                        if distance == 0 and k == 0 and number >= n_proj:
                            once(("own", mine), lambda: wait_all(own_out))
                            if not part.crossing:
                                once(("direct", mine), wo_ready)
                        piece = (mine, number, k, distance, side)
                        handle(part, k, distance, side, at, False, (way,), piece not in waited)
                        waited.add(piece)

                if turn:
                    pl.when(s == mine)(body)
            events.clear()

        for entry in TABLE:
            if len(entry) == 6:
                events.append(entry)
            else:
                flush()
                job(*entry)
        flush()
    else:
        wait_all(own_out)
        wo_ready()

        def spread(part):
            deal(part, 0, 0, False)
            for n in range(1, n_sp + 1):
                if n < n_sp:
                    deal(part, n, 0, False)
                for k in range(1, n_out):
                    deal(part, n - 1, k, False)

        for part in parts[:n_proj]:
            spread(part)
        job(0, 0, 0)
        for n in range(chunks):
            job(1, n, 0)
            job(2, n, 0)
            job(2, n, 1)
        for n in range(chunks):
            job(3, n, 0)
        job(4, 0, 0)
        for number in (2, 3, 4):
            for n in range(chunks):
                job(2, n, number)
        job(5, 0, 0)
        for part in parts[n_proj:]:
            spread(part)
        for at in range(n_sp):
            for k in range(n_out):
                hand_over(parts[-1], source(k, at), False)
        job(6, 0, 0)
        for own in (True, False):
            lax.fori_loop(0, n_sp, lambda n, c, own=own: (project_out(n, own), c)[1], 0)

    for source_s in range(n_sp):
        out_copy(source_s).wait()
    if tabled:
        events = [entry for entry in TABLE if len(entry) == 6]
        for mine in range(n_sp):

            def drain(mine=mine):
                for way, number, k, distance, side, _ in [entry for entry in events if entry[5] == mine]:
                    at = mine - distance if side == 0 else mine + distance
                    if way == HAND:
                        hand_over(parts[number], source(k, at), True)
                    else:
                        handle(parts[number], k, distance, side, at, True, (way,))

            pl.when(s == mine)(drain)
    else:
        for part in parts:
            for k in range(n_out):
                for distance in range(n_sp):
                    deal(part, distance, k, True)
        for at in range(n_sp):
            for k in range(n_out):
                hand_over(parts[-1], source(k, at), True)
    for which in range(2):
        when(has_right, lambda which=which: halo_copy(which).wait_send())
        for k in range(n_tp - 1):
            mix_copy(which, k).wait_send()
    for copy in wo_copies + list(tok_copies.values()):
        copy.wait_send()


def on_device(tokens, norm_gain, w_query, w_key, w_value, w_conv_in, w_conv_b, w_conv_c,
              conv_taps, sink_logits, w_attn_out, w_conv_out):
    n_sp, n_fs, n_tp = (lax.axis_size(axis) for axis in ("sp", "fs", "tp"))
    n_out = n_fs // 2
    shards = n_sp * n_fs
    rows, cols = tokens.shape[1:]
    width = cols * n_tp
    q_cols, kv_cols, channels = w_query.shape[1], w_key.shape[1], w_conv_in.shape[1]
    out_rows, out_cols = w_attn_out.shape
    separate = kv_cols % 128 == 0
    weights = [w_query]
    weights += [w_key, w_value] if separate else [jnp.concatenate([w_key, w_value], axis=1)]
    weights += [w_conv_in, w_conv_b, w_conv_c]
    owned = rows // n_tp
    kinds = part_kinds(out_rows)
    lanes = sum(lanes_of(wide, n_out) for wide, _, _ in kinds)
    kv_here = kv_cols // HEAD
    group = q_cols // kv_cols
    dma = pltpu.SemaphoreType.DMA
    summed = pl.pallas_call(
        functools.partial(layer_kernel, (n_sp, n_out, n_tp, 5, separate)),
        out_shape=jax.ShapeDtypeStruct((owned, width), BF16),
        in_specs=[pl.BlockSpec(memory_space=pltpu.HBM)] * (len(weights) + 6),
        out_specs=pl.BlockSpec(memory_space=pl.ANY),
        scratch_shapes=[
            pltpu.VMEM((rows, width), BF16),
            pltpu.VMEM((5, width, q_cols), BF16),
            pltpu.VMEM((2 * n_tp, shards, out_rows, out_cols), BF16),
            pltpu.VMEM((rows, q_cols), BF16),
            pltpu.VMEM((WINDOW + rows, 2 * kv_cols), BF16),
            pltpu.VMEM((rows, channels), BF16),
            pltpu.VMEM((rows, channels), BF16),
            pltpu.VMEM((HALO + rows, channels), BF16),
            pltpu.VMEM((rows, q_cols), BF16),
            pltpu.VMEM((rows, channels), BF16),
            pltpu.VMEM((n_tp - 1, owned, q_cols), BF16),
            pltpu.VMEM((n_tp - 1, owned, channels), BF16),
            pltpu.VMEM((kv_here, group * WINDOW, 2 * WINDOW), F32),
            dma((lanes * n_sp * 2,)),
            dma((len(kinds) * shards,)),
            dma((12,)),
            dma((n_tp - 1, 2)),
            dma((n_tp - 1, 2)),
            dma((n_tp - 1, 4)),
            dma((n_tp - 1, 4)),
            dma((2,)),
            dma((2,)),
            dma((2, n_tp - 1)),
            dma((2, n_tp - 1)),
            dma((n_tp - 1, shards)),
            dma((n_tp - 1, shards)),
            dma((n_tp - 1, shards)),
            dma((n_tp - 1, shards)),
            pltpu.VMEM((owned, width), BF16),
            dma((n_sp,)),
            pltpu.VMEM((1, width), F32),
            pltpu.VMEM(conv_taps.shape, BF16),
            pltpu.SMEM(sink_logits.shape, F32),
        ],
        compiler_params=pltpu.CompilerParams(
            collective_id=0, has_side_effects=True, vmem_limit_bytes=60 * 1024 * 1024
        ),
    )(tokens[0], norm_gain[None], conv_taps, sink_logits, *weights, w_attn_out, w_conv_out)
    return copy_out(summed)[None]


def copy_out(array):
    rows, width = array.shape
    count = 8
    step = rows // count

    def kernel(source, target, held, sem):
        cut = lambda n: pl.ds(n * step, step)
        reads = [pltpu.make_async_copy(source.at[cut(n)], held.at[cut(n)], sem.at[0, n]) for n in range(count)]
        writes = [pltpu.make_async_copy(held.at[cut(n)], target.at[cut(n)], sem.at[1, n]) for n in range(count)]
        for copy in reads:
            copy.start()
        for read, write in zip(reads, writes):
            read.wait()
            write.start()
        for copy in writes:
            copy.wait()

    anywhere = pl.BlockSpec(memory_space=pl.ANY)
    return pl.pallas_call(
        kernel,
        out_shape=jax.ShapeDtypeStruct(array.shape, array.dtype),
        in_specs=[anywhere],
        out_specs=anywhere,
        scratch_shapes=[pltpu.VMEM(array.shape, array.dtype), pltpu.SemaphoreType.DMA((2, count))],
        compiler_params=pltpu.CompilerParams(vmem_limit_bytes=60 * 1024 * 1024),
    )(array)


def solution(mesh):
    placed = (
        P("fs", "sp", "tp"),
        P(),
        P(("sp", "fs"), "tp"),
        P(("sp", "fs"), "tp"),
        P(("sp", "fs"), "tp"),
        P(("sp", "fs"), "tp"),
        P(("sp", "fs"), "tp"),
        P(("sp", "fs"), "tp"),
        P(None, "tp"),
        P("tp"),
        P("tp", ("sp", "fs")),
        P("tp", ("sp", "fs")),
    )
    return jax.shard_map(
        on_device,
        mesh=mesh,
        in_specs=placed,
        out_specs=P("fs", ("sp", "tp"), None),
        check_vma=False,
    )
```
